32 devices in a mesh: sp: 4 (over z), tp: 4 (over y, x), dp: 2 (over core).
Axes of the slice: x: 2, y: 2, z: 4, core: 2. Of those that a mesh axis runs over, the one named last changes fastest.
Arguments:
- latent: bfloat16 [2, 1536, 2048], P('dp', 'sp'), may hold values from -6 to 6
- conditioning: bfloat16 [2, 2048], P(None, 'sp'), may hold values from -6 to 6
- context_cond: bfloat16 [2048], P('sp'), may hold values from -6 to 6
- modulation: bfloat16 [3, 2048, 2048], P(None, 'sp', ('tp', 'dp')), may hold values from -4.2426407 to 4.2426407
- context: bfloat16 [2, 256, 2048], P('dp', 'sp'), may hold values from -6 to 6
- query_weight: bfloat16 [2048, 1024], P(None, 'tp'), may hold values from -2.1213203 to 2.1213203
- key_projection: bfloat16 [2048, 256], P(None, 'tp'), may hold values from -0.13258252 to 0.13258252
- value_projection: bfloat16 [2048, 256], P(None, 'tp'), may hold values from -0.125 to 0.125
- out_weight: bfloat16 [1024, 2048], P(None, 'tp'), may hold values from -0.1875 to 0.1875
- sink_head_logit: float32 [16], P('tp'), may hold values from 5 to 7.5
- prefix_logit_bias: float32 [16], P('tp'), may hold values from -2.5 to -1
Outputs:
- updated: float32 [2, 1536, 2048], P('dp', 'sp', 'tp')
The draws below stay inside these ranges and needn't reach their ends.
All inputs are finite; a program needn't handle non-finite values.
Results may differ from the reference program's by a relative error of at most 0.0073.
Values may be sent and summed in bfloat16 or wider, within the bound.
A program may use at most 64 MiB of HBM per device.

```python
import jax
import jax.numpy as jnp
from jax import lax

MODEL_WIDTH = 2048
QUERY_HEADS = 16
KEY_VALUE_HEADS = 4
HEAD_SIZE = 64
GRID_W = 64
WINDOW_REACH = 128
SAMPLES = 2
LATENT_TOKENS = 1536
CONTEXT_TOKENS = 256


def key_lookup_table(key):
    clip_bound = 6.0 * MODEL_WIDTH ** (-0.5)
    sampled_draws = jax.random.normal(jax.random.fold_in(key, 71), (MODEL_WIDTH, KEY_VALUE_HEADS * HEAD_SIZE), jnp.float32) * MODEL_WIDTH ** (-0.5)
    return jnp.clip(sampled_draws, -clip_bound, clip_bound)


def draw_key_projection(key, part):
    return key_lookup_table(key).astype(jnp.bfloat16)


def draw_query_weight(key, part):
    query_key = jax.random.fold_in(key, 72)
    clip_bound = 6.0 * MODEL_WIDTH ** (-0.5)
    sampled_draws = jax.random.normal(query_key, (MODEL_WIDTH, QUERY_HEADS * HEAD_SIZE), jnp.float32) * MODEL_WIDTH ** (-0.5)
    sampled_draws = jnp.clip(sampled_draws, -clip_bound, clip_bound)
    return sampled_draws.astype(jnp.bfloat16)


def draw_modulation(key, part):
    mod_key = jax.random.fold_in(key, 73)
    sampled_draws = jnp.clip(jax.random.normal(mod_key, (3, MODEL_WIDTH, MODEL_WIDTH), jnp.float32), -6.0, 6.0)
    boost = jnp.array([1.0, 1.0, 32.0], jnp.float32)[:, None, None]
    return (sampled_draws * boost * MODEL_WIDTH ** (-0.5)).astype(jnp.bfloat16)


def block_scale(rng, extent, cuts, low, largest):
    def one(position, shards_of):
        draws = jax.random.uniform(jax.random.fold_in(jax.random.fold_in(rng, 6), position), (shards_of,), jnp.float32, low / len(cuts), largest / len(cuts))
        return jnp.repeat(jnp.exp(draws), extent[position] // shards_of).reshape((-1,) + (1,) * (len(extent) - position - 1))

    factor_of = one(*cuts[0])
    for cut in cuts[1:]:
        factor_of = factor_of * one(*cut)
    return factor_of


def bell_draw(key, shape, deviation, limit, split=(), kind=jnp.bfloat16):
    drawn = jax.random.normal(key, shape, jnp.float32) * deviation
    if len(split) > 0:
        drawn = block_scale(key, shape, split, -0.22, 0.18) * drawn
    return jnp.clip(drawn, min=-limit, max=limit).astype(kind)


def setup_inputs(seed: int = 0) -> dict:
    key_list = jax.random.split(jax.random.key(seed), 12)
    latent = bell_draw(key_list[0], (SAMPLES, LATENT_TOKENS, MODEL_WIDTH), 1.0, 6.0, ((0, 2), (1, 4)))
    conditioning = bell_draw(key_list[1], (SAMPLES, MODEL_WIDTH), 1.0, 6.0, ((1, 4),))
    context_cond = bell_draw(key_list[2], (MODEL_WIDTH,), 1.0, 6.0, ((0, 4),))
    modulation = draw_modulation(jax.random.fold_in(key_list[11], 71), 0)
    context = bell_draw(key_list[4], (SAMPLES, CONTEXT_TOKENS, MODEL_WIDTH), 1.0, 6.0, ((0, 2), (1, 4)))
    query_weight = draw_query_weight(jax.random.fold_in(key_list[11], 71), 0)
    key_projection = draw_key_projection(jax.random.fold_in(key_list[11], 71), 0)
    value_projection = bell_draw(key_list[7], (MODEL_WIDTH, KEY_VALUE_HEADS * HEAD_SIZE), MODEL_WIDTH ** -0.5, 0.125, ((1, 4),))
    out_weight = bell_draw(key_list[8], (QUERY_HEADS * HEAD_SIZE, MODEL_WIDTH), (QUERY_HEADS * HEAD_SIZE) ** -0.5, 0.1875, ((1, 4),))
    sink_head_logit = jnp.clip(5.0 + 2.5 * jax.random.uniform(key_list[9], (QUERY_HEADS,), jnp.float32) ** block_scale(key_list[9], (QUERY_HEADS,), ((0, 4),), -0.2, 0.2), 5.0, 7.5)
    prefix_logit_bias = jnp.clip(-2.5 + 1.5 * jax.random.uniform(key_list[10], (QUERY_HEADS,), jnp.float32) ** block_scale(key_list[10], (QUERY_HEADS,), ((0, 4),), -0.2, 0.2), -2.5, -1.0)
    return {"latent": latent, "conditioning": conditioning, "context_cond": context_cond, "modulation": modulation, "context": context, "query_weight": query_weight, "key_projection": key_projection, "value_projection": value_projection, "out_weight": out_weight, "sink_head_logit": sink_head_logit, "prefix_logit_bias": prefix_logit_bias}


NORM_EPSILON = 1e-06
ROTARY_BASE = 10000.0
MASKED = -1e+30

def layer_norm(tok_rows):
    vectors = tok_rows.astype(jnp.float32)
    centre = lax.optimization_barrier(jnp.mean(vectors, axis=-1, keepdims=True))
    spread = lax.optimization_barrier(jnp.mean(jnp.square(vectors - centre), axis=-1, keepdims=True))
    return (vectors - centre) * lax.rsqrt(spread + NORM_EPSILON)

def turn_half(segment, token_positions):
    half_width = segment.shape[-1]
    quarter = half_width // 2
    frequency = ROTARY_BASE ** (-jnp.arange(0, half_width, 2, dtype=jnp.float32) / half_width)
    angles = token_positions.astype(jnp.float32)[:, None] * frequency[None, :]
    cosine = jnp.cos(angles)[:, None, :]
    sine_table = jnp.sin(angles)[:, None, :]
    leading = segment[..., :quarter]
    trailing = segment[..., quarter:]
    return jnp.concatenate([leading * cosine - trailing * sine_table, trailing * cosine + leading * sine_table], axis=-1)

def apply_rotary(head_rows, token_positions):
    half_width = head_rows.shape[-1] // 2
    return jnp.concatenate([turn_half(head_rows[..., :half_width], token_positions // GRID_W), turn_half(head_rows[..., half_width:], token_positions % GRID_W)], axis=-1)

def rounded_length(array):
    return lax.optimization_barrier(array.astype(jnp.bfloat16))

def reference(latent, conditioning, context_cond, modulation, context, query_weight, key_projection, value_projection, out_weight, sink_head_logit, prefix_logit_bias):
    cond_rows = jnp.concatenate([conditioning, context_cond[None, :]], axis=0)
    activated = jax.nn.silu(cond_rows.astype(jnp.float32)).astype(jnp.bfloat16)
    mod_all = jnp.stack([jnp.dot(activated, modulation[index], preferred_element_type=jnp.float32) for index in range(3)])
    ctx_shift = mod_all[0, -1]
    ctx_scale = mod_all[1, -1]
    heads_per_group = QUERY_HEADS // KEY_VALUE_HEADS
    block_list = LATENT_TOKENS // WINDOW_REACH
    factor = HEAD_SIZE ** (-0.5)
    token_positions = jnp.arange(LATENT_TOKENS, dtype=jnp.int32)
    block_start = jnp.arange(block_list, dtype=jnp.int32)[:, None] * WINDOW_REACH
    query_pos = block_start + jnp.arange(WINDOW_REACH, dtype=jnp.int32)[None, :]
    key_pos = block_start - WINDOW_REACH + jnp.arange(3 * WINDOW_REACH, dtype=jnp.int32)[None, :]
    inside = (key_pos >= 0) & (key_pos < LATENT_TOKENS)
    valid = (jnp.abs(query_pos[:, :, None] - key_pos[:, None, :]) <= WINDOW_REACH) & inside[:, None, :]
    head_bias_rows = prefix_logit_bias.astype(jnp.float32).reshape(KEY_VALUE_HEADS, heads_per_group)[:, :, None, None]
    sink_head_rows = sink_head_logit.astype(jnp.float32).reshape(KEY_VALUE_HEADS, heads_per_group)[:, :, None, None]

    def one_sample(operands):
        sample_rows, sample_ctx, mod_shift, mod_scale, mod_gate = operands
        normalized_input = (layer_norm(sample_rows) * (1.0 + mod_scale) + mod_shift).astype(jnp.bfloat16)
        ctx_normed = (layer_norm(sample_ctx) * (1.0 + ctx_scale) + ctx_shift).astype(jnp.bfloat16)
        query_rows = rounded_length(apply_rotary(jnp.dot(normalized_input, query_weight, preferred_element_type=jnp.float32).reshape(LATENT_TOKENS, QUERY_HEADS, HEAD_SIZE), token_positions))
        key_token_rows = rounded_length(apply_rotary(jnp.dot(normalized_input, key_projection, preferred_element_type=jnp.float32).reshape(LATENT_TOKENS, KEY_VALUE_HEADS, HEAD_SIZE), token_positions))
        value_token_rows = rounded_length(jnp.dot(normalized_input, value_projection, preferred_element_type=jnp.float32)).reshape(LATENT_TOKENS, KEY_VALUE_HEADS, HEAD_SIZE)
        prefix_keys = rounded_length(jnp.dot(ctx_normed, key_projection, preferred_element_type=jnp.float32))
        prefix_keys = prefix_keys.reshape(CONTEXT_TOKENS, KEY_VALUE_HEADS, HEAD_SIZE).astype(jnp.float32)
        prefix_values = rounded_length(jnp.dot(ctx_normed, value_projection, preferred_element_type=jnp.float32))
        prefix_values = prefix_values.reshape(CONTEXT_TOKENS, KEY_VALUE_HEADS, HEAD_SIZE).astype(jnp.float32)
        padding_amount = ((WINDOW_REACH, WINDOW_REACH), (0, 0), (0, 0))
        key_padded_rows = jnp.pad(key_token_rows, padding_amount).reshape(block_list + 2, WINDOW_REACH, KEY_VALUE_HEADS, HEAD_SIZE)
        value_padded_rows = jnp.pad(value_token_rows, padding_amount).reshape(block_list + 2, WINDOW_REACH, KEY_VALUE_HEADS, HEAD_SIZE)
        window_keys = jnp.concatenate([key_padded_rows[:-2], key_padded_rows[1:-1], key_padded_rows[2:]], axis=1).astype(jnp.float32)
        window_values = jnp.concatenate([value_padded_rows[:-2], value_padded_rows[1:-1], value_padded_rows[2:]], axis=1).astype(jnp.float32)
        query_block_list = query_rows.reshape(block_list, WINDOW_REACH, KEY_VALUE_HEADS, heads_per_group, HEAD_SIZE).astype(jnp.float32)

        def one_block(pieces):
            block_queries, block_keys, block_values, block_valid = pieces
            win_scores = jnp.einsum('qkgd,jkd->kgqj', block_queries, block_keys) * factor
            win_scores = jnp.where(block_valid[None, None], win_scores, MASKED)
            ctx_scores = jnp.einsum('qkgd,ckd->kgqc', block_queries, prefix_keys) * factor + head_bias_rows
            sink_scores = jnp.broadcast_to(sink_head_rows, win_scores.shape[:-1] + (1,))
            probs = jax.nn.softmax(jnp.concatenate([win_scores, ctx_scores, sink_scores], axis=-1), axis=-1)
            win_probs = rounded_length(probs[..., :3 * WINDOW_REACH]).astype(jnp.float32)
            ctx_probs = rounded_length(probs[..., 3 * WINDOW_REACH:3 * WINDOW_REACH + CONTEXT_TOKENS]).astype(jnp.float32)
            summed = jnp.einsum('kgqj,jkd->qkgd', win_probs, block_values) + jnp.einsum('kgqc,ckd->qkgd', ctx_probs, prefix_values)
            return summed.astype(jnp.bfloat16)
        attended = lax.map(one_block, (query_block_list, window_keys, window_values, valid))
        attended = attended.reshape(LATENT_TOKENS, QUERY_HEADS * HEAD_SIZE)
        mixed = jnp.dot(attended, out_weight, preferred_element_type=jnp.float32)
        return sample_rows.astype(jnp.float32) + mod_gate * mixed
    return lax.map(one_sample, (latent, context, mod_all[0, :-1], mod_all[1, :-1], mod_all[2, :-1]))
```

```python
import functools

import jax
import jax.numpy as jnp
import numpy as np
from jax import lax
from jax.experimental import pallas as pl
from jax.experimental.pallas import tpu as pltpu
from jax.sharding import PartitionSpec as P

HEAD_SIZE = 64
GRID_W = 64
WINDOW_REACH = 128
NORM_EPSILON = 1e-06
ROTARY_BASE = 10000.0
MASKED = -1e30
LANES = 128
MESH = pl.DeviceIdType.MESH
F32 = jnp.float32
BF16 = jnp.bfloat16


def rotary_tables(grid_rows):
    half = HEAD_SIZE // 2
    quarter = half // 2
    lane = np.arange(LANES) % HEAD_SIZE
    frequency = ROTARY_BASE ** (-2.0 * (lane % quarter) / half)
    frequency = frequency.astype(np.float32).astype(np.float64)
    sign = np.where(lane % half < quarter, -1.0, 1.0)
    by_row = lane < half

    def tables(count, keep):
        angles = np.arange(count)[:, None] * frequency[None, :]
        cosine = np.where(keep[None, :], np.cos(angles), 0.0)
        sine = np.where(keep[None, :], np.sin(angles) * sign[None, :], 0.0)
        return np.stack([cosine, sine]).astype(np.float32)

    return tables(grid_rows, by_row), tables(GRID_W, ~by_row)


def block_kernel(
    dims,
    lat_hbm, cond_hbm, cctx_hbm, mod_hbm, ctx_hbm, qw_hbm, kw_hbm, vw_hbm, ow_hbm,
    sink_hbm, bias_hbm, rowt_hbm, colt_hbm,
    outv,
    lat, cond, cctx, mod, ctx, qw, ow, sink, bias, rowt, colt,
    act, pack, packs, total, sendb, slots, modv,
    xn, xnc, nrm, nrmc, kvw, cosv, sinv, kvb, cxb, ke, ko, ve, vo, q, att,
    in_sem, a_s, a_r, b_s, b_r, h_s, h_r, c_s, c_r, g_s, g_r,
):
    n_sp, n_tp, n_dp, samples = dims
    sp, tp, dp = lax.axis_index("sp"), lax.axis_index("tp"), lax.axis_index("dp")
    n_td = n_tp * n_dp
    me = tp * n_dp + dp
    tok, width = lat.shape
    cols = mod.shape[2]
    n_ctx = ctx.shape[0]
    reach = WINDOW_REACH
    blocks = tok // reach
    q_width = qw.shape[1]
    pairs = q_width // LANES

    barrier = pltpu.get_barrier_semaphore()
    for o in range(1, n_sp):
        pl.semaphore_signal(
            barrier, inc=1, device_id={"sp": lax.rem(sp + o, n_sp)}, device_id_type=MESH
        )

    def td_peer(o):
        lin = lax.rem(me + o, n_td)
        return lin // n_dp, lax.rem(lin, n_dp)

    for o in range(1, n_td):
        t, d = td_peer(o)
        pl.semaphore_signal(barrier, inc=1, device_id={"tp": t, "dp": d}, device_id_type=MESH)

    pairs_in = [
        (cond_hbm, cond), (cctx_hbm, cctx), (mod_hbm, mod), (ctx_hbm, ctx), (lat_hbm, lat),
        (kw_hbm, kvw.at[pl.ds(0, HEAD_SIZE)]), (vw_hbm, kvw.at[pl.ds(HEAD_SIZE, HEAD_SIZE)]), (rowt_hbm, rowt), (colt_hbm, colt), (qw_hbm, qw),
        (sink_hbm, sink), (bias_hbm, bias), (ow_hbm, ow),
    ]
    loads = [
        pltpu.make_async_copy(src, dst, in_sem.at[i]) for i, (src, dst) in enumerate(pairs_in)
    ]
    for load in loads:
        load.start()

    act[...] = jnp.zeros_like(act)
    loads[0].wait()
    loads[1].wait()
    act[0:samples, :] = cond[...].astype(F32)
    act[samples : samples + 1, :] = cctx[...].astype(F32).reshape(1, cctx.shape[0])
    v = act[...]
    activated = (v / (1.0 + jnp.exp(-v))).astype(BF16)
    pack[...] = jnp.zeros_like(pack)
    loads[2].wait()
    n_rows = samples + 1
    for m in range(3):
        count = n_rows if m < 2 else samples
        part = jnp.dot(activated, mod[m], preferred_element_type=F32)
        pack[m * n_rows : m * n_rows + count, :] = part[0:count, :]

    pl.semaphore_wait(barrier, n_sp - 1 + n_td - 1)
    a_copies = []
    for o in range(1, n_sp):
        copy = pltpu.make_async_remote_copy(
            src_ref=pack, dst_ref=packs.at[o - 1], send_sem=a_s.at[o - 1], recv_sem=a_r.at[o - 1],
            device_id={"sp": lax.rem(sp + o, n_sp)}, device_id_type=MESH,
        )
        copy.start()
        a_copies.append(copy)

    step = 16
    chunk = 64

    def normalise(src, dst, first, last):
        def body(i, carry):
            rows = pl.ds(pl.multiple_of(i * chunk, chunk), chunk)
            x = src[rows, :].astype(F32)
            x = x - jnp.mean(x, axis=-1, keepdims=True)
            spread = jnp.mean(x * x, axis=-1, keepdims=True)
            dst[rows, :] = x * lax.rsqrt(spread + NORM_EPSILON)
            return carry

        lax.fori_loop(first, last, body, 0)

    loads[3].wait()
    normalise(ctx, xnc, 0, n_ctx // chunk)
    loads[4].wait()
    middle = tok // chunk // 3
    normalise(lat, xn, 0, middle)

    for copy in a_copies:
        copy.wait_recv()
    summed = pack[...]
    for o in range(1, n_sp):
        summed = summed + packs[o - 1]
    total[...] = summed
    for d in range(n_dp):
        for row, source in enumerate(
            (d, n_rows + d, 2 * n_rows + d, samples, n_rows + samples)
        ):
            sendb[d, row : row + 1, :] = total[source : source + 1, :]
        sendb[d, 5:8, :] = jnp.zeros((3, cols), F32)
    b_copies = []
    for o in range(1, n_td):
        t, d = td_peer(o)
        copy = pltpu.make_async_remote_copy(
            src_ref=sendb.at[d], dst_ref=slots.at[me], send_sem=b_s.at[o - 1],
            recv_sem=b_r.at[o - 1], device_id={"tp": t, "dp": d}, device_id_type=MESH,
        )
        copy.start()
        b_copies.append(copy)
    slots[me] = sendb[dp]

    normalise(lat, xn, middle, tok // chunk)
    loads[5].wait()
    loads[6].wait()
    loads[7].wait()
    loads[8].wait()
    groups = tok // GRID_W
    for g in range(groups):
        row = pl.ds(sp * groups + g, 1)
        span = slice(g * GRID_W, (g + 1) * GRID_W)
        cosv[span, :] = rowt[0, row, :] + colt[0]
        sinv[span, :] = rowt[1, row, :] + colt[1]
    loads[9].wait()
    loads[10].wait()
    loads[11].wait()

    for copy in b_copies:
        copy.wait_recv()
    for j in range(n_td):
        modv[:, j * cols : (j + 1) * cols] = slots[j]

    def condition(src, dst, count, shift_row, scale_row):
        def body(i, carry):
            rows = pl.ds(pl.multiple_of(i * step, step), step)
            scale = 1.0 + modv[scale_row : scale_row + 1, :]
            dst[rows, :] = (src[rows, :] * scale + modv[shift_row : shift_row + 1, :]).astype(BF16)
            return carry

        lax.fori_loop(0, count // step, body, 0)

    condition(xnc, nrmc, n_ctx, 3, 4)
    nt = (((1,), (1,)), ((), ()))
    cxb[0] = lax.dot_general(nrmc[...], kvw[...], nt, preferred_element_type=F32).astype(BF16)
    c_copies = []
    for o in range(1, n_sp):
        copy = pltpu.make_async_remote_copy(
            src_ref=cxb.at[0], dst_ref=cxb.at[o], send_sem=c_s.at[o - 1], recv_sem=c_r.at[o - 1],
            device_id={"sp": lax.rem(sp + o, n_sp)}, device_id_type=MESH,
        )
        copy.start()
        c_copies.append(copy)

    half = HEAD_SIZE // 2
    quarter = half // 2

    def turn(u, cosine, sine):
        w = u.shape[1]
        lane = lax.broadcasted_iota(jnp.int32, u.shape, 1)
        first = lax.rem(lane, half) < quarter
        swapped = jnp.where(first, pltpu.roll(u, w - quarter, 1), pltpu.roll(u, quarter, 1))
        return u * cosine + swapped * sine

    condition(xn, nrm, tok, 0, 1)
    u = lax.dot_general(nrm[...], kvw[...], nt, preferred_element_type=F32)
    key_lane = lax.broadcasted_iota(jnp.int32, u.shape, 1) < HEAD_SIZE
    kv_rows = jnp.where(key_lane, turn(u, cosv[...], sinv[...]), u)
    kvb[reach : reach + tok, :] = kv_rows.astype(BF16)

    up = pltpu.make_async_remote_copy(
        src_ref=kvb.at[pl.ds(tok, reach)], dst_ref=kvb.at[pl.ds(0, reach)],
        send_sem=h_s.at[0], recv_sem=h_r.at[0],
        device_id={"sp": lax.rem(sp + 1, n_sp)}, device_id_type=MESH,
    )
    down = pltpu.make_async_remote_copy(
        src_ref=kvb.at[pl.ds(reach, reach)], dst_ref=kvb.at[pl.ds(reach + tok, reach)],
        send_sem=h_s.at[1], recv_sem=h_r.at[1],
        device_id={"sp": lax.rem(sp + n_sp - 1, n_sp)}, device_id_type=MESH,
    )

    @pl.when(sp < n_sp - 1)
    def _():
        up.start()

    @pl.when(sp > 0)
    def _():
        down.start()

    factor = HEAD_SIZE ** (-0.5)
    u = jnp.dot(nrm[...], qw[...], preferred_element_type=F32)
    for p in range(pairs):
        span = slice(p * LANES, (p + 1) * LANES)
        q[:, span] = (turn(u[:, span], cosv[...], sinv[...]) * factor).astype(BF16)

    def expand(rows, at):
        x = rows.astype(F32)
        low = lax.broadcasted_iota(jnp.int32, x.shape, 1) < HEAD_SIZE
        keys = jnp.where(low, x, 0.0)
        vals = jnp.where(low, 0.0, x)
        span = slice(at, at + x.shape[0])
        ke[span, :] = keys.astype(BF16)
        ko[span, :] = pltpu.roll(keys, HEAD_SIZE, 1).astype(BF16)
        vo[span, :] = vals.astype(BF16)
        ve[span, :] = pltpu.roll(vals, HEAD_SIZE, 1).astype(BF16)

    window = tok + 2 * reach
    expand(kvb[reach : reach + tok, :], reach)
    expand(cxb[0], window)
    for o in range(1, n_sp):
        c_copies[o - 1].wait_recv()
        expand(cxb[o], window + o * n_ctx)

    m_rows = pairs * reach
    row = lax.broadcasted_iota(jnp.int32, (m_rows, 1), 0)

    def per_head(ref, parity):
        column = jnp.full((m_rows, 1), ref[parity], F32)
        for p in range(1, pairs):
            column = jnp.where(row >= p * reach, ref[2 * p + parity], column)
        return column

    n_all_ctx = n_sp * n_ctx
    delta = lax.broadcasted_iota(jnp.int32, (m_rows, reach), 1) - lax.rem(
        lax.broadcasted_iota(jnp.int32, (m_rows, reach), 0), reach
    )
    far = 4 * reach
    low_edge = jnp.where(sp == 0, far, 0)
    high_edge = jnp.where(sp == n_sp - 1, -far, 0)
    g_copies = {}
    relayed = n_tp == 4
    direct = (1, 2) if relayed else range(1, n_tp)

    def partner(o):
        if not relayed:
            return lax.rem(tp + o, n_tp)
        x, y = lax.rem(tp, 2), tp // 2
        x = 1 - x if o % 2 else x
        y = 1 - y if o // 2 else y
        return 2 * y + x

    def owner(o):
        return partner(o) if relayed else lax.rem(tp + n_tp - o, n_tp)


    def attend(b):
        rows = slice(b * reach, (b + 1) * reach)
        q2 = jnp.concatenate(
            [q[rows, p * LANES : (p + 1) * LANES] for p in range(pairs)], axis=0
        )
        before_ok = delta >= (low_edge if b == 0 else 0)
        after_ok = delta <= (high_edge if b == blocks - 1 else 0)
        win = slice(b * reach, (b + 3) * reach)
        pre = slice(window, window + n_all_ctx)
        result = jnp.zeros((m_rows, LANES), F32)
        for parity, k_ref, v_ref in ((0, ke, ve), (1, ko, vo)):
            sw = lax.dot_general(q2, k_ref[win, :], nt, preferred_element_type=F32)
            s0 = jnp.where(before_ok, sw[:, 0:reach], MASKED)
            s1 = sw[:, reach : 2 * reach]
            s2 = jnp.where(after_ok, sw[:, 2 * reach : 3 * reach], MASKED)
            sc = lax.dot_general(q2, k_ref[pre, :], nt, preferred_element_type=F32)
            sc = sc + per_head(bias, parity)
            sunk = per_head(sink, parity)
            top = jnp.maximum(jnp.maximum(s0, s1), s2)
            for c in range(n_all_ctx // LANES):
                top = jnp.maximum(top, sc[:, c * LANES : (c + 1) * LANES])
            highest = jnp.maximum(jnp.max(top, axis=-1, keepdims=True), sunk)
            e0, e1, e2 = jnp.exp(s0 - highest), jnp.exp(s1 - highest), jnp.exp(s2 - highest)
            ec = jnp.exp(sc - highest)
            mass = e0 + e1 + e2
            for c in range(n_all_ctx // LANES):
                mass = mass + ec[:, c * LANES : (c + 1) * LANES]
            denominator = jnp.sum(mass, axis=-1, keepdims=True) + jnp.exp(sunk - highest)
            ew = jnp.concatenate([e0, e1, e2], axis=1).astype(BF16)
            weighed = jnp.dot(ew, v_ref[win, :], preferred_element_type=F32)
            weighed = weighed + jnp.dot(ec.astype(BF16), v_ref[pre, :], preferred_element_type=F32)
            result = result + weighed / denominator
        for p in range(pairs):
            att[0, b, :, p * LANES : (p + 1) * LANES] = result[
                p * reach : (p + 1) * reach, :
            ].astype(BF16)
        for o in direct:
            copy = pltpu.make_async_remote_copy(
                src_ref=att.at[0, b], dst_ref=att.at[o, b], send_sem=g_s.at[b, o - 1],
                recv_sem=g_r.at[b, o - 1], device_id={"tp": partner(o)}, device_id_type=MESH,
            )
            copy.start()
            g_copies[b, o] = copy

    def forward(b):
        for o in direct:
            g_copies[b, o].wait_recv()
            part = pl.ds((o - 1) * (reach // 2), reach // 2)
            copy = pltpu.make_async_remote_copy(
                src_ref=att.at[o, b, part], dst_ref=att.at[3, b, part],
                send_sem=g_s.at[b, 1 + o], recv_sem=g_r.at[b, 1 + o],
                device_id={"tp": partner(3 - o)}, device_id_type=MESH,
            )
            copy.start()
            g_copies[b, 2 + o] = copy

    order = list(range(1, blocks - 1)) + ([0, blocks - 1] if blocks > 1 else [0])
    for b in order:
        if b == 0:
            @pl.when(sp > 0)
            def _():
                up.wait_recv()

            @pl.when(sp == 0)
            def _():
                kvb[0:reach, :] = jnp.zeros((reach, LANES), BF16)

            expand(kvb[0:reach, :], 0)
        if b == blocks - 1:
            @pl.when(sp < n_sp - 1)
            def _():
                down.wait_recv()

            @pl.when(sp == n_sp - 1)
            def _():
                kvb[reach + tok : window, :] = jnp.zeros((reach, LANES), BF16)

            expand(kvb[reach + tok : window, :], reach + tok)
        attend(b)

    loads[12].wait()
    out_cols = ow.shape[1]
    mine = pl.ds(pl.multiple_of(tp * out_cols, out_cols), out_cols)
    gate = modv[2:3, mine]

    def project(b, o):
        w = ow[pl.ds(pl.multiple_of(owner(o) * q_width, q_width), q_width), :]
        return jnp.dot(att[o, b], w, preferred_element_type=F32)

    for b in order:
        if relayed:
            forward(b)
        outv[b * reach : (b + 1) * reach, :] = project(b, 0)
    for b in order:
        rows = slice(b * reach, (b + 1) * reach)
        mixed = outv[rows, :]
        for o in range(1, n_tp):
            if not relayed:
                g_copies[b, o].wait_recv()
            elif o == 3:
                g_copies[b, 3].wait_recv()
                g_copies[b, 4].wait_recv()
            mixed = mixed + project(b, o)
        outv[rows, :] = lat[rows, mine].astype(F32) + gate * mixed

    for copy in a_copies + b_copies + c_copies + list(g_copies.values()):
        copy.wait_send()

    @pl.when(sp < n_sp - 1)
    def _():
        up.wait_send()

    @pl.when(sp > 0)
    def _():
        down.wait_send()


def per_device(
    latent, conditioning, context_cond, modulation, context, query_weight, key_projection,
    value_projection, out_weight, sink_head_logit, prefix_logit_bias,
):
    n_sp, n_tp, n_dp = lax.axis_size("sp"), lax.axis_size("tp"), lax.axis_size("dp")
    samples = conditioning.shape[0]
    _, tok, width = latent.shape
    n_ctx = context.shape[1]
    depth, cols = modulation.shape[1:]
    q_width = query_weight.shape[1]
    heads = q_width // HEAD_SIZE
    out_cols = out_weight.shape[1]
    blocks = tok // WINDOW_REACH
    window = tok + 2 * WINDOW_REACH
    keys = window + n_sp * n_ctx
    n_td = n_tp * n_dp
    act_rows = -(-(samples + 1) // 8) * 8
    pack_rows = -(-(3 * samples + 2) // 8) * 8
    row_table, col_table = rotary_tables(n_sp * tok // GRID_W)
    vm = pltpu.VMEM
    dma = pltpu.SemaphoreType.DMA
    scratch = [
        vm((tok, width), BF16), vm((samples, depth), BF16), vm((depth,), BF16),
        vm((3, depth, cols), BF16), vm((n_ctx, width), BF16), vm((width, q_width), BF16),
        vm(out_weight.shape, BF16), pltpu.SMEM((heads,), F32), pltpu.SMEM((heads,), F32),
        vm(row_table.shape, F32), vm(col_table.shape, F32),
        vm((act_rows, depth), F32), vm((pack_rows, cols), F32),
        vm((n_sp - 1, pack_rows, cols), F32), vm((pack_rows, cols), F32),
        vm((n_dp, 8, cols), F32), vm((n_td, 8, cols), F32), vm((8, width), F32),
        vm((tok, width), F32), vm((n_ctx, width), F32), vm((tok, width), BF16),
        vm((n_ctx, width), BF16), vm((LANES, width), BF16), vm((tok, LANES), F32),
        vm((tok, LANES), F32), vm((window, LANES), BF16), vm((n_sp, n_ctx, LANES), BF16),
        vm((keys, LANES), BF16), vm((keys, LANES), BF16), vm((keys, LANES), BF16),
        vm((keys, LANES), BF16), vm((tok, q_width), BF16),
        vm((n_tp, blocks, WINDOW_REACH, q_width), BF16),
        dma((13,)), dma((n_sp - 1,)), dma((n_sp - 1,)), dma((n_td - 1,)),
        dma((n_td - 1,)), dma((2,)), dma((2,)), dma((n_sp - 1,)), dma((n_sp - 1,)),
        dma((blocks, n_tp)), dma((blocks, n_tp)),
    ]
    anywhere = pl.BlockSpec(memory_space=pl.ANY)
    stays = pl.BlockSpec(memory_space=pltpu.HBM)
    out = pl.pallas_call(
        functools.partial(block_kernel, (n_sp, n_tp, n_dp, samples)),
        out_shape=pltpu.VMEM((tok, out_cols), F32),
        in_specs=[stays] * 13,
        out_specs=pl.BlockSpec(memory_space=pltpu.VMEM),
        scratch_shapes=scratch,
        compiler_params=pltpu.CompilerParams(
            collective_id=0, has_side_effects=True, vmem_limit_bytes=66000000
        ),
        name="fused_block",
    )(
        latent[0], conditioning, context_cond, modulation, context[0], query_weight,
        key_projection.T, value_projection.T, out_weight, sink_head_logit, prefix_logit_bias,
        jnp.asarray(row_table), jnp.asarray(col_table),
    )
    return out[None]


def solution(mesh):
    placed = (
        P("dp", "sp", None),
        P(None, "sp"),
        P("sp"),
        P(None, "sp", ("tp", "dp")),
        P("dp", "sp", None),
        P(None, "tp"),
        P(None, "tp"),
        P(None, "tp"),
        P(None, "tp"),
        P("tp"),
        P("tp"),
    )
    return jax.shard_map(
        per_device, mesh=mesh, in_specs=placed, out_specs=P("dp", "sp", "tp"), check_vma=False
    )
```

```python
import functools

import jax
import jax.numpy as jnp
import numpy as np
from jax import lax
from jax.experimental import pallas as pl
from jax.experimental.pallas import tpu as pltpu
from jax.sharding import PartitionSpec as P

HEAD_SIZE = 64
GRID_W = 64
WINDOW_REACH = 128
NORM_EPSILON = 1e-06
ROTARY_BASE = 10000.0
MASKED = -1e30
LANES = 128
MESH = pl.DeviceIdType.MESH
F32 = jnp.float32
BF16 = jnp.bfloat16


def rotary_tables(grid_rows):
    half = HEAD_SIZE // 2
    quarter = half // 2
    lane = np.arange(LANES) % HEAD_SIZE
    frequency = ROTARY_BASE ** (-2.0 * (lane % quarter) / half)
    frequency = frequency.astype(np.float32).astype(np.float64)
    sign = np.where(lane % half < quarter, -1.0, 1.0)
    by_row = lane < half

    def tables(count, keep):
        angles = np.arange(count)[:, None] * frequency[None, :]
        cosine = np.where(keep[None, :], np.cos(angles), 0.0)
        sine = np.where(keep[None, :], np.sin(angles) * sign[None, :], 0.0)
        return np.stack([cosine, sine]).astype(np.float32)

    return tables(grid_rows, by_row), tables(GRID_W, ~by_row)


def block_kernel(
    dims,
    lat_hbm, cond_hbm, cctx_hbm, mod_hbm, ctx_hbm, qw_hbm, kw_hbm, vw_hbm, ow_hbm,
    sink_hbm, bias_hbm, rowt_hbm, colt_hbm,
    outv,
    lat, cond, cctx, mod, ctx, wall, ow, sink, bias, rowt, colt,
    act, packf, pack, packs, total, sendb, slots, modv,
    xn, xnc, nrm, nrmc, kvw, cosv, sinv, acc, accc, kvb, cxb, kd, vd, q4, att,
    in_sem, a_s, a_r, b_s, b_r, h_s, h_r, c_s, c_r, g_s, g_r,
):
    n_sp, n_tp, n_dp, samples = dims
    sp, tp, dp = lax.axis_index("sp"), lax.axis_index("tp"), lax.axis_index("dp")
    n_td = n_tp * n_dp
    me = tp * n_dp + dp
    tok, width = lat.shape
    cols = mod.shape[2]
    group = n_dp * cols
    n_ctx = ctx.shape[0]
    reach = WINDOW_REACH
    blocks = tok // reach
    q_width = wall.shape[1] - LANES
    pairs = q_width // LANES
    heads = 2 * pairs

    barrier = pltpu.get_barrier_semaphore()
    for o in range(1, n_sp):
        pl.semaphore_signal(
            barrier, inc=1, device_id={"sp": lax.rem(sp + o, n_sp)}, device_id_type=MESH
        )
    for o in range(1, n_td):
        lin = lax.rem(me + o, n_td)
        pl.semaphore_signal(
            barrier, inc=1, device_id={"tp": lin // n_dp, "dp": lax.rem(lin, n_dp)},
            device_id_type=MESH,
        )

    relayed = n_tp == 4
    direct = (1, 2) if relayed else range(1, n_tp)

    def partner(o):
        if not relayed:
            return lax.rem(tp + o, n_tp)
        x, y = lax.rem(tp, 2), tp // 2
        x = 1 - x if o % 2 else x
        y = 1 - y if o // 2 else y
        return 2 * y + x

    def owner(o):
        return partner(o) if relayed else lax.rem(tp + n_tp - o, n_tp)

    pairs_in = [
        (cond_hbm, cond), (cctx_hbm, cctx), (mod_hbm.at[0], mod.at[0]), (mod_hbm.at[1], mod.at[1]),
        (mod_hbm.at[2], mod.at[2]), (ctx_hbm, ctx), (lat_hbm, lat),
        (kw_hbm, kvw.at[pl.ds(0, HEAD_SIZE)]), (vw_hbm, kvw.at[pl.ds(HEAD_SIZE, HEAD_SIZE)]),
        (rowt_hbm, rowt), (colt_hbm, colt), (qw_hbm, wall.at[:, pl.ds(0, q_width)]),
        (sink_hbm, sink), (bias_hbm, bias), (ow_hbm, ow),
    ]
    loads = [
        pltpu.make_async_copy(src, dst, in_sem.at[i]) for i, (src, dst) in enumerate(pairs_in)
    ]
    for load in loads[:6]:
        load.start()

    act[...] = jnp.zeros_like(act)
    loads[0].wait()
    loads[1].wait()
    for load in loads[6:]:
        load.start()
    act[0:samples, :] = cond[...].astype(F32)
    act[samples : samples + 1, :] = cctx[...].astype(F32).reshape(1, cctx.shape[0])
    v = act[...]
    activated = (v / (1.0 + jnp.exp(-v))).astype(BF16)
    packf[...] = jnp.zeros_like(packf)
    n_rows = samples + 1
    for m in range(3):
        loads[2 + m].wait()
        count = n_rows if m < 2 else samples
        part = jnp.dot(activated, mod[m], preferred_element_type=F32)
        packf[m * n_rows : m * n_rows + count, :] = part[0:count, :]
    pack[...] = packf[...].astype(BF16)

    pl.semaphore_wait(barrier, n_sp - 1 + n_td - 1)
    a_copies = []
    for o in range(1, n_sp):
        copy = pltpu.make_async_remote_copy(
            src_ref=pack, dst_ref=packs.at[o - 1], send_sem=a_s.at[o - 1], recv_sem=a_r.at[o - 1],
            device_id={"sp": lax.rem(sp + o, n_sp)}, device_id_type=MESH,
        )
        copy.start()
        a_copies.append(copy)

    chunk = 64

    def normalise(src, dst, first, last):
        def body(i, carry):
            rows = pl.ds(pl.multiple_of(i * chunk, chunk), chunk)
            x = src[rows, :].astype(F32)
            x = x - jnp.mean(x, axis=-1, keepdims=True)
            spread = jnp.mean(x * x, axis=-1, keepdims=True)
            x = x * lax.rsqrt(spread + NORM_EPSILON)
            for t in range(n_tp):
                dst[t, rows, :] = x[:, t * group : (t + 1) * group]
            return carry

        lax.fori_loop(first, last, body, 0)

    loads[5].wait()
    normalise(ctx, xnc, 0, n_ctx // chunk)
    loads[6].wait()
    normalise(lat, xn, 0, tok // chunk)

    for copy in a_copies:
        copy.wait_recv()
    summed = packf[...]
    for o in range(1, n_sp):
        summed = summed + packs[o - 1].astype(F32)
    total[...] = summed
    for d in range(n_dp):
        rows = [
            total[source : source + 1, :]
            for source in (d, n_rows + d, 2 * n_rows + d, samples, n_rows + samples)
        ]
        rows.append(jnp.zeros((3, cols), F32))
        sendb[d] = jnp.concatenate(rows, axis=0).astype(BF16)
    b_copies = {}
    for o in range(n_tp):
        for e in range(n_dp):
            if o == 0 and e == 0:
                continue
            d = lax.rem(dp + e, n_dp)
            copy = pltpu.make_async_remote_copy(
                src_ref=sendb.at[d], dst_ref=slots.at[o * n_dp + dp],
                send_sem=b_s.at[o * n_dp + e], recv_sem=b_r.at[o * n_dp + e],
                device_id={"tp": partner(o), "dp": d}, device_id_type=MESH,
            )
            copy.start()
            b_copies[o, e] = copy
    slots[dp] = sendb[dp]

    for load in loads[7:14]:
        load.wait()
    groups = tok // GRID_W
    for g in range(groups):
        row = pl.ds(sp * groups + g, 1)
        span = slice(g * GRID_W, (g + 1) * GRID_W)
        cosv[span, :] = rowt[0, row, :] + colt[0]
        sinv[span, :] = rowt[1, row, :] + colt[1]
    for j in range(width // LANES):
        span = slice(j * LANES, (j + 1) * LANES)
        wall[span, q_width:] = kvw[:, span].astype(F32).T.astype(BF16)

    def condition(src, dst, count, o, g, shift_row, scale_row):
        scale = 1.0 + modv[o, scale_row : scale_row + 1, :]
        shift = modv[o, shift_row : shift_row + 1, :]
        for i in range(0, count, chunk):
            rows = slice(i, i + chunk)
            dst[rows, :] = (src[g, rows, :] * scale + shift).astype(BF16)

    c_copies = []
    for o in range(n_tp):
        for e in range(n_dp):
            if o or e:
                b_copies[o, e].wait_recv()
        for d in range(n_dp):
            modv[o, :, d * cols : (d + 1) * cols] = slots[o * n_dp + d].astype(F32)
        g = owner(o)
        weight_rows = pl.ds(pl.multiple_of(g * group, group), group)
        condition(xnc, nrmc, n_ctx, o, g, 3, 4)
        u = jnp.dot(nrmc[...], wall[weight_rows, q_width:], preferred_element_type=F32)
        if o:
            u = accc[...] + u
        if o < n_tp - 1:
            accc[...] = u
        else:
            cxb[0] = u.astype(BF16)
            for r in range(1, n_sp):
                copy = pltpu.make_async_remote_copy(
                    src_ref=cxb.at[0], dst_ref=cxb.at[r], send_sem=c_s.at[r - 1],
                    recv_sem=c_r.at[r - 1], device_id={"sp": lax.rem(sp + r, n_sp)},
                    device_id_type=MESH,
                )
                copy.start()
                c_copies.append(copy)
        condition(xn, nrm, tok, o, g, 0, 1)
        u = jnp.dot(nrm[...], wall[weight_rows, :], preferred_element_type=F32)
        if o:
            u = acc[...] + u
        acc[...] = u

    half = HEAD_SIZE // 2
    quarter = half // 2

    def turn(u, cosine, sine):
        w = u.shape[1]
        lane = lax.broadcasted_iota(jnp.int32, u.shape, 1)
        first = lax.rem(lane, half) < quarter
        swapped = jnp.where(first, pltpu.roll(u, w - quarter, 1), pltpu.roll(u, quarter, 1))
        return u * cosine + swapped * sine

    def low_half(shape):
        return lax.broadcasted_iota(jnp.int32, shape, 1) < HEAD_SIZE

    def expand(x, at):
        low = low_half(x.shape)
        other = pltpu.roll(x, HEAD_SIZE, 1)
        span = slice(at, at + x.shape[0])
        kd[span, :] = jnp.where(low, x, other).astype(BF16)
        vd[span, :] = jnp.where(low, other, x).astype(BF16)

    u = acc[:, q_width:]
    kv_rows = jnp.where(low_half(u.shape), turn(u, cosv[...], sinv[...]), u)
    kvb[reach : reach + tok, :] = kv_rows.astype(BF16)

    up = pltpu.make_async_remote_copy(
        src_ref=kvb.at[pl.ds(tok, reach)], dst_ref=kvb.at[pl.ds(0, reach)],
        send_sem=h_s.at[0], recv_sem=h_r.at[0],
        device_id={"sp": lax.rem(sp + 1, n_sp)}, device_id_type=MESH,
    )
    down = pltpu.make_async_remote_copy(
        src_ref=kvb.at[pl.ds(reach, reach)], dst_ref=kvb.at[pl.ds(reach + tok, reach)],
        send_sem=h_s.at[1], recv_sem=h_r.at[1],
        device_id={"sp": lax.rem(sp + n_sp - 1, n_sp)}, device_id_type=MESH,
    )

    @pl.when(sp < n_sp - 1)
    def _():
        up.start()

    @pl.when(sp > 0)
    def _():
        down.start()

    expand(kv_rows, reach)

    factor = HEAD_SIZE ** (-0.5)
    for p in range(pairs):
        t = turn(acc[:, p * LANES : (p + 1) * LANES], cosv[...], sinv[...]) * factor
        low = low_half(t.shape)
        for parity, kept in ((0, jnp.where(low, t, 0.0)), (1, jnp.where(low, 0.0, t))):
            kept = kept.astype(BF16)
            at = (2 * p + parity) * reach
            for b in range(blocks):
                q4[b, at : at + reach, :] = kept[b * reach : (b + 1) * reach, :]

    window = tok + 2 * reach
    m_rows = heads * reach
    nt = (((1,), (1,)), ((), ()))

    def per_head(ref):
        return jnp.concatenate([jnp.full((reach, 1), ref[h], F32) for h in range(heads)], axis=0)

    n_all_ctx = n_sp * n_ctx
    delta = lax.broadcasted_iota(jnp.int32, (m_rows, reach), 1) - lax.rem(
        lax.broadcasted_iota(jnp.int32, (m_rows, reach), 0), reach
    )
    far = 4 * reach
    low_edge = jnp.where(sp == 0, far, 0)
    high_edge = jnp.where(sp == n_sp - 1, -far, 0)

    def scores(b, first, count):
        keys = kd[first : first + count, :]
        return lax.dot_general(q4[b], keys, nt, preferred_element_type=F32)

    def tiles(s):
        return [s[:, c * LANES : (c + 1) * LANES] for c in range(s.shape[1] // LANES)]

    def soften(parts, highest):
        powers = [jnp.exp(s - highest) for s in parts]
        mass = powers[0]
        for e in powers[1:]:
            mass = mass + e
        return powers, jnp.sum(mass, axis=-1, keepdims=True)

    def top_of(parts):
        top = parts[0]
        for s in parts[1:]:
            top = jnp.maximum(top, s)
        return jnp.max(top, axis=-1, keepdims=True)

    def weigh(powers, first):
        e = jnp.concatenate(powers, axis=1).astype(BF16)
        return jnp.dot(e, vd[first : first + e.shape[1], :], preferred_element_type=F32)

    def within(b):
        first, last = max(b - 1, 0), min(b + 1, blocks - 1)
        at = reach + first * reach
        parts = tiles(scores(b, at, (last - first + 1) * reach))
        if b > 0:
            parts[0] = jnp.where(delta >= 0, parts[0], MASKED)
        if b < blocks - 1:
            parts[-1] = jnp.where(delta <= 0, parts[-1], MASKED)
        sunk = per_head(sink)
        highest = jnp.maximum(top_of(parts), sunk)
        powers, mass = soften(parts, highest)
        return highest, mass + jnp.exp(sunk - highest), weigh(powers, at)

    g_copies = {}

    def beyond(b, state):
        highest, mass, weighed = state
        column = per_head(bias)
        groups = [(window, [s + column for s in tiles(scores(b, window, n_all_ctx))])]
        if b == 0:
            s = scores(b, 0, reach)
            groups.append((0, [jnp.where(delta >= low_edge, s, MASKED)]))
        if b == blocks - 1:
            s = scores(b, reach + tok, reach)
            groups.append((reach + tok, [jnp.where(delta <= high_edge, s, MASKED)]))
        top = jnp.maximum(top_of(sum([parts for _, parts in groups], [])), highest)
        fade = jnp.exp(highest - top)
        mass = mass * fade
        weighed = weighed * fade
        for at, parts in groups:
            powers, more = soften(parts, top)
            mass = mass + more
            weighed = weighed + weigh(powers, at)
        result = weighed / mass
        low = low_half((reach, LANES))
        for p in range(pairs):
            even = result[2 * p * reach : (2 * p + 1) * reach, :]
            odd = result[(2 * p + 1) * reach : (2 * p + 2) * reach, :]
            att[0, b, :, p * LANES : (p + 1) * LANES] = jnp.where(low, even, odd).astype(BF16)
        for o in direct:
            copy = pltpu.make_async_remote_copy(
                src_ref=att.at[0, b], dst_ref=att.at[o, b], send_sem=g_s.at[b, o - 1],
                recv_sem=g_r.at[b, o - 1], device_id={"tp": partner(o)}, device_id_type=MESH,
            )
            copy.start()
            g_copies[b, o] = copy

    def forward(b):
        for o in direct:
            g_copies[b, o].wait_recv()
            part = pl.ds((o - 1) * (reach // 2), reach // 2)
            copy = pltpu.make_async_remote_copy(
                src_ref=att.at[o, b, part], dst_ref=att.at[3, b, part],
                send_sem=g_s.at[b, 1 + o], recv_sem=g_r.at[b, 1 + o],
                device_id={"tp": partner(3 - o)}, device_id_type=MESH,
            )
            copy.start()
            g_copies[b, 2 + o] = copy

    order = list(range(1, blocks - 1)) + ([0, blocks - 1] if blocks > 1 else [0])
    states = {}
    for b in order:
        states[b] = within(b)
    for r in range(1, n_sp):
        c_copies[r - 1].wait_recv()
    for r in range(n_sp):
        expand(cxb[r].astype(F32), window + r * n_ctx)
    for b in order:
        if b == 0:
            @pl.when(sp > 0)
            def _():
                up.wait_recv()

            @pl.when(sp == 0)
            def _():
                kvb[0:reach, :] = jnp.zeros((reach, LANES), BF16)

            expand(kvb[0:reach, :].astype(F32), 0)
        if b == blocks - 1:
            @pl.when(sp < n_sp - 1)
            def _():
                down.wait_recv()

            @pl.when(sp == n_sp - 1)
            def _():
                kvb[reach + tok : window, :] = jnp.zeros((reach, LANES), BF16)

            expand(kvb[reach + tok : window, :].astype(F32), reach + tok)
        beyond(b, states[b])

    loads[14].wait()
    out_cols = ow.shape[1]
    mine = pl.ds(pl.multiple_of(tp * out_cols, out_cols), out_cols)
    gate = modv[0, 2:3, :]

    def project(b, o):
        w = ow[pl.ds(pl.multiple_of(owner(o) * q_width, q_width), q_width), :]
        return jnp.dot(att[o, b], w, preferred_element_type=F32)

    for b in order:
        if relayed:
            forward(b)
        mixed = project(b, 0)
        for o in direct:
            if not relayed:
                g_copies[b, o].wait_recv()
            mixed = mixed + project(b, o)
        outv[b * reach : (b + 1) * reach, :] = mixed
    for b in order:
        rows = slice(b * reach, (b + 1) * reach)
        mixed = outv[rows, :]
        if relayed:
            g_copies[b, 3].wait_recv()
            g_copies[b, 4].wait_recv()
            mixed = mixed + project(b, 3)
        outv[rows, :] = lat[rows, mine].astype(F32) + gate * mixed

    for copy in a_copies + list(b_copies.values()) + c_copies + list(g_copies.values()):
        copy.wait_send()

    @pl.when(sp < n_sp - 1)
    def _():
        up.wait_send()

    @pl.when(sp > 0)
    def _():
        down.wait_send()


def per_device(
    latent, conditioning, context_cond, modulation, context, query_weight, key_projection,
    value_projection, out_weight, sink_head_logit, prefix_logit_bias,
):
    n_sp, n_tp, n_dp = lax.axis_size("sp"), lax.axis_size("tp"), lax.axis_size("dp")
    samples = conditioning.shape[0]
    _, tok, width = latent.shape
    n_ctx = context.shape[1]
    depth, cols = modulation.shape[1:]
    q_width = query_weight.shape[1]
    heads = q_width // HEAD_SIZE
    out_cols = out_weight.shape[1]
    blocks = tok // WINDOW_REACH
    window = tok + 2 * WINDOW_REACH
    keys = window + n_sp * n_ctx
    n_td = n_tp * n_dp
    act_rows = -(-(samples + 1) // 8) * 8
    pack_rows = -(-(3 * samples + 2) // 8) * 8
    row_table, col_table = rotary_tables(n_sp * tok // GRID_W)
    vm = pltpu.VMEM
    dma = pltpu.SemaphoreType.DMA
    group = n_dp * cols
    scratch = [
        vm((tok, width), BF16), vm((samples, depth), BF16), vm((depth,), BF16),
        vm((3, depth, cols), BF16), vm((n_ctx, width), BF16), vm((width, q_width + LANES), BF16),
        vm(out_weight.shape, BF16), pltpu.SMEM((heads,), F32), pltpu.SMEM((heads,), F32),
        vm(row_table.shape, F32), vm(col_table.shape, F32),
        vm((act_rows, depth), F32), vm((pack_rows, cols), F32), vm((pack_rows, cols), BF16),
        vm((n_sp - 1, pack_rows, cols), BF16), vm((pack_rows, cols), F32),
        vm((n_dp, 8, cols), BF16), vm((n_td, 8, cols), BF16), vm((n_tp, 8, group), F32),
        vm((n_tp, tok, group), F32), vm((n_tp, n_ctx, group), F32), vm((tok, group), BF16),
        vm((n_ctx, group), BF16), vm((LANES, width), BF16), vm((tok, LANES), F32),
        vm((tok, LANES), F32), vm((tok, q_width + LANES), F32), vm((n_ctx, LANES), F32),
        vm((window, LANES), BF16), vm((n_sp, n_ctx, LANES), BF16),
        vm((keys, LANES), BF16), vm((keys, LANES), BF16),
        vm((blocks, heads * WINDOW_REACH, LANES), BF16),
        vm((n_tp, blocks, WINDOW_REACH, q_width), BF16),
        dma((15,)), dma((n_sp - 1,)), dma((n_sp - 1,)), dma((n_td,)),
        dma((n_td,)), dma((2,)), dma((2,)), dma((n_sp - 1,)), dma((n_sp - 1,)),
        dma((blocks, n_tp)), dma((blocks, n_tp)),
    ]
    stays = pl.BlockSpec(memory_space=pltpu.HBM)
    out = pl.pallas_call(
        functools.partial(block_kernel, (n_sp, n_tp, n_dp, samples)),
        out_shape=pltpu.VMEM((tok, out_cols), F32),
        in_specs=[stays] * 13,
        out_specs=pl.BlockSpec(memory_space=pltpu.VMEM),
        scratch_shapes=scratch,
        compiler_params=pltpu.CompilerParams(
            collective_id=0, has_side_effects=True, vmem_limit_bytes=66000000
        ),
        name="fused_block",
    )(
        latent[0], conditioning, context_cond, modulation, context[0], query_weight,
        key_projection.T, value_projection.T, out_weight, sink_head_logit, prefix_logit_bias,
        jnp.asarray(row_table), jnp.asarray(col_table),
    )
    return out[None]


def solution(mesh):
    placed = (
        P("dp", "sp", None),
        P(None, "sp"),
        P("sp"),
        P(None, "sp", ("tp", "dp")),
        P("dp", "sp", None),
        P(None, "tp"),
        P(None, "tp"),
        P(None, "tp"),
        P(None, "tp"),
        P("tp"),
        P("tp"),
    )
    return jax.shard_map(
        per_device, mesh=mesh, in_specs=placed, out_specs=P("dp", "sp", "tp"), check_vma=False
    )
```

```python
import functools

import jax
import jax.numpy as jnp
import numpy as np
from jax import lax
from jax.experimental import pallas as pl
from jax.experimental.pallas import tpu as pltpu
from jax.sharding import PartitionSpec as P

HEAD_SIZE = 64
GRID_W = 64
WINDOW_REACH = 128
NORM_EPSILON = 1e-06
ROTARY_BASE = 10000.0
MASKED = -1e30
LANES = 128
MESH = pl.DeviceIdType.MESH
F32 = jnp.float32
BF16 = jnp.bfloat16


def rotary_tables(grid_rows):
    half = HEAD_SIZE // 2
    quarter = half // 2
    lane = np.arange(LANES) % HEAD_SIZE
    frequency = ROTARY_BASE ** (-2.0 * (lane % quarter) / half)
    frequency = frequency.astype(np.float32).astype(np.float64)
    sign = np.where(lane % half < quarter, -1.0, 1.0)
    by_row = lane < half

    def tables(count, keep):
        angles = np.arange(count)[:, None] * frequency[None, :]
        cosine = np.where(keep[None, :], np.cos(angles), 0.0)
        sine = np.where(keep[None, :], np.sin(angles) * sign[None, :], 0.0)
        return np.stack([cosine, sine]).astype(np.float32)

    return tables(grid_rows, by_row), tables(GRID_W, ~by_row)


def block_kernel(
    dims,
    lat_hbm, cond_hbm, cctx_hbm, mod_hbm, ctx_hbm, qw_hbm, kw_hbm, vw_hbm, ow_hbm,
    sink_hbm, bias_hbm, rowt_hbm, colt_hbm,
    outv,
    lat, cond, cctx, mod, ctx, wall, ow, sink, bias, rowt, colt,
    act, packf, pack, packs, total, sendb, slots, modv,
    xn, xnc, nrm, nrmc, kvw, cosv, sinv, acc, accc, kvb, cxb, kd, vd, q4, att,
    in_sem, a_s, a_r, b_s, b_r, h_s, h_r, c_s, c_r, g_s, g_r,
):
    n_sp, n_tp, n_dp, samples = dims
    sp, tp, dp = lax.axis_index("sp"), lax.axis_index("tp"), lax.axis_index("dp")
    n_td = n_tp * n_dp
    me = tp * n_dp + dp
    tok, width = lat.shape
    cols = mod.shape[2]
    group = n_dp * cols
    n_ctx = ctx.shape[0]
    reach = WINDOW_REACH
    blocks = tok // reach
    q_width = wall.shape[1] - LANES
    pairs = q_width // LANES
    heads = 2 * pairs

    barrier = pltpu.get_barrier_semaphore()
    for o in range(1, n_sp):
        pl.semaphore_signal(
            barrier, inc=1, device_id={"sp": lax.rem(sp + o, n_sp)}, device_id_type=MESH
        )
    for o in range(1, n_td):
        lin = lax.rem(me + o, n_td)
        pl.semaphore_signal(
            barrier, inc=1, device_id={"tp": lin // n_dp, "dp": lax.rem(lin, n_dp)},
            device_id_type=MESH,
        )

    relayed = n_tp == 4
    direct = (1, 2) if relayed else range(1, n_tp)

    def partner(o):
        if not relayed:
            return lax.rem(tp + o, n_tp)
        x, y = lax.rem(tp, 2), tp // 2
        x = 1 - x if o % 2 else x
        y = 1 - y if o // 2 else y
        return 2 * y + x

    def owner(o):
        return partner(o) if relayed else lax.rem(tp + n_tp - o, n_tp)

    pairs_in = [
        (cond_hbm, cond), (cctx_hbm, cctx), (mod_hbm.at[0], mod.at[0]), (mod_hbm.at[1], mod.at[1]),
        (mod_hbm.at[2], mod.at[2]), (ctx_hbm, ctx), (lat_hbm, lat),
        (kw_hbm, kvw.at[pl.ds(0, HEAD_SIZE)]), (vw_hbm, kvw.at[pl.ds(HEAD_SIZE, HEAD_SIZE)]),
        (rowt_hbm, rowt), (colt_hbm, colt), (qw_hbm, wall.at[:, pl.ds(0, q_width)]),
        (sink_hbm, sink), (bias_hbm, bias), (ow_hbm, ow),
    ]
    loads = [
        pltpu.make_async_copy(src, dst, in_sem.at[i]) for i, (src, dst) in enumerate(pairs_in)
    ]
    for load in loads[:6]:
        load.start()

    act[...] = jnp.zeros_like(act)
    loads[0].wait()
    loads[1].wait()
    for load in loads[6:]:
        load.start()
    act[0:samples, :] = cond[...].astype(F32)
    act[samples : samples + 1, :] = cctx[...].astype(F32).reshape(1, cctx.shape[0])
    v = act[...]
    activated = (v / (1.0 + jnp.exp(-v))).astype(BF16)
    packf[...] = jnp.zeros_like(packf)
    n_rows = samples + 1
    for m in range(3):
        loads[2 + m].wait()
        count = n_rows if m < 2 else samples
        part = jnp.dot(activated, mod[m], preferred_element_type=F32)
        packf[m * n_rows : m * n_rows + count, :] = part[0:count, :]
    pack[...] = packf[...].astype(BF16)

    pl.semaphore_wait(barrier, n_sp - 1 + n_td - 1)
    a_copies = []
    for o in range(1, n_sp):
        copy = pltpu.make_async_remote_copy(
            src_ref=pack, dst_ref=packs.at[o - 1], send_sem=a_s.at[o - 1], recv_sem=a_r.at[o - 1],
            device_id={"sp": lax.rem(sp + o, n_sp)}, device_id_type=MESH,
        )
        copy.start()
        a_copies.append(copy)

    chunk = 64

    def normalise(src, dst, first, last):
        def body(i, carry):
            rows = pl.ds(pl.multiple_of(i * chunk, chunk), chunk)
            x = src[rows, :].astype(F32)
            x = x - jnp.mean(x, axis=-1, keepdims=True)
            spread = jnp.mean(x * x, axis=-1, keepdims=True)
            x = x * lax.rsqrt(spread + NORM_EPSILON)
            for t in range(n_tp):
                dst[t, rows, :] = x[:, t * group : (t + 1) * group]
            return carry

        lax.fori_loop(first, last, body, 0)

    loads[5].wait()
    normalise(ctx, xnc, 0, n_ctx // chunk)
    loads[6].wait()
    normalise(lat, xn, 0, tok // chunk)

    for copy in a_copies:
        copy.wait_recv()
    summed = packf[...]
    for o in range(1, n_sp):
        summed = summed + packs[o - 1].astype(F32)
    total[...] = summed
    for d in range(n_dp):
        rows = [
            total[source : source + 1, :]
            for source in (d, n_rows + d, 2 * n_rows + d, samples, n_rows + samples)
        ]
        rows.append(jnp.zeros((3, cols), F32))
        sendb[d] = jnp.concatenate(rows, axis=0).astype(BF16)
    b_copies = {}
    for o in range(n_tp):
        for e in range(n_dp):
            if o == 0 and e == 0:
                continue
            d = lax.rem(dp + e, n_dp)
            copy = pltpu.make_async_remote_copy(
                src_ref=sendb.at[d], dst_ref=slots.at[o * n_dp + dp],
                send_sem=b_s.at[o * n_dp + e], recv_sem=b_r.at[o * n_dp + e],
                device_id={"tp": partner(o), "dp": d}, device_id_type=MESH,
            )
            copy.start()
            b_copies[o, e] = copy
    slots[dp] = sendb[dp]

    for load in loads[7:14]:
        load.wait()
    groups = tok // GRID_W
    for g in range(groups):
        row = pl.ds(sp * groups + g, 1)
        span = slice(g * GRID_W, (g + 1) * GRID_W)
        cosv[span, :] = rowt[0, row, :] + colt[0]
        sinv[span, :] = rowt[1, row, :] + colt[1]
    for j in range(width // LANES):
        span = slice(j * LANES, (j + 1) * LANES)
        wall[span, q_width:] = kvw[:, span].astype(F32).T.astype(BF16)

    def condition(src, dst, count, o, g, shift_row, scale_row):
        scale = 1.0 + modv[o, scale_row : scale_row + 1, :]
        shift = modv[o, shift_row : shift_row + 1, :]
        for i in range(0, count, chunk):
            rows = slice(i, i + chunk)
            dst[rows, :] = (src[g, rows, :] * scale + shift).astype(BF16)

    c_copies = []
    for o in range(n_tp):
        for e in range(n_dp):
            if o or e:
                b_copies[o, e].wait_recv()
        for d in range(n_dp):
            modv[o, :, d * cols : (d + 1) * cols] = slots[o * n_dp + d].astype(F32)
        g = owner(o)
        weight_rows = pl.ds(pl.multiple_of(g * group, group), group)
        condition(xnc, nrmc, n_ctx, o, g, 3, 4)
        u = jnp.dot(nrmc[...], wall[weight_rows, q_width:], preferred_element_type=F32)
        if o:
            u = accc[...] + u
        if o < n_tp - 1:
            accc[...] = u
        else:
            cxb[0] = u.astype(BF16)
            for r in range(1, n_sp):
                copy = pltpu.make_async_remote_copy(
                    src_ref=cxb.at[0], dst_ref=cxb.at[r], send_sem=c_s.at[r - 1],
                    recv_sem=c_r.at[r - 1], device_id={"sp": lax.rem(sp + r, n_sp)},
                    device_id_type=MESH,
                )
                copy.start()
                c_copies.append(copy)
        condition(xn, nrm, tok, o, g, 0, 1)
        u = jnp.dot(nrm[...], wall[weight_rows, :], preferred_element_type=F32)
        if o:
            u = acc[...] + u
        acc[...] = u

    half = HEAD_SIZE // 2
    quarter = half // 2

    def turn(u, cosine, sine):
        w = u.shape[1]
        lane = lax.broadcasted_iota(jnp.int32, u.shape, 1)
        first = lax.rem(lane, half) < quarter
        swapped = jnp.where(first, pltpu.roll(u, w - quarter, 1), pltpu.roll(u, quarter, 1))
        return u * cosine + swapped * sine

    def low_half(shape):
        return lax.broadcasted_iota(jnp.int32, shape, 1) < HEAD_SIZE

    def expand(x, at):
        low = low_half(x.shape)
        other = pltpu.roll(x, HEAD_SIZE, 1)
        span = slice(at, at + x.shape[0])
        kd[span, :] = jnp.where(low, x, other).astype(BF16)
        vd[span, :] = jnp.where(low, other, x).astype(BF16)

    u = acc[:, q_width:]
    kv_rows = jnp.where(low_half(u.shape), turn(u, cosv[...], sinv[...]), u)
    kvb[reach : reach + tok, :] = kv_rows.astype(BF16)

    up = pltpu.make_async_remote_copy(
        src_ref=kvb.at[pl.ds(tok, reach)], dst_ref=kvb.at[pl.ds(0, reach)],
        send_sem=h_s.at[0], recv_sem=h_r.at[0],
        device_id={"sp": lax.rem(sp + 1, n_sp)}, device_id_type=MESH,
    )
    down = pltpu.make_async_remote_copy(
        src_ref=kvb.at[pl.ds(reach, reach)], dst_ref=kvb.at[pl.ds(reach + tok, reach)],
        send_sem=h_s.at[1], recv_sem=h_r.at[1],
        device_id={"sp": lax.rem(sp + n_sp - 1, n_sp)}, device_id_type=MESH,
    )

    @pl.when(sp < n_sp - 1)
    def _():
        up.start()

    @pl.when(sp > 0)
    def _():
        down.start()

    expand(kv_rows, reach)

    factor = HEAD_SIZE ** (-0.5)
    for p in range(pairs):
        t = turn(acc[:, p * LANES : (p + 1) * LANES], cosv[...], sinv[...]) * factor
        low = low_half(t.shape)
        for parity, kept in ((0, jnp.where(low, t, 0.0)), (1, jnp.where(low, 0.0, t))):
            kept = kept.astype(BF16)
            at = (2 * p + parity) * reach
            for b in range(blocks):
                q4[b, at : at + reach, :] = kept[b * reach : (b + 1) * reach, :]

    window = tok + 2 * reach
    nt = (((1,), (1,)), ((), ()))
    n_all_ctx = n_sp * n_ctx
    delta = lax.broadcasted_iota(jnp.int32, (reach, reach), 1) - lax.broadcasted_iota(
        jnp.int32, (reach, reach), 0
    )
    far = 4 * reach
    low_edge = jnp.where(sp == 0, far, 0)
    high_edge = jnp.where(sp == n_sp - 1, -far, 0)

    def scores(b, first, count):
        keys = kd[first : first + count, :]
        return lax.dot_general(q4[b], keys, nt, preferred_element_type=F32)

    def tiles(s, h):
        rows = slice(h * reach, (h + 1) * reach)
        return [s[rows, c * LANES : (c + 1) * LANES] for c in range(s.shape[1] // LANES)]

    def soften(parts, highest):
        powers = [jnp.exp(s - highest) for s in parts]
        mass = powers[0]
        for e in powers[1:]:
            mass = mass + e
        powers = jnp.concatenate([e.astype(BF16) for e in powers], axis=1)
        return powers, jnp.sum(mass, axis=-1, keepdims=True)

    def top_of(parts):
        top = parts[0]
        for s in parts[1:]:
            top = jnp.maximum(top, s)
        return jnp.max(top, axis=-1, keepdims=True)

    def weigh(powers, first):
        e = jnp.concatenate(powers, axis=0)
        return jnp.dot(e, vd[first : first + e.shape[1], :], preferred_element_type=F32)

    def within(b):
        first, last = max(b - 1, 0), min(b + 1, blocks - 1)
        at = reach + first * reach
        s = scores(b, at, (last - first + 1) * reach)
        tops, masses, powers = [], [], []
        for h in range(heads):
            parts = tiles(s, h)
            if b > 0:
                parts[0] = jnp.where(delta >= 0, parts[0], MASKED)
            if b < blocks - 1:
                parts[-1] = jnp.where(delta <= 0, parts[-1], MASKED)
            highest = jnp.maximum(top_of(parts), sink[h])
            e, mass = soften(parts, highest)
            tops.append(highest)
            masses.append(mass + jnp.exp(sink[h] - highest))
            powers.append(e)
        return tops, masses, weigh(powers, at)

    g_copies = {}

    def beyond(b, state):
        tops, masses, weighed = state
        parts_of = [(window, scores(b, window, n_all_ctx))]
        if b == 0:
            parts_of.append((0, scores(b, 0, reach)))
        if b == blocks - 1:
            parts_of.append((reach + tok, scores(b, reach + tok, reach)))
        fades, powers = [], [[] for _ in parts_of]
        for h in range(heads):
            groups = [[s + bias[h] for s in tiles(parts_of[0][1], h)]]
            if b == 0:
                groups.append([jnp.where(delta >= low_edge, parts_of[-1][1][h * reach : (h + 1) * reach], MASKED)])
            if b == blocks - 1:
                groups.append([jnp.where(delta <= high_edge, parts_of[-1][1][h * reach : (h + 1) * reach], MASKED)])
            top = jnp.maximum(top_of(sum(groups, [])), tops[h])
            fade = jnp.exp(tops[h] - top)
            mass = masses[h] * fade
            for i, parts in enumerate(groups):
                e, more = soften(parts, top)
                powers[i].append(e)
                mass = mass + more
            share = 1.0 / mass
            fades.append((fade * share, share))
        more = weigh(powers[0], window)
        for i in range(1, len(parts_of)):
            more = more + weigh(powers[i], parts_of[i][0])
        low = low_half((reach, LANES))
        for p in range(pairs):
            halves = []
            for h in (2 * p, 2 * p + 1):
                rows = slice(h * reach, (h + 1) * reach)
                halves.append(weighed[rows, :] * fades[h][0] + more[rows, :] * fades[h][1])
            att[0, b, :, p * LANES : (p + 1) * LANES] = jnp.where(low, *halves).astype(BF16)
        for o in direct:
            copy = pltpu.make_async_remote_copy(
                src_ref=att.at[0, b], dst_ref=att.at[o, b], send_sem=g_s.at[b, o - 1],
                recv_sem=g_r.at[b, o - 1], device_id={"tp": partner(o)}, device_id_type=MESH,
            )
            copy.start()
            g_copies[b, o] = copy

    def forward(b):
        for o in direct:
            g_copies[b, o].wait_recv()
            part = pl.ds((o - 1) * (reach // 2), reach // 2)
            copy = pltpu.make_async_remote_copy(
                src_ref=att.at[o, b, part], dst_ref=att.at[3, b, part],
                send_sem=g_s.at[b, 1 + o], recv_sem=g_r.at[b, 1 + o],
                device_id={"tp": partner(3 - o)}, device_id_type=MESH,
            )
            copy.start()
            g_copies[b, 2 + o] = copy

    order = list(range(1, blocks - 1)) + ([0, blocks - 1] if blocks > 1 else [0])
    states = {}
    for b in order:
        states[b] = within(b)
    for r in range(1, n_sp):
        c_copies[r - 1].wait_recv()
    for r in range(n_sp):
        expand(cxb[r].astype(F32), window + r * n_ctx)
    for b in order:
        if b == 0:
            @pl.when(sp > 0)
            def _():
                up.wait_recv()

            @pl.when(sp == 0)
            def _():
                kvb[0:reach, :] = jnp.zeros((reach, LANES), BF16)

            expand(kvb[0:reach, :].astype(F32), 0)
        if b == blocks - 1:
            @pl.when(sp < n_sp - 1)
            def _():
                down.wait_recv()

            @pl.when(sp == n_sp - 1)
            def _():
                kvb[reach + tok : window, :] = jnp.zeros((reach, LANES), BF16)

            expand(kvb[reach + tok : window, :].astype(F32), reach + tok)
        beyond(b, states[b])

    loads[14].wait()
    out_cols = ow.shape[1]
    mine = pl.ds(pl.multiple_of(tp * out_cols, out_cols), out_cols)
    gate = modv[0, 2:3, :]

    def project(b, o):
        w = ow[pl.ds(pl.multiple_of(owner(o) * q_width, q_width), q_width), :]
        return jnp.dot(att[o, b], w, preferred_element_type=F32)

    for b in order:
        if relayed:
            forward(b)
        mixed = project(b, 0)
        for o in direct:
            if not relayed:
                g_copies[b, o].wait_recv()
            mixed = mixed + project(b, o)
        outv[b * reach : (b + 1) * reach, :] = mixed
    for b in order:
        rows = slice(b * reach, (b + 1) * reach)
        mixed = outv[rows, :]
        if relayed:
            g_copies[b, 3].wait_recv()
            g_copies[b, 4].wait_recv()
            mixed = mixed + project(b, 3)
        outv[rows, :] = lat[rows, mine].astype(F32) + gate * mixed

    for copy in a_copies + list(b_copies.values()) + c_copies + list(g_copies.values()):
        copy.wait_send()

    @pl.when(sp < n_sp - 1)
    def _():
        up.wait_send()

    @pl.when(sp > 0)
    def _():
        down.wait_send()


def per_device(
    latent, conditioning, context_cond, modulation, context, query_weight, key_projection,
    value_projection, out_weight, sink_head_logit, prefix_logit_bias,
):
    n_sp, n_tp, n_dp = lax.axis_size("sp"), lax.axis_size("tp"), lax.axis_size("dp")
    samples = conditioning.shape[0]
    _, tok, width = latent.shape
    n_ctx = context.shape[1]
    depth, cols = modulation.shape[1:]
    q_width = query_weight.shape[1]
    heads = q_width // HEAD_SIZE
    out_cols = out_weight.shape[1]
    blocks = tok // WINDOW_REACH
    window = tok + 2 * WINDOW_REACH
    keys = window + n_sp * n_ctx
    n_td = n_tp * n_dp
    act_rows = -(-(samples + 1) // 8) * 8
    pack_rows = -(-(3 * samples + 2) // 8) * 8
    row_table, col_table = rotary_tables(n_sp * tok // GRID_W)
    vm = pltpu.VMEM
    dma = pltpu.SemaphoreType.DMA
    group = n_dp * cols
    scratch = [
        vm((tok, width), BF16), vm((samples, depth), BF16), vm((depth,), BF16),
        vm((3, depth, cols), BF16), vm((n_ctx, width), BF16), vm((width, q_width + LANES), BF16),
        vm(out_weight.shape, BF16), pltpu.SMEM((heads,), F32), pltpu.SMEM((heads,), F32),
        vm(row_table.shape, F32), vm(col_table.shape, F32),
        vm((act_rows, depth), F32), vm((pack_rows, cols), F32), vm((pack_rows, cols), BF16),
        vm((n_sp - 1, pack_rows, cols), BF16), vm((pack_rows, cols), F32),
        vm((n_dp, 8, cols), BF16), vm((n_td, 8, cols), BF16), vm((n_tp, 8, group), F32),
        vm((n_tp, tok, group), F32), vm((n_tp, n_ctx, group), F32), vm((tok, group), BF16),
        vm((n_ctx, group), BF16), vm((LANES, width), BF16), vm((tok, LANES), F32),
        vm((tok, LANES), F32), vm((tok, q_width + LANES), F32), vm((n_ctx, LANES), F32),
        vm((window, LANES), BF16), vm((n_sp, n_ctx, LANES), BF16),
        vm((keys, LANES), BF16), vm((keys, LANES), BF16),
        vm((blocks, heads * WINDOW_REACH, LANES), BF16),
        vm((n_tp, blocks, WINDOW_REACH, q_width), BF16),
        dma((15,)), dma((n_sp - 1,)), dma((n_sp - 1,)), dma((n_td,)),
        dma((n_td,)), dma((2,)), dma((2,)), dma((n_sp - 1,)), dma((n_sp - 1,)),
        dma((blocks, n_tp)), dma((blocks, n_tp)),
    ]
    stays = pl.BlockSpec(memory_space=pltpu.HBM)
    out = pl.pallas_call(
        functools.partial(block_kernel, (n_sp, n_tp, n_dp, samples)),
        out_shape=pltpu.VMEM((tok, out_cols), F32),
        in_specs=[stays] * 13,
        out_specs=pl.BlockSpec(memory_space=pltpu.VMEM),
        scratch_shapes=scratch,
        compiler_params=pltpu.CompilerParams(
            collective_id=0, has_side_effects=True, vmem_limit_bytes=66000000
        ),
        name="fused_block",
    )(
        latent[0], conditioning, context_cond, modulation, context[0], query_weight,
        key_projection.T, value_projection.T, out_weight, sink_head_logit, prefix_logit_bias,
        jnp.asarray(row_table), jnp.asarray(col_table),
    )
    return out[None]


def solution(mesh):
    placed = (
        P("dp", "sp", None),
        P(None, "sp"),
        P("sp"),
        P(None, "sp", ("tp", "dp")),
        P("dp", "sp", None),
        P(None, "tp"),
        P(None, "tp"),
        P(None, "tp"),
        P(None, "tp"),
        P("tp"),
        P("tp"),
    )
    return jax.shard_map(
        per_device, mesh=mesh, in_specs=placed, out_specs=P("dp", "sp", "tp"), check_vma=False
    )
```

```python
import functools

import jax
import jax.numpy as jnp
import numpy as np
from jax import lax
from jax.experimental import pallas as pl
from jax.experimental.pallas import tpu as pltpu
from jax.sharding import PartitionSpec as P

HEAD_SIZE = 64
GRID_W = 64
WINDOW_REACH = 128
NORM_EPSILON = 1e-06
ROTARY_BASE = 10000.0
MASKED = -1e30
LANES = 128
MESH = pl.DeviceIdType.MESH
F32 = jnp.float32
BF16 = jnp.bfloat16


def rotary_tables(grid_rows):
    half = HEAD_SIZE // 2
    quarter = half // 2
    lane = np.arange(LANES) % HEAD_SIZE
    frequency = ROTARY_BASE ** (-2.0 * (lane % quarter) / half)
    frequency = frequency.astype(np.float32).astype(np.float64)
    sign = np.where(lane % half < quarter, -1.0, 1.0)
    by_row = lane < half

    def tables(count, keep):
        angles = np.arange(count)[:, None] * frequency[None, :]
        cosine = np.where(keep[None, :], np.cos(angles), 0.0)
        sine = np.where(keep[None, :], np.sin(angles) * sign[None, :], 0.0)
        return np.stack([cosine, sine]).astype(np.float32)

    return tables(grid_rows, by_row), tables(GRID_W, ~by_row)


def block_kernel(
    dims,
    lat_hbm, cond_hbm, cctx_hbm, mod_hbm, ctx_hbm, qw_hbm, kw_hbm, vw_hbm, ow_hbm,
    sink_hbm, bias_hbm, turn_hbm,
    outv,
    lat, cond, cctx, mod, ctx, wall, ow, sink, bias, angles,
    act, packf, pack, packs, total, sendb, slots, modv,
    xn, xnc, nrm, nrmc, kvw, cosv, sinv, acc, accc, kvb, cxs, cxb, kd, vd, q4, att,
    in_sem, a_s, a_r, x_s, x_r, b_s, b_r, h_s, h_r, c_s, c_r, g_s, g_r,
):
    n_sp, n_tp, n_dp, samples = dims
    sp, tp, dp = lax.axis_index("sp"), lax.axis_index("tp"), lax.axis_index("dp")
    n_td = n_tp * n_dp
    me = tp * n_dp + dp
    tok, width = lat.shape
    cols = mod.shape[2]
    group = n_dp * cols
    n_ctx = ctx.shape[1]
    core, lead, pair = lax.rem(dp, 2), dp - lax.rem(dp, 2) + 1, dp // 2
    n_pairs = n_dp // 2
    reach = WINDOW_REACH
    blocks = tok // reach
    q_width = wall.shape[1] - LANES
    pairs = q_width // LANES
    heads = 2 * pairs

    barrier = pltpu.get_barrier_semaphore()
    for o in range(1, n_sp):
        for d in (dp, 2 * pair + 1 - core):
            pl.semaphore_signal(
                barrier, inc=1, device_id={"sp": lax.rem(sp + o, n_sp), "dp": d},
                device_id_type=MESH,
            )
    for o in range(1, n_td):
        lin = lax.rem(me + o, n_td)
        pl.semaphore_signal(
            barrier, inc=1, device_id={"tp": lin // n_dp, "dp": lax.rem(lin, n_dp)},
            device_id_type=MESH,
        )

    relayed = n_tp == 4
    direct = (1, 2) if relayed else range(1, n_tp)

    def partner(o):
        if not relayed:
            return lax.rem(tp + o, n_tp)
        x, y = lax.rem(tp, 2), tp // 2
        x = 1 - x if o % 2 else x
        y = 1 - y if o // 2 else y
        return 2 * y + x

    def owner(o):
        return partner(o) if relayed else lax.rem(tp + n_tp - o, n_tp)

    pairs_in = [
        (cond_hbm, cond, 0), (cctx_hbm, cctx, 1), (mod_hbm, mod, 2), (ctx_hbm, ctx.at[0], 3),
        (lat_hbm, lat, 4), (kw_hbm, kvw.at[pl.ds(0, HEAD_SIZE)], 5),
        (vw_hbm, kvw.at[pl.ds(HEAD_SIZE, HEAD_SIZE)], 5), (turn_hbm, angles, 6),
        (qw_hbm, wall.at[:, pl.ds(0, q_width)], 7), (sink_hbm, sink, 8), (bias_hbm, bias, 9),
        (ow_hbm, ow, 10),
    ]
    loads = [pltpu.make_async_copy(src, dst, in_sem.at[i]) for src, dst, i in pairs_in]
    for load in loads[:4]:
        load.start()

    def remote(src, dst, left, arrived, **device):
        return pltpu.make_async_remote_copy(
            src_ref=src, dst_ref=dst, send_sem=left, recv_sem=arrived, device_id=device,
            device_id_type=MESH,
        )

    def bytes_of(ref, semaphore):
        pltpu.make_async_copy(ref, ref, semaphore).wait()

    act[...] = jnp.zeros_like(act)
    loads[0].wait()
    loads[1].wait()
    for load in loads[4:]:
        load.start()
    act[0:samples, :] = cond[...].astype(F32)
    act[samples : samples + 1, :] = cctx[...].astype(F32).reshape(1, cctx.shape[0])
    v = act[...]
    activated = (v / (1.0 + jnp.exp(-v))).astype(BF16)
    packf[...] = jnp.zeros_like(packf)
    n_rows = samples + 1
    loads[2].wait()
    for m in range(3):
        count = n_rows if m < 2 else samples
        part = jnp.dot(activated, mod[m], preferred_element_type=F32)
        packf[m * n_rows : m * n_rows + count, :] = part[0:count, :]
    pack[...] = packf[...].astype(BF16)

    pl.semaphore_wait(barrier, 2 * (n_sp - 1) + n_td - 1)
    a_copies = [
        remote(
            pack, packs.at[2 * o - 1 + core if o else 0], a_s.at[0], a_r.at[0],
            sp=lax.rem(sp + o, n_sp), dp=lead,
        )
        for o in range(n_sp)
    ]
    for copy in a_copies[1:]:
        copy.start()
    spare = remote(ctx.at[0], ctx.at[1], x_s.at[0], x_r.at[0], dp=lead)
    loads[3].wait()

    @pl.when(core == 0)
    def _():
        a_copies[0].start()
        spare.start()

    chunk = 64

    def normalise(src, dst, first, last):
        def body(i, carry):
            rows = pl.ds(pl.multiple_of(i * chunk, chunk), chunk)
            x = src[rows, :].astype(F32)
            x = x - jnp.mean(x, axis=-1, keepdims=True)
            spread = jnp.mean(x * x, axis=-1, keepdims=True)
            x = x * lax.rsqrt(spread + NORM_EPSILON)
            for t in range(n_tp):
                dst[t, rows, :] = x[:, t * group : (t + 1) * group]
            return carry

        lax.fori_loop(first, last, body, 0)

    def normalise_context(which):
        for i in range(0, n_ctx, chunk):
            x = ctx[which, i : i + chunk, :].astype(F32)
            x = x - jnp.mean(x, axis=-1, keepdims=True)
            spread = jnp.mean(x * x, axis=-1, keepdims=True)
            x = x * lax.rsqrt(spread + NORM_EPSILON)
            at = which * n_ctx + i
            for t in range(n_tp):
                xnc[t, at : at + chunk, :] = x[:, t * group : (t + 1) * group]

    loads[4].wait()
    normalise(lat, xn, 0, tok // chunk)

    @pl.when(core == 1)
    def _():
        normalise_context(0)
        spare.wait_recv()
        normalise_context(1)


    b_copies = [
        remote(
            sendb.at[lax.rem(dp + e, n_dp)], slots.at[o, pair], b_s.at[o], b_r.at[o],
            tp=partner(o), dp=lax.rem(dp + e, n_dp),
        )
        for o in range(n_tp)
        for e in range(n_dp)
        if o or e
    ]

    @pl.when(core == 1)
    def _():
        bytes_of(packs, a_r.at[0])
        for c in range(2):
            summed = packf[...] if c else packs[0].astype(F32)
            for o in range(1, n_sp):
                summed = summed + packs[2 * o - 1 + c].astype(F32)
            total[c] = summed
        for d in range(n_dp):
            for c in range(2):
                rows = [
                    total[c, source : source + 1, :]
                    for source in (d, n_rows + d, 2 * n_rows + d, samples, n_rows + samples)
                ]
                rows.append(jnp.zeros((3, cols), F32))
                sendb[d, c] = jnp.concatenate(rows, axis=0).astype(BF16)
        for copy in b_copies:
            copy.start()
        slots[0, pair] = sendb[dp]

    bytes_of(kvw, in_sem.at[5])
    for load in loads[7:11]:
        load.wait()
    groups = tok // GRID_W
    for g in range(groups):
        row = pl.ds(GRID_W + sp * groups + g, 1)
        span = slice(g * GRID_W, (g + 1) * GRID_W)
        cosv[span, :] = angles[0, row, :] + angles[0, 0:GRID_W, :]
        sinv[span, :] = angles[1, row, :] + angles[1, 0:GRID_W, :]
    for j in range(width // LANES):
        span = slice(j * LANES, (j + 1) * LANES)
        wall[span, q_width:] = kvw[:, span].astype(F32).T.astype(BF16)

    def condition(src, dst, count, o, g, shift_row, scale_row):
        scale = 1.0 + modv[o, scale_row : scale_row + 1, :]
        shift = modv[o, shift_row : shift_row + 1, :]
        for i in range(0, count, chunk):
            rows = slice(i, i + chunk)
            dst[rows, :] = (src[g, rows, :] * scale + shift).astype(BF16)

    c_copies = [remote(cxs.at[0], cxb.at[0], c_s.at[0], c_r.at[0], dp=dp - core)]
    for r in range(1, n_sp):
        for c in range(2):
            c_copies.append(
                remote(
                    cxs.at[c], cxb.at[r], c_s.at[c], c_r.at[0],
                    sp=lax.rem(sp + r, n_sp), dp=2 * pair + c,
                )
            )
    for o in range(n_tp):
        if o:
            bytes_of(slots.at[o], b_r.at[o])
        else:
            @pl.when(core == 0)
            def _():
                bytes_of(slots.at[0], b_r.at[0])

            if n_pairs > 1:
                @pl.when(core == 1)
                def _():
                    bytes_of(slots.at[0, pl.ds(1, n_pairs - 1)], b_r.at[0])
        for d in range(n_dp):
            modv[o, :, d * cols : (d + 1) * cols] = slots[o, d // 2, d % 2].astype(F32)
        g = owner(o)
        weight_rows = pl.ds(pl.multiple_of(g * group, group), group)

        @pl.when(core == 1)
        def _():
            condition(xnc, nrmc, 2 * n_ctx, o, g, 3, 4)
            u = jnp.dot(nrmc[...], wall[weight_rows, q_width:], preferred_element_type=F32)
            if o:
                u = accc[...] + u
            if o < n_tp - 1:
                accc[...] = u
            else:
                cxs[0] = u[n_ctx:, :].astype(BF16)
                cxs[1] = u[0:n_ctx, :].astype(BF16)
                for copy in c_copies[1:] + c_copies[:1]:
                    copy.start()
                cxb[0] = u[0:n_ctx, :].astype(BF16)

        condition(xn, nrm, tok, o, g, 0, 1)
        u = jnp.dot(nrm[...], wall[weight_rows, :], preferred_element_type=F32)
        if o:
            u = acc[...] + u
        acc[...] = u

    half = HEAD_SIZE // 2
    quarter = half // 2

    def turn(u, cosine, sine):
        w = u.shape[1]
        lane = lax.broadcasted_iota(jnp.int32, u.shape, 1)
        first = lax.rem(lane, half) < quarter
        swapped = jnp.where(first, pltpu.roll(u, w - quarter, 1), pltpu.roll(u, quarter, 1))
        return u * cosine + swapped * sine

    def low_half(shape):
        return lax.broadcasted_iota(jnp.int32, shape, 1) < HEAD_SIZE

    def expand(x, at):
        low = low_half(x.shape)
        other = pltpu.roll(x, HEAD_SIZE, 1)
        span = slice(at, at + x.shape[0])
        kd[span, :] = jnp.where(low, x, other).astype(BF16)
        vd[span, :] = jnp.where(low, other, x).astype(BF16)

    u = acc[:, q_width:]
    kv_rows = jnp.where(low_half(u.shape), turn(u, cosv[...], sinv[...]), u)
    kvb[reach : reach + tok, :] = kv_rows.astype(BF16)

    up = remote(
        kvb.at[pl.ds(tok, reach)], kvb.at[pl.ds(0, reach)], h_s.at[0], h_r.at[0],
         sp=lax.rem(sp + 1, n_sp)
    )
    down = remote(
        kvb.at[pl.ds(reach, reach)], kvb.at[pl.ds(reach + tok, reach)], h_s.at[1], h_r.at[1],
        sp=lax.rem(sp + n_sp - 1, n_sp),
    )

    @pl.when(sp < n_sp - 1)
    def _():
        up.start()

    @pl.when(sp > 0)
    def _():
        down.start()

    expand(kv_rows, reach)

    factor = HEAD_SIZE ** (-0.5)
    for p in range(pairs):
        t = turn(acc[:, p * LANES : (p + 1) * LANES], cosv[...], sinv[...]) * factor
        low = low_half(t.shape)
        for parity, kept in ((0, jnp.where(low, t, 0.0)), (1, jnp.where(low, 0.0, t))):
            kept = kept.astype(BF16)
            at = (2 * p + parity) * reach
            for b in range(blocks):
                q4[b, at : at + reach, :] = kept[b * reach : (b + 1) * reach, :]

    window = tok + 2 * reach
    nt = (((1,), (1,)), ((), ()))
    n_all_ctx = n_sp * n_ctx
    delta = lax.broadcasted_iota(jnp.int32, (reach, reach), 1) - lax.broadcasted_iota(
        jnp.int32, (reach, reach), 0
    )
    far = 4 * reach
    low_edge = jnp.where(sp == 0, far, 0)
    high_edge = jnp.where(sp == n_sp - 1, -far, 0)

    def scores(b, first, count):
        keys = kd[first : first + count, :]
        return lax.dot_general(q4[b], keys, nt, preferred_element_type=F32)

    def tiles(s, h):
        rows = slice(h * reach, (h + 1) * reach)
        return [s[rows, c * LANES : (c + 1) * LANES] for c in range(s.shape[1] // LANES)]

    def soften(parts, highest):
        powers = [jnp.exp(s - highest) for s in parts]
        mass = powers[0]
        for e in powers[1:]:
            mass = mass + e
        powers = jnp.concatenate([e.astype(BF16) for e in powers], axis=1)
        return powers, jnp.sum(mass, axis=-1, keepdims=True)

    def top_of(parts):
        top = parts[0]
        for s in parts[1:]:
            top = jnp.maximum(top, s)
        return jnp.max(top, axis=-1, keepdims=True)

    def weigh(powers, first):
        e = jnp.concatenate(powers, axis=0)
        return jnp.dot(e, vd[first : first + e.shape[1], :], preferred_element_type=F32)

    def within(b):
        first, last = max(b - 1, 0), min(b + 1, blocks - 1)
        at = reach + first * reach
        s = scores(b, at, (last - first + 1) * reach)
        tops, masses, powers = [], [], []
        for h in range(heads):
            parts = tiles(s, h)
            if b > 0:
                parts[0] = jnp.where(delta >= 0, parts[0], MASKED)
            if b < blocks - 1:
                parts[-1] = jnp.where(delta <= 0, parts[-1], MASKED)
            highest = jnp.maximum(top_of(parts), sink[h])
            e, mass = soften(parts, highest)
            tops.append(highest)
            masses.append(mass + jnp.exp(sink[h] - highest))
            powers.append(e)
        return tops, masses, weigh(powers, at)

    g_copies = {}

    def beyond(b, state):
        tops, masses, weighed = state
        parts_of = [(window, scores(b, window, n_all_ctx))]
        if b == 0:
            parts_of.append((0, scores(b, 0, reach)))
        if b == blocks - 1:
            parts_of.append((reach + tok, scores(b, reach + tok, reach)))
        fades, powers = [], [[] for _ in parts_of]
        for h in range(heads):
            groups = [[s + bias[h] for s in tiles(parts_of[0][1], h)]]
            if b == 0:
                groups.append([jnp.where(delta >= low_edge, parts_of[-1][1][h * reach : (h + 1) * reach], MASKED)])
            if b == blocks - 1:
                groups.append([jnp.where(delta <= high_edge, parts_of[-1][1][h * reach : (h + 1) * reach], MASKED)])
            top = jnp.maximum(top_of(sum(groups, [])), tops[h])
            fade = jnp.exp(tops[h] - top)
            mass = masses[h] * fade
            for i, parts in enumerate(groups):
                e, more = soften(parts, top)
                powers[i].append(e)
                mass = mass + more
            share = 1.0 / mass
            fades.append((fade * share, share))
        more = weigh(powers[0], window)
        for i in range(1, len(parts_of)):
            more = more + weigh(powers[i], parts_of[i][0])
        low = low_half((reach, LANES))
        for p in range(pairs):
            halves = []
            for h in (2 * p, 2 * p + 1):
                rows = slice(h * reach, (h + 1) * reach)
                halves.append(weighed[rows, :] * fades[h][0] + more[rows, :] * fades[h][1])
            att[0, b, :, p * LANES : (p + 1) * LANES] = jnp.where(low, *halves).astype(BF16)
        for o in direct:
            g_copies[b, o] = remote(
                att.at[0, b], att.at[o, b], g_s.at[0], g_r.at[b, 0], tp=partner(o)
            )
            g_copies[b, o].start()

    def forward(b):
        for o in direct:
            part = pl.ds((o - 1) * (reach // 2), reach // 2)
            g_copies[b, 2 + o] = remote(
                att.at[o, b, part], att.at[3, b, part], g_s.at[1], g_r.at[b, 1],
                tp=partner(3 - o),
            )
            g_copies[b, 2 + o].start()

    order = list(range(1, blocks - 1)) + ([0, blocks - 1] if blocks > 1 else [0])
    states = {}
    for b in order:
        states[b] = within(b)

    @pl.when(core == 0)
    def _():
        bytes_of(cxb, c_r.at[0])

    @pl.when(core == 1)
    def _():
        bytes_of(cxb.at[pl.ds(1, n_sp - 1)], c_r.at[0])

    for r in range(n_sp):
        expand(cxb[r].astype(F32), window + r * n_ctx)
    for b in order:
        if b == 0:
            @pl.when(sp > 0)
            def _():
                up.wait_recv()

            @pl.when(sp == 0)
            def _():
                kvb[0:reach, :] = jnp.zeros((reach, LANES), BF16)

            expand(kvb[0:reach, :].astype(F32), 0)
        if b == blocks - 1:
            @pl.when(sp < n_sp - 1)
            def _():
                down.wait_recv()

            @pl.when(sp == n_sp - 1)
            def _():
                kvb[reach + tok : window, :] = jnp.zeros((reach, LANES), BF16)

            expand(kvb[reach + tok : window, :].astype(F32), reach + tok)
        beyond(b, states[b])

    loads[11].wait()
    out_cols = ow.shape[1]
    mine = pl.ds(pl.multiple_of(tp * out_cols, out_cols), out_cols)
    gate = modv[0, 2:3, :]

    def project(b, o):
        w = ow[pl.ds(pl.multiple_of(owner(o) * q_width, q_width), q_width), :]
        return jnp.dot(att[o, b], w, preferred_element_type=F32)

    for b in order:
        bytes_of(att.at[pl.ds(1, len(direct)), b], g_r.at[b, 0])
        if relayed:
            forward(b)
        mixed = project(b, 0)
        for o in direct:
            mixed = mixed + project(b, o)
        outv[b * reach : (b + 1) * reach, :] = mixed
    for b in order:
        rows = slice(b * reach, (b + 1) * reach)
        mixed = outv[rows, :]
        if relayed:
            bytes_of(att.at[3, b], g_r.at[b, 1])
            mixed = mixed + project(b, 3)
        outv[rows, :] = lat[rows, mine].astype(F32) + gate * mixed

    bytes_of(att.at[pl.ds(1, len(direct))], g_s.at[0])
    if relayed:
        bytes_of(att.at[3], g_s.at[1])

    @pl.when(core == 0)
    def _():
        bytes_of(packs.at[pl.ds(0, n_sp)], a_s.at[0])
        spare.wait_send()

    @pl.when(core == 1)
    def _():
        bytes_of(packs.at[pl.ds(0, n_sp - 1)], a_s.at[0])
        bytes_of(sendb.at[pl.ds(0, n_dp - 1)], b_s.at[0])
        for o in range(1, n_tp):
            bytes_of(sendb, b_s.at[o])
        bytes_of(cxb, c_s.at[0])
        bytes_of(cxb.at[pl.ds(1, n_sp - 1)], c_s.at[1])

    @pl.when(sp < n_sp - 1)
    def _():
        up.wait_send()

    @pl.when(sp > 0)
    def _():
        down.wait_send()


def per_device(
    latent, conditioning, context_cond, modulation, context, query_weight, key_projection,
    value_projection, out_weight, sink_head_logit, prefix_logit_bias,
):
    n_sp, n_tp, n_dp = lax.axis_size("sp"), lax.axis_size("tp"), lax.axis_size("dp")
    samples = conditioning.shape[0]
    _, tok, width = latent.shape
    n_ctx = context.shape[1]
    depth, cols = modulation.shape[1:]
    q_width = query_weight.shape[1]
    heads = q_width // HEAD_SIZE
    out_cols = out_weight.shape[1]
    blocks = tok // WINDOW_REACH
    window = tok + 2 * WINDOW_REACH
    keys = window + n_sp * n_ctx
    n_td = n_tp * n_dp
    act_rows = -(-(samples + 1) // 8) * 8
    pack_rows = -(-(3 * samples + 2) // 8) * 8
    row_table, col_table = rotary_tables(n_sp * tok // GRID_W)
    table = np.concatenate([col_table, row_table], axis=1)
    vm = pltpu.VMEM
    dma = pltpu.SemaphoreType.DMA
    group = n_dp * cols
    scratch = [
        vm((tok, width), BF16), vm((samples, depth), BF16), vm((depth,), BF16),
        vm((3, depth, cols), BF16), vm((2, n_ctx, width), BF16), vm((width, q_width + LANES), BF16),
        vm(out_weight.shape, BF16), pltpu.SMEM((heads,), F32), pltpu.SMEM((heads,), F32),
        vm(table.shape, F32),
        vm((act_rows, depth), F32), vm((pack_rows, cols), F32), vm((pack_rows, cols), BF16),
        vm((2 * n_sp - 1, pack_rows, cols), BF16), vm((2, pack_rows, cols), F32),
        vm((n_dp, 2, 8, cols), BF16), vm((n_tp, n_dp // 2, 2, 8, cols), BF16),
        vm((n_tp, 8, group), F32),
        vm((n_tp, tok, group), F32), vm((n_tp, 2 * n_ctx, group), F32), vm((tok, group), BF16),
        vm((2 * n_ctx, group), BF16), vm((LANES, width), BF16), vm((tok, LANES), F32),
        vm((tok, LANES), F32), vm((tok, q_width + LANES), F32), vm((2 * n_ctx, LANES), F32),
        vm((window, LANES), BF16), vm((2, n_ctx, LANES), BF16), vm((n_sp, n_ctx, LANES), BF16),
        vm((keys, LANES), BF16), vm((keys, LANES), BF16),
        vm((blocks, heads * WINDOW_REACH, LANES), BF16),
        vm((n_tp, blocks, WINDOW_REACH, q_width), BF16),
        dma((11,)), dma((1,)), dma((1,)), dma((1,)), dma((1,)), dma((n_tp,)), dma((n_tp,)),
        dma((2,)), dma((2,)), dma((2,)), dma((1,)), dma((2,)), dma((blocks, 2)),
    ]
    stays = pl.BlockSpec(memory_space=pltpu.HBM)
    out = pl.pallas_call(
        functools.partial(block_kernel, (n_sp, n_tp, n_dp, samples)),
        out_shape=pltpu.VMEM((tok, out_cols), F32),
        in_specs=[stays] * 12,
        out_specs=pl.BlockSpec(memory_space=pltpu.VMEM),
        scratch_shapes=scratch,
        compiler_params=pltpu.CompilerParams(
            collective_id=0, has_side_effects=True, vmem_limit_bytes=66000000
        ),
        name="fused_block",
    )(
        latent[0], conditioning, context_cond, modulation, context[0], query_weight,
        key_projection.T, value_projection.T, out_weight, sink_head_logit, prefix_logit_bias,
        jnp.asarray(table),
    )
    return out[None]


def solution(mesh):
    placed = (
        P("dp", "sp", None),
        P(None, "sp"),
        P("sp"),
        P(None, "sp", ("tp", "dp")),
        P("dp", "sp", None),
        P(None, "tp"),
        P(None, "tp"),
        P(None, "tp"),
        P(None, "tp"),
        P("tp"),
        P("tp"),
    )
    return jax.shard_map(
        per_device, mesh=mesh, in_specs=placed, out_specs=P("dp", "sp", "tp"), check_vma=False
    )
```

```python
import functools

import jax
import jax.numpy as jnp
import numpy as np
from jax import lax
from jax.experimental import pallas as pl
from jax.experimental.pallas import tpu as pltpu
from jax.sharding import PartitionSpec as P

HEAD_SIZE = 64
GRID_W = 64
WINDOW_REACH = 128
NORM_EPSILON = 1e-06
ROTARY_BASE = 10000.0
MASKED = -1e30
LANES = 128
MESH = pl.DeviceIdType.MESH
F32 = jnp.float32
BF16 = jnp.bfloat16


def rotary_tables(grid_rows):
    half = HEAD_SIZE // 2
    quarter = half // 2
    lane = np.arange(LANES) % HEAD_SIZE
    frequency = ROTARY_BASE ** (-2.0 * (lane % quarter) / half)
    frequency = frequency.astype(np.float32).astype(np.float64)
    sign = np.where(lane % half < quarter, -1.0, 1.0)
    by_row = lane < half

    def tables(count, keep):
        angles = np.arange(count)[:, None] * frequency[None, :]
        cosine = np.where(keep[None, :], np.cos(angles), 0.0)
        sine = np.where(keep[None, :], np.sin(angles) * sign[None, :], 0.0)
        return np.stack([cosine, sine]).astype(np.float32)

    return tables(grid_rows, by_row), tables(GRID_W, ~by_row)


def block_kernel(
    dims,
    lat_hbm, cond_hbm, cctx_hbm, mod_hbm, ctx_hbm, qw_hbm, kw_hbm, vw_hbm, ow_hbm,
    sink_hbm, bias_hbm, turn_hbm,
    outv,
    lat, cond, cctx, mod, ctx, wall, ow, sink, bias, angles,
    act, packf, pack, packs, total, sendb, slots, modv, gatef, gates, gateb, gatev,
    xn, xnc, nrm, nrmc, kvw, cosv, sinv, acc, accc, kvb, cxs, cxb, kd, vd, q4, att,
    in_sem, a_s, a_r, x_s, x_r, b_s, b_r, h_s, h_r, c_s, c_r, g_s, g_r, v_s, v_r, w_s, w_r,
):
    n_sp, n_tp, n_dp, samples = dims
    sp, tp, dp = lax.axis_index("sp"), lax.axis_index("tp"), lax.axis_index("dp")
    n_td = n_tp * n_dp
    me = tp * n_dp + dp
    tok, width = lat.shape
    cols = mod.shape[2]
    group = n_dp * cols
    n_ctx = ctx.shape[1]
    core, lead, pair = lax.rem(dp, 2), dp - lax.rem(dp, 2) + 1, dp // 2
    n_pairs = n_dp // 2
    reach = WINDOW_REACH
    blocks = tok // reach
    q_width = wall.shape[1] - LANES
    pairs = q_width // LANES
    heads = 2 * pairs

    barrier = pltpu.get_barrier_semaphore()
    @pl.when(core == 1)
    def _():
        for o in range(1, n_sp):
            for d in (2 * pair, 2 * pair + 1):
                pl.semaphore_signal(
                    barrier, inc=1, device_id={"sp": lax.rem(sp + o, n_sp), "dp": d},
                    device_id_type=MESH,
                )

    for o in range(1, n_td):
        lin = lax.rem(me + o, n_td)
        pl.semaphore_signal(
            barrier, inc=1, device_id={"tp": lin // n_dp, "dp": lax.rem(lin, n_dp)},
            device_id_type=MESH,
        )

    relayed = n_tp == 4
    direct = (1, 2) if relayed else range(1, n_tp)

    def partner(o):
        if not relayed:
            return lax.rem(tp + o, n_tp)
        x, y = lax.rem(tp, 2), tp // 2
        x = 1 - x if o % 2 else x
        y = 1 - y if o // 2 else y
        return 2 * y + x

    def owner(o):
        return partner(o) if relayed else lax.rem(tp + n_tp - o, n_tp)

    pairs_in = [
        (cond_hbm, cond, 0), (cctx_hbm, cctx, 1),
        (mod_hbm.at[pl.ds(0, 2)], mod.at[pl.ds(0, 2)], 2), (ctx_hbm, ctx.at[0], 3),
        (mod_hbm.at[2], mod.at[2], 4), (lat_hbm, lat, 5),
        (kw_hbm, kvw.at[pl.ds(0, HEAD_SIZE)], 6),
        (vw_hbm, kvw.at[pl.ds(HEAD_SIZE, HEAD_SIZE)], 6),
        (qw_hbm, wall.at[:, pl.ds(0, q_width)], 6), (turn_hbm, angles, 7), (sink_hbm, sink, 8),
        (bias_hbm, bias, 9), (ow_hbm, ow, 10),
    ]
    loads = [pltpu.make_async_copy(src, dst, in_sem.at[i]) for src, dst, i in pairs_in]
    for load in loads[:4]:
        load.start()

    def remote(src, dst, left, arrived, **device):
        return pltpu.make_async_remote_copy(
            src_ref=src, dst_ref=dst, send_sem=left, recv_sem=arrived, device_id=device,
            device_id_type=MESH,
        )

    def bytes_of(ref, semaphore):
        pltpu.make_async_copy(ref, ref, semaphore).wait()

    act[...] = jnp.zeros_like(act)
    loads[0].wait()
    loads[1].wait()
    for load in loads[4:]:
        load.start()
    act[0:samples, :] = cond[...].astype(F32)
    act[samples : samples + 1, :] = cctx[...].astype(F32).reshape(1, cctx.shape[0])
    v = act[...]
    activated = (v / (1.0 + jnp.exp(-v))).astype(BF16)
    packf[...] = jnp.zeros_like(packf)
    n_rows = samples + 1
    loads[2].wait()
    for m in range(2):
        part = jnp.dot(activated, mod[m], preferred_element_type=F32)
        packf[m * n_rows : (m + 1) * n_rows, :] = part[0:n_rows, :]
    pack[...] = packf[...].astype(BF16)

    pl.semaphore_wait(barrier, n_sp - 1 + n_td - 1)
    a_copies = [
        remote(
            pack, packs.at[2 * o - 1 + core if o else 0], a_s.at[0], a_r.at[0],
            sp=lax.rem(sp + o, n_sp), dp=lead,
        )
        for o in range(n_sp)
    ]
    for copy in a_copies[1:]:
        copy.start()
    spare = remote(ctx.at[0], ctx.at[1], x_s.at[0], x_r.at[0], dp=lead)

    @pl.when(core == 0)
    def _():
        a_copies[0].start()

    loads[4].wait()
    gatef[...] = jnp.dot(activated, mod[2], preferred_element_type=F32)
    v_copies = [
        remote(
            gatef, gates.at[2 * o - 1 + core if o else 0], v_s.at[0], v_r.at[0],
            sp=lax.rem(sp + o, n_sp), dp=lead,
        )
        for o in range(n_sp)
    ]
    for copy in v_copies[1:]:
        copy.start()
    loads[3].wait()

    @pl.when(core == 0)
    def _():
        v_copies[0].start()
        spare.start()

    chunk = 64

    def normalise(src, dst, first, last):
        def body(i, carry):
            rows = pl.ds(pl.multiple_of(i * chunk, chunk), chunk)
            x = src[rows, :].astype(F32)
            x = x - jnp.mean(x, axis=-1, keepdims=True)
            spread = jnp.mean(x * x, axis=-1, keepdims=True)
            x = x * lax.rsqrt(spread + NORM_EPSILON)
            for t in range(n_tp):
                dst[t, rows, :] = x[:, t * group : (t + 1) * group]
            return carry

        lax.fori_loop(first, last, body, 0)

    def normalise_context(which):
        for i in range(0, n_ctx, chunk):
            x = ctx[which, i : i + chunk, :].astype(F32)
            x = x - jnp.mean(x, axis=-1, keepdims=True)
            spread = jnp.mean(x * x, axis=-1, keepdims=True)
            x = x * lax.rsqrt(spread + NORM_EPSILON)
            at = which * n_ctx + i
            for t in range(n_tp):
                xnc[t, at : at + chunk, :] = x[:, t * group : (t + 1) * group]

    loads[5].wait()
    normalise(lat, xn, 0, tok // chunk)

    @pl.when(core == 1)
    def _():
        normalise_context(0)
        spare.wait_recv()
        normalise_context(1)


    b_copies = [
        remote(
            sendb.at[lax.rem(dp + e, n_dp)], slots.at[o, pair], b_s.at[0], b_r.at[o],
            tp=partner(o), dp=lax.rem(dp + e, n_dp),
        )
        for o in range(n_tp)
        for e in range(n_dp)
        if o or e
    ]

    @pl.when(core == 1)
    def _():
        bytes_of(packs, a_r.at[0])
        for c in range(2):
            summed = packf[...] if c else packs[0].astype(F32)
            for o in range(1, n_sp):
                summed = summed + packs[2 * o - 1 + c].astype(F32)
            total[c] = summed
        for d in range(n_dp):
            for c in range(2):
                rows = [
                    total[c, source : source + 1, :]
                    for source in (d, n_rows + d, samples, n_rows + samples)
                ]
                rows.append(jnp.zeros((4, cols), F32))
                sendb[d, c] = jnp.concatenate(rows, axis=0).astype(BF16)
        for copy in b_copies:
            copy.start()
        slots[0, pair] = sendb[dp]

    bytes_of(wall, in_sem.at[6])
    for load in loads[9:12]:
        load.wait()
    groups = tok // GRID_W
    for g in range(groups):
        row = pl.ds(GRID_W + sp * groups + g, 1)
        span = slice(g * GRID_W, (g + 1) * GRID_W)
        cosv[span, :] = angles[0, row, :] + angles[0, 0:GRID_W, :]
        sinv[span, :] = angles[1, row, :] + angles[1, 0:GRID_W, :]
    for j in range(width // LANES):
        span = slice(j * LANES, (j + 1) * LANES)
        wall[span, q_width:] = kvw[:, span].astype(F32).T.astype(BF16)

    def condition(src, dst, count, o, g, shift_row, scale_row):
        scale = 1.0 + modv[o, scale_row : scale_row + 1, :]
        shift = modv[o, shift_row : shift_row + 1, :]
        for i in range(0, count, chunk):
            rows = slice(i, i + chunk)
            dst[rows, :] = (src[g, rows, :] * scale + shift).astype(BF16)

    c_copies = [remote(cxs.at[0], cxb.at[0], c_s.at[0], c_r.at[0], dp=dp - core)]
    for r in range(1, n_sp):
        for c in range(2):
            c_copies.append(
                remote(
                    cxs.at[c], cxb.at[r], c_s.at[0], c_r.at[0],
                    sp=lax.rem(sp + r, n_sp), dp=2 * pair + c,
                )
            )
    for o in range(n_tp):
        if o:
            bytes_of(slots.at[o], b_r.at[o])
        else:
            @pl.when(core == 0)
            def _():
                bytes_of(slots.at[0], b_r.at[0])

            if n_pairs > 1:
                @pl.when(core == 1)
                def _():
                    bytes_of(slots.at[0, pl.ds(1, n_pairs - 1)], b_r.at[0])
        for d in range(n_dp):
            modv[o, :, d * cols : (d + 1) * cols] = slots[o, d // 2, d % 2].astype(F32)
        g = owner(o)
        weight_rows = pl.ds(pl.multiple_of(g * group, group), group)

        @pl.when(core == 1)
        def _():
            condition(xnc, nrmc, 2 * n_ctx, o, g, 2, 3)
            u = jnp.dot(nrmc[...], wall[weight_rows, q_width:], preferred_element_type=F32)
            if o:
                u = accc[...] + u
            if o < n_tp - 1:
                accc[...] = u
            else:
                cxs[0] = u[n_ctx:, :].astype(BF16)
                cxs[1] = u[0:n_ctx, :].astype(BF16)
                for copy in c_copies[1:] + c_copies[:1]:
                    copy.start()
                cxb[0] = u[0:n_ctx, :].astype(BF16)

        condition(xn, nrm, tok, o, g, 0, 1)
        u = jnp.dot(nrm[...], wall[weight_rows, :], preferred_element_type=F32)
        if o:
            u = acc[...] + u
        acc[...] = u

    half = HEAD_SIZE // 2
    quarter = half // 2

    def turn(u, cosine, sine):
        w = u.shape[1]
        lane = lax.broadcasted_iota(jnp.int32, u.shape, 1)
        first = lax.rem(lane, half) < quarter
        swapped = jnp.where(first, pltpu.roll(u, w - quarter, 1), pltpu.roll(u, quarter, 1))
        return u * cosine + swapped * sine

    def low_half(shape):
        return lax.broadcasted_iota(jnp.int32, shape, 1) < HEAD_SIZE

    def expand(x, at):
        low = low_half(x.shape)
        other = pltpu.roll(x, HEAD_SIZE, 1)
        span = slice(at, at + x.shape[0])
        kd[span, :] = jnp.where(low, x, other).astype(BF16)
        vd[span, :] = jnp.where(low, other, x).astype(BF16)

    u = acc[:, q_width:]
    kv_rows = jnp.where(low_half(u.shape), turn(u, cosv[...], sinv[...]), u)
    kvb[reach : reach + tok, :] = kv_rows.astype(BF16)

    up = remote(
        kvb.at[pl.ds(tok, reach)], kvb.at[pl.ds(0, reach)], h_s.at[0], h_r.at[0],
         sp=lax.rem(sp + 1, n_sp)
    )
    down = remote(
        kvb.at[pl.ds(reach, reach)], kvb.at[pl.ds(reach + tok, reach)], h_s.at[0], h_r.at[1],
        sp=lax.rem(sp + n_sp - 1, n_sp),
    )

    @pl.when(sp < n_sp - 1)
    def _():
        up.start()

    @pl.when(sp > 0)
    def _():
        down.start()

    expand(kv_rows, reach)

    factor = HEAD_SIZE ** (-0.5)
    for p in range(pairs):
        t = turn(acc[:, p * LANES : (p + 1) * LANES], cosv[...], sinv[...]) * factor
        low = low_half(t.shape)
        for parity, kept in ((0, jnp.where(low, t, 0.0)), (1, jnp.where(low, 0.0, t))):
            kept = kept.astype(BF16)
            at = (2 * p + parity) * reach
            for b in range(blocks):
                q4[b, at : at + reach, :] = kept[b * reach : (b + 1) * reach, :]

    window = tok + 2 * reach
    nt = (((1,), (1,)), ((), ()))
    n_all_ctx = n_sp * n_ctx
    delta = lax.broadcasted_iota(jnp.int32, (reach, reach), 1) - lax.broadcasted_iota(
        jnp.int32, (reach, reach), 0
    )
    far = 4 * reach
    low_edge = jnp.where(sp == 0, far, 0)
    high_edge = jnp.where(sp == n_sp - 1, -far, 0)

    def scores(b, first, count):
        keys = kd[first : first + count, :]
        return lax.dot_general(q4[b], keys, nt, preferred_element_type=F32)

    def tiles(s, h):
        rows = slice(h * reach, (h + 1) * reach)
        return [s[rows, c * LANES : (c + 1) * LANES] for c in range(s.shape[1] // LANES)]

    def soften(parts, highest):
        powers = [jnp.exp(s - highest) for s in parts]
        mass = powers[0]
        for e in powers[1:]:
            mass = mass + e
        powers = jnp.concatenate([e.astype(BF16) for e in powers], axis=1)
        return powers, jnp.sum(mass, axis=-1, keepdims=True)

    def top_of(parts):
        top = parts[0]
        for s in parts[1:]:
            top = jnp.maximum(top, s)
        return jnp.max(top, axis=-1, keepdims=True)

    def weigh(powers, first):
        e = jnp.concatenate(powers, axis=0)
        return jnp.dot(e, vd[first : first + e.shape[1], :], preferred_element_type=F32)

    def within(b):
        first, last = max(b - 1, 0), min(b + 1, blocks - 1)
        at = reach + first * reach
        s = scores(b, at, (last - first + 1) * reach)
        tops, masses, powers = [], [], []
        for h in range(heads):
            parts = tiles(s, h)
            if b > 0:
                parts[0] = jnp.where(delta >= 0, parts[0], MASKED)
            if b < blocks - 1:
                parts[-1] = jnp.where(delta <= 0, parts[-1], MASKED)
            highest = jnp.maximum(top_of(parts), sink[h])
            e, mass = soften(parts, highest)
            tops.append(highest)
            masses.append(mass + jnp.exp(sink[h] - highest))
            powers.append(e)
        return tops, masses, weigh(powers, at)


    def beyond(b, state, some):
        tops, masses, weighed = state
        first, last = some[0] * reach, (some[-1] + 1) * reach
        q2 = q4[b, first:last, :]

        def scores(at, count):
            keys = kd[at : at + count, :]
            return lax.dot_general(q2, keys, nt, preferred_element_type=F32)

        parts_of = [(window, scores(window, n_all_ctx))]
        edges = []
        if b == 0:
            edges.append((0, lambda s: jnp.where(delta >= low_edge, s, MASKED)))
        if b == blocks - 1:
            edges.append((reach + tok, lambda s: jnp.where(delta <= high_edge, s, MASKED)))
        for at, _ in edges:
            parts_of.append((at, scores(at, reach)))
        fades, powers = {}, [[] for _ in parts_of]
        for i, h in enumerate(some):
            groups = [[s + bias[h] for s in tiles(parts_of[0][1], i)]]
            for (_, mask), (_, s) in zip(edges, parts_of[1:]):
                groups.append([mask(s) for s in tiles(s, i)])
            top = jnp.maximum(top_of(sum(groups, [])), tops[h])
            fade = jnp.exp(tops[h] - top)
            mass = masses[h] * fade
            for kept, parts in zip(powers, groups):
                e, more = soften(parts, top)
                kept.append(e)
                mass = mass + more
            share = 1.0 / mass
            fades[h] = (fade * share, share)
        more = weigh(powers[0], window)
        for kept, (at, _) in zip(powers[1:], parts_of[1:]):
            more = more + weigh(kept, at)
        low = low_half((reach, LANES))
        for p in range(some[0] // 2, some[-1] // 2 + 1):
            halves = []
            for h in (2 * p, 2 * p + 1):
                rows = slice(h * reach, (h + 1) * reach)
                mine = slice(h * reach - first, (h + 1) * reach - first)
                halves.append(weighed[rows, :] * fades[h][0] + more[mine, :] * fades[h][1])
            att[0, b, :, p * LANES : (p + 1) * LANES] = jnp.where(low, *halves).astype(BF16)
        lanes = pl.ds(some[0] * HEAD_SIZE, len(some) * HEAD_SIZE)
        for o in direct:
            remote(
                att.at[0, b, :, lanes], att.at[o, b, :, lanes], g_s.at[0], g_r.at[b, 0],
                tp=partner(o),
            ).start()

    def forward(b):
        for o in direct:
            part = pl.ds((o - 1) * (reach // 2), reach // 2)
            remote(
                att.at[o, b, part], att.at[3, b, part], g_s.at[0], g_r.at[b, 1], tp=partner(3 - o)
            ).start()

    order = list(range(1, blocks - 1)) + ([0, blocks - 1] if blocks > 1 else [0])
    states = {}
    for b in order:
        states[b] = within(b)
    w_copies = [
        remote(
            gateb.at[lax.rem(dp + e, n_dp)], gatev.at[pair], w_s.at[0], w_r.at[0],
            dp=lax.rem(dp + e, n_dp),
        )
        for e in range(1, n_dp)
    ]

    @pl.when(core == 1)
    def _():
        bytes_of(gates, v_r.at[0])
        for c in range(2):
            summed = gatef[...] if c else gates[0]
            for o in range(1, n_sp):
                summed = summed + gates[2 * o - 1 + c]
            for d in range(n_dp):
                gateb[d, c] = jnp.broadcast_to(summed[d : d + 1, :], (8, cols))
        for copy in w_copies:
            copy.start()
        gatev[pair] = gateb[dp]


    @pl.when(core == 0)
    def _():
        bytes_of(cxb.at[pl.ds(0, n_sp)], c_r.at[0])

    @pl.when(core == 1)
    def _():
        bytes_of(cxb.at[pl.ds(1, n_sp - 1)], c_r.at[0])

    for r in range(n_sp):
        expand(cxb[r].astype(F32), window + r * n_ctx)
    for b in order:
        if b == 0:
            @pl.when(sp > 0)
            def _():
                up.wait_recv()

            @pl.when(sp == 0)
            def _():
                kvb[0:reach, :] = jnp.zeros((reach, LANES), BF16)

            expand(kvb[0:reach, :].astype(F32), 0)
        if b == blocks - 1:
            @pl.when(sp < n_sp - 1)
            def _():
                down.wait_recv()

            @pl.when(sp == n_sp - 1)
            def _():
                kvb[reach + tok : window, :] = jnp.zeros((reach, LANES), BF16)

            expand(kvb[reach + tok : window, :].astype(F32), reach + tok)
        if b == order[0]:
            for p in range(pairs):
                beyond(b, states[b], (2 * p, 2 * p + 1))
        else:
            beyond(b, states[b], tuple(range(heads)))

    loads[12].wait()
    out_cols = ow.shape[1]
    mine = pl.ds(pl.multiple_of(tp * out_cols, out_cols), out_cols)

    @pl.when(core == 0)
    def _():
        bytes_of(gatev, w_r.at[0])

    if n_pairs > 1:
        @pl.when(core == 1)
        def _():
            bytes_of(gatev.at[pl.ds(1, n_pairs - 1)], w_r.at[0])

    for d in range(n_dp):
        modv[0, :, d * cols : (d + 1) * cols] = gatev[d // 2, d % 2]
    gate = modv[0, 0:1, :]

    def project(b, o):
        w = ow[pl.ds(pl.multiple_of(owner(o) * q_width, q_width), q_width), :]
        return jnp.dot(att[o, b], w, preferred_element_type=F32)

    for b in order:
        bytes_of(att.at[pl.ds(1, len(direct)), b], g_r.at[b, 0])
        if relayed:
            forward(b)
        mixed = project(b, 0)
        for o in direct:
            mixed = mixed + project(b, o)
        outv[b * reach : (b + 1) * reach, :] = mixed
    for b in order:
        rows = slice(b * reach, (b + 1) * reach)
        mixed = outv[rows, :]
        if relayed:
            bytes_of(att.at[3, b], g_r.at[b, 1])
            mixed = mixed + project(b, 3)
        outv[rows, :] = lat[rows, mine].astype(F32) + gate * mixed

    bytes_of(att.at[pl.ds(1, n_tp - 1)], g_s.at[0])

    @pl.when(core == 0)
    def _():
        bytes_of(packs.at[pl.ds(0, n_sp)], a_s.at[0])
        bytes_of(gates.at[pl.ds(0, n_sp)], v_s.at[0])
        spare.wait_send()

    @pl.when(core == 1)
    def _():
        bytes_of(packs.at[pl.ds(0, n_sp - 1)], a_s.at[0])
        bytes_of(gates.at[pl.ds(0, n_sp - 1)], v_s.at[0])
        bytes_of(sendb.at[pl.ds(0, n_td - 1)], b_s.at[0])
        bytes_of(gateb.at[pl.ds(0, n_dp - 1)], w_s.at[0])
        bytes_of(cxb, c_s.at[0])

    edge = jnp.logical_or(sp == 0, sp == n_sp - 1)

    @pl.when(edge)
    def _():
        bytes_of(kvb.at[pl.ds(0, reach)], h_s.at[0])

    @pl.when(jnp.logical_not(edge))
    def _():
        bytes_of(kvb.at[pl.ds(0, 2 * reach)], h_s.at[0])


def per_device(
    latent, conditioning, context_cond, modulation, context, query_weight, key_projection,
    value_projection, out_weight, sink_head_logit, prefix_logit_bias,
):
    n_sp, n_tp, n_dp = lax.axis_size("sp"), lax.axis_size("tp"), lax.axis_size("dp")
    samples = conditioning.shape[0]
    _, tok, width = latent.shape
    n_ctx = context.shape[1]
    depth, cols = modulation.shape[1:]
    q_width = query_weight.shape[1]
    heads = q_width // HEAD_SIZE
    out_cols = out_weight.shape[1]
    blocks = tok // WINDOW_REACH
    window = tok + 2 * WINDOW_REACH
    keys = window + n_sp * n_ctx
    n_td = n_tp * n_dp
    act_rows = -(-(samples + 1) // 8) * 8
    pack_rows = -(-(2 * samples + 2) // 8) * 8
    row_table, col_table = rotary_tables(n_sp * tok // GRID_W)
    table = np.concatenate([col_table, row_table], axis=1)
    vm = pltpu.VMEM
    dma = pltpu.SemaphoreType.DMA
    group = n_dp * cols
    scratch = [
        vm((tok, width), BF16), vm((samples, depth), BF16), vm((depth,), BF16),
        vm((3, depth, cols), BF16), vm((2, n_ctx, width), BF16), vm((width, q_width + LANES), BF16),
        vm(out_weight.shape, BF16), pltpu.SMEM((heads,), F32), pltpu.SMEM((heads,), F32),
        vm(table.shape, F32),
        vm((act_rows, depth), F32), vm((pack_rows, cols), F32), vm((pack_rows, cols), BF16),
        vm((2 * n_sp - 1, pack_rows, cols), BF16), vm((2, pack_rows, cols), F32),
        vm((n_td, 2, 8, cols), BF16), vm((n_tp, n_dp // 2, 2, 8, cols), BF16),
        vm((n_tp, 8, group), F32), vm((act_rows, cols), F32),
        vm((2 * n_sp - 1, act_rows, cols), F32), vm((n_dp, 2, 8, cols), F32),
        vm((n_dp // 2, 2, 8, cols), F32),
        vm((n_tp, tok, group), F32), vm((n_tp, 2 * n_ctx, group), F32), vm((tok, group), BF16),
        vm((2 * n_ctx, group), BF16), vm((LANES, width), BF16), vm((tok, LANES), F32),
        vm((tok, LANES), F32), vm((tok, q_width + LANES), F32), vm((2 * n_ctx, LANES), F32),
        vm((window, LANES), BF16), vm((2, n_ctx, LANES), BF16), vm((2 * n_sp - 1, n_ctx, LANES), BF16),
        vm((keys, LANES), BF16), vm((keys, LANES), BF16),
        vm((blocks, heads * WINDOW_REACH, LANES), BF16),
        vm((n_tp, blocks, WINDOW_REACH, q_width), BF16),
        dma((11,)), dma((1,)), dma((1,)), dma((1,)), dma((1,)), dma((1,)), dma((n_tp,)),
        dma((1,)), dma((2,)), dma((1,)), dma((1,)), dma((1,)), dma((blocks, 2)), dma((1,)),
        dma((1,)), dma((1,)), dma((1,)),
    ]
    stays = pl.BlockSpec(memory_space=pltpu.HBM)
    out = pl.pallas_call(
        functools.partial(block_kernel, (n_sp, n_tp, n_dp, samples)),
        out_shape=pltpu.VMEM((tok, out_cols), F32),
        in_specs=[stays] * 12,
        out_specs=pl.BlockSpec(memory_space=pltpu.VMEM),
        scratch_shapes=scratch,
        compiler_params=pltpu.CompilerParams(
            collective_id=0, has_side_effects=True, vmem_limit_bytes=66000000
        ),
        name="fused_block",
    )(
        latent[0], conditioning, context_cond, modulation, context[0], query_weight,
        key_projection.T, value_projection.T, out_weight, sink_head_logit, prefix_logit_bias,
        jnp.asarray(table),
    )
    return out[None]


def solution(mesh):
    placed = (
        P("dp", "sp", None),
        P(None, "sp"),
        P("sp"),
        P(None, "sp", ("tp", "dp")),
        P("dp", "sp", None),
        P(None, "tp"),
        P(None, "tp"),
        P(None, "tp"),
        P(None, "tp"),
        P("tp"),
        P("tp"),
    )
    return jax.shard_map(
        per_device, mesh=mesh, in_specs=placed, out_specs=P("dp", "sp", "tp"), check_vma=False
    )
```

```python
import functools

import jax
import jax.numpy as jnp
import numpy as np
from jax import lax
from jax.experimental import pallas as pl
from jax.experimental.pallas import tpu as pltpu
from jax.sharding import PartitionSpec as P

HEAD_SIZE = 64
GRID_W = 64
WINDOW_REACH = 128
NORM_EPSILON = 1e-06
ROTARY_BASE = 10000.0
MASKED = -1e30
LANES = 128
MESH = pl.DeviceIdType.MESH
F32 = jnp.float32
BF16 = jnp.bfloat16


def rotary_tables(grid_rows):
    half = HEAD_SIZE // 2
    quarter = half // 2
    lane = np.arange(LANES) % HEAD_SIZE
    frequency = ROTARY_BASE ** (-2.0 * (lane % quarter) / half)
    frequency = frequency.astype(np.float32).astype(np.float64)
    sign = np.where(lane % half < quarter, -1.0, 1.0)
    by_row = lane < half

    def tables(count, keep):
        angles = np.arange(count)[:, None] * frequency[None, :]
        cosine = np.where(keep[None, :], np.cos(angles), 0.0)
        sine = np.where(keep[None, :], np.sin(angles) * sign[None, :], 0.0)
        return np.stack([cosine, sine]).astype(np.float32)

    return tables(grid_rows, by_row), tables(GRID_W, ~by_row)


def block_kernel(
    dims,
    lat_hbm, cond_hbm, cctx_hbm, mod_hbm, ctx_hbm, qw_hbm, kw_hbm, vw_hbm, ow_hbm,
    sink_hbm, bias_hbm, turn_hbm,
    outv,
    lat, cond, cctx, mod, ctx, wall, ow, sink, bias, angles,
    act, packf, pack, packs, total, sendb, slots, modv, gatef, gates, gateb, gatev,
    xn, xnc, nrm, nrmc, kvw, cosv, sinv, acc, accc, kvb, cxs, cxb, kd, vd, q4, att,
    in_sem, a_s, a_r, x_s, x_r, b_s, b_r, h_s, h_r, c_s, c_r, g_s, g_r, v_s, v_r, w_s, w_r,
):
    n_sp, n_tp, n_dp, samples = dims
    sp, tp, dp = lax.axis_index("sp"), lax.axis_index("tp"), lax.axis_index("dp")
    n_td = n_tp * n_dp
    me = tp * n_dp + dp
    tok, width = lat.shape
    cols = mod.shape[2]
    group = n_dp * cols
    n_ctx = ctx.shape[1]
    core, lead, pair = lax.rem(dp, 2), dp - lax.rem(dp, 2) + 1, dp // 2
    n_pairs = n_dp // 2
    reach = WINDOW_REACH
    blocks = tok // reach
    q_width = wall.shape[1] - LANES
    pairs = q_width // LANES
    heads = 2 * pairs

    barrier = pltpu.get_barrier_semaphore()
    @pl.when(core == 1)
    def _():
        for o in range(1, n_sp):
            for d in (2 * pair, 2 * pair + 1):
                pl.semaphore_signal(
                    barrier, inc=1, device_id={"sp": lax.rem(sp + o, n_sp), "dp": d},
                    device_id_type=MESH,
                )

    for o in range(1, n_td):
        lin = lax.rem(me + o, n_td)
        pl.semaphore_signal(
            barrier, inc=1, device_id={"tp": lin // n_dp, "dp": lax.rem(lin, n_dp)},
            device_id_type=MESH,
        )

    relayed = n_tp == 4
    direct = (1, 2) if relayed else range(1, n_tp)

    def partner(o):
        if not relayed:
            return lax.rem(tp + o, n_tp)
        x, y = lax.rem(tp, 2), tp // 2
        x = 1 - x if o % 2 else x
        y = 1 - y if o // 2 else y
        return 2 * y + x

    def owner(o):
        return partner(o) if relayed else lax.rem(tp + n_tp - o, n_tp)

    pairs_in = [
        (cond_hbm, cond, 0), (cctx_hbm, cctx, 1),
        (mod_hbm.at[pl.ds(0, 2)], mod.at[pl.ds(0, 2)], 2), (ctx_hbm, ctx.at[0], 3),
        (mod_hbm.at[2], mod.at[2], 4), (lat_hbm, lat, 5),
        (kw_hbm, kvw.at[pl.ds(0, HEAD_SIZE)], 6),
        (vw_hbm, kvw.at[pl.ds(HEAD_SIZE, HEAD_SIZE)], 6),
        (qw_hbm, wall.at[:, pl.ds(0, q_width)], 6), (turn_hbm, angles, 7), (sink_hbm, sink, 8),
        (bias_hbm, bias, 9), (ow_hbm, ow, 10),
    ]
    loads = [pltpu.make_async_copy(src, dst, in_sem.at[i]) for src, dst, i in pairs_in]
    for load in loads[:4]:
        load.start()

    def remote(src, dst, left, arrived, **device):
        return pltpu.make_async_remote_copy(
            src_ref=src, dst_ref=dst, send_sem=left, recv_sem=arrived, device_id=device,
            device_id_type=MESH,
        )

    def bytes_of(ref, semaphore):
        pltpu.make_async_copy(ref, ref, semaphore).wait()

    act[...] = jnp.zeros_like(act)
    loads[0].wait()
    loads[1].wait()
    for load in loads[4:]:
        load.start()
    act[0:samples, :] = cond[...].astype(F32)
    act[samples : samples + 1, :] = cctx[...].astype(F32).reshape(1, cctx.shape[0])
    v = act[...]
    activated = (v / (1.0 + jnp.exp(-v))).astype(BF16)
    packf[...] = jnp.zeros_like(packf)
    n_rows = samples + 1
    loads[2].wait()
    for m in range(2):
        part = jnp.dot(activated, mod[m], preferred_element_type=F32)
        packf[m * n_rows : (m + 1) * n_rows, :] = part[0:n_rows, :]
    pack[...] = packf[...].astype(BF16)

    pl.semaphore_wait(barrier, n_sp - 1 + n_td - 1)
    a_copies = [
        remote(
            pack, packs.at[2 * o - 1 + core if o else 0], a_s.at[0], a_r.at[0],
            sp=lax.rem(sp + o, n_sp), dp=lead,
        )
        for o in range(n_sp)
    ]
    for copy in a_copies[1:]:
        copy.start()
    spare = remote(ctx.at[0], ctx.at[1], x_s.at[0], x_r.at[0], dp=lead)

    @pl.when(core == 0)
    def _():
        a_copies[0].start()

    loads[4].wait()
    gatef[...] = jnp.dot(activated, mod[2], preferred_element_type=F32)
    v_copies = [
        remote(
            gatef, gates.at[2 * o - 1 + core if o else 0], v_s.at[0], v_r.at[0],
            sp=lax.rem(sp + o, n_sp), dp=lead,
        )
        for o in range(n_sp)
    ]
    for copy in v_copies[1:]:
        copy.start()
    loads[3].wait()

    @pl.when(core == 0)
    def _():
        v_copies[0].start()
        spare.start()

    chunk = 64

    def normalise(src, dst, first, last):
        def body(i, carry):
            rows = pl.ds(pl.multiple_of(i * chunk, chunk), chunk)
            x = src[rows, :].astype(F32)
            x = x - jnp.mean(x, axis=-1, keepdims=True)
            spread = jnp.mean(x * x, axis=-1, keepdims=True)
            x = x * lax.rsqrt(spread + NORM_EPSILON)
            for t in range(n_tp):
                dst[t, rows, :] = x[:, t * group : (t + 1) * group]
            return carry

        lax.fori_loop(first, last, body, 0)

    def normalise_context(which):
        for i in range(0, n_ctx, chunk):
            x = ctx[which, i : i + chunk, :].astype(F32)
            x = x - jnp.mean(x, axis=-1, keepdims=True)
            spread = jnp.mean(x * x, axis=-1, keepdims=True)
            x = x * lax.rsqrt(spread + NORM_EPSILON)
            at = which * n_ctx + i
            for t in range(n_tp):
                xnc[t, at : at + chunk, :] = x[:, t * group : (t + 1) * group]

    loads[5].wait()
    normalise(lat, xn, 0, tok // chunk)

    @pl.when(core == 1)
    def _():
        normalise_context(0)
        spare.wait_recv()
        normalise_context(1)


    b_copies = [
        remote(
            sendb.at[lax.rem(dp + e, n_dp)], slots.at[o, pair], b_s.at[0], b_r.at[o],
            tp=partner(o), dp=lax.rem(dp + e, n_dp),
        )
        for o in range(n_tp)
        for e in range(n_dp)
        if o or e
    ]

    @pl.when(core == 1)
    def _():
        bytes_of(packs, a_r.at[0])
        for c in range(2):
            summed = packf[...] if c else packs[0].astype(F32)
            for o in range(1, n_sp):
                summed = summed + packs[2 * o - 1 + c].astype(F32)
            total[c] = summed
        for d in range(n_dp):
            for c in range(2):
                rows = [
                    total[c, source : source + 1, :]
                    for source in (d, n_rows + d, samples, n_rows + samples)
                ]
                rows.append(jnp.zeros((4, cols), F32))
                sendb[d, c] = jnp.concatenate(rows, axis=0).astype(BF16)
        for copy in b_copies:
            copy.start()
        slots[0, pair] = sendb[dp]

    bytes_of(wall, in_sem.at[6])
    for load in loads[9:12]:
        load.wait()
    groups = tok // GRID_W
    for g in range(groups):
        row = pl.ds(GRID_W + sp * groups + g, 1)
        span = slice(g * GRID_W, (g + 1) * GRID_W)
        cosv[span, :] = angles[0, row, :] + angles[0, 0:GRID_W, :]
        sinv[span, :] = angles[1, row, :] + angles[1, 0:GRID_W, :]
    for j in range(width // LANES):
        span = slice(j * LANES, (j + 1) * LANES)
        wall[span, q_width:] = kvw[:, span].astype(F32).T.astype(BF16)

    def condition(src, dst, count, o, g, shift_row, scale_row):
        scale = 1.0 + modv[o, scale_row : scale_row + 1, :]
        shift = modv[o, shift_row : shift_row + 1, :]
        for i in range(0, count, chunk):
            rows = slice(i, i + chunk)
            dst[o, rows, :] = (src[g, rows, :] * scale + shift).astype(BF16)

    c_copies = [remote(cxs.at[0], cxb.at[0], c_s.at[0], c_r.at[0], dp=dp - core)]
    for r in range(1, n_sp):
        for c in range(2):
            c_copies.append(
                remote(
                    cxs.at[c], cxb.at[r], c_s.at[0], c_r.at[0],
                    sp=lax.rem(sp + r, n_sp), dp=2 * pair + c,
                )
            )
    def land(o):
        if o:
            bytes_of(slots.at[o], b_r.at[o])
        else:
            @pl.when(core == 0)
            def _():
                bytes_of(slots.at[0], b_r.at[0])

            if n_pairs > 1:
                @pl.when(core == 1)
                def _():
                    bytes_of(slots.at[0, pl.ds(1, n_pairs - 1)], b_r.at[0])
        for d in range(n_dp):
            modv[o, :, d * cols : (d + 1) * cols] = slots[o, d // 2, d % 2].astype(F32)

    def weight_rows(o):
        return pl.ds(pl.multiple_of(owner(o) * group, group), group)

    def context_part(o):
        condition(xnc, nrmc, 2 * n_ctx, o, owner(o), 2, 3)
        weights = wall[weight_rows(o), q_width:]
        return jnp.dot(nrmc[o], weights, preferred_element_type=F32)

    def latent_part(o):
        condition(xn, nrm, tok, o, owner(o), 0, 1)
        u = jnp.dot(nrm[o], wall[weight_rows(o), :], preferred_element_type=F32)
        acc[...] = acc[...] + u if o else u

    land(0)

    @pl.when(core == 1)
    def _():
        accc[...] = context_part(0)

    latent_part(0)

    @pl.when(core == 1)
    def _():
        u = accc[...]
        for o in range(1, n_tp):
            land(o)
            u = u + context_part(o)
        cxs[0] = u[n_ctx:, :].astype(BF16)
        cxs[1] = u[0:n_ctx, :].astype(BF16)
        for copy in c_copies[1:] + c_copies[:1]:
            copy.start()
        cxb[0] = u[0:n_ctx, :].astype(BF16)
        for o in range(1, n_tp):
            latent_part(o)

    @pl.when(core == 0)
    def _():
        for o in range(1, n_tp):
            land(o)
            latent_part(o)

    half = HEAD_SIZE // 2
    quarter = half // 2

    def turn(u, cosine, sine):
        w = u.shape[1]
        lane = lax.broadcasted_iota(jnp.int32, u.shape, 1)
        first = lax.rem(lane, half) < quarter
        swapped = jnp.where(first, pltpu.roll(u, w - quarter, 1), pltpu.roll(u, quarter, 1))
        return u * cosine + swapped * sine

    def low_half(shape):
        return lax.broadcasted_iota(jnp.int32, shape, 1) < HEAD_SIZE

    def expand(x, at):
        low = low_half(x.shape)
        other = pltpu.roll(x, HEAD_SIZE, 1)
        span = slice(at, at + x.shape[0])
        kd[span, :] = jnp.where(low, x, other).astype(BF16)
        vd[span, :] = jnp.where(low, other, x).astype(BF16)

    u = acc[:, q_width:]
    kv_rows = jnp.where(low_half(u.shape), turn(u, cosv[...], sinv[...]), u)
    kvb[reach : reach + tok, :] = kv_rows.astype(BF16)

    up = remote(
        kvb.at[pl.ds(tok, reach)], kvb.at[pl.ds(0, reach)], h_s.at[0], h_r.at[0],
         sp=lax.rem(sp + 1, n_sp)
    )
    down = remote(
        kvb.at[pl.ds(reach, reach)], kvb.at[pl.ds(reach + tok, reach)], h_s.at[0], h_r.at[1],
        sp=lax.rem(sp + n_sp - 1, n_sp),
    )

    @pl.when(sp < n_sp - 1)
    def _():
        up.start()

    @pl.when(sp > 0)
    def _():
        down.start()

    expand(kv_rows, reach)

    factor = HEAD_SIZE ** (-0.5)
    for p in range(pairs):
        t = turn(acc[:, p * LANES : (p + 1) * LANES], cosv[...], sinv[...]) * factor
        low = low_half(t.shape)
        for parity, kept in ((0, jnp.where(low, t, 0.0)), (1, jnp.where(low, 0.0, t))):
            kept = kept.astype(BF16)
            at = (2 * p + parity) * reach
            for b in range(blocks):
                q4[b, at : at + reach, :] = kept[b * reach : (b + 1) * reach, :]

    window = tok + 2 * reach
    nt = (((1,), (1,)), ((), ()))
    n_all_ctx = n_sp * n_ctx
    delta = lax.broadcasted_iota(jnp.int32, (reach, reach), 1) - lax.broadcasted_iota(
        jnp.int32, (reach, reach), 0
    )
    far = 4 * reach
    low_edge = jnp.where(sp == 0, far, 0)
    high_edge = jnp.where(sp == n_sp - 1, -far, 0)

    def scores(b, first, count):
        keys = kd[first : first + count, :]
        return lax.dot_general(q4[b], keys, nt, preferred_element_type=F32)

    def tiles(s, h):
        rows = slice(h * reach, (h + 1) * reach)
        return [s[rows, c * LANES : (c + 1) * LANES] for c in range(s.shape[1] // LANES)]

    def soften(parts, highest):
        powers = [jnp.exp(s - highest) for s in parts]
        mass = powers[0]
        for e in powers[1:]:
            mass = mass + e
        powers = jnp.concatenate([e.astype(BF16) for e in powers], axis=1)
        return powers, jnp.sum(mass, axis=-1, keepdims=True)

    def top_of(parts):
        top = parts[0]
        for s in parts[1:]:
            top = jnp.maximum(top, s)
        return jnp.max(top, axis=-1, keepdims=True)

    def weigh(powers, first):
        e = jnp.concatenate(powers, axis=0)
        return jnp.dot(e, vd[first : first + e.shape[1], :], preferred_element_type=F32)

    def within(b):
        first, last = max(b - 1, 0), min(b + 1, blocks - 1)
        at = reach + first * reach
        s = scores(b, at, (last - first + 1) * reach)
        tops, masses, powers = [], [], []
        for h in range(heads):
            parts = tiles(s, h)
            if b > 0:
                parts[0] = jnp.where(delta >= 0, parts[0], MASKED)
            if b < blocks - 1:
                parts[-1] = jnp.where(delta <= 0, parts[-1], MASKED)
            highest = jnp.maximum(top_of(parts), sink[h])
            e, mass = soften(parts, highest)
            tops.append(highest)
            masses.append(mass + jnp.exp(sink[h] - highest))
            powers.append(e)
        return tops, masses, weigh(powers, at)


    def beyond(b, state, some):
        tops, masses, weighed = state
        first, last = some[0] * reach, (some[-1] + 1) * reach
        q2 = q4[b, first:last, :]

        def scores(at, count):
            keys = kd[at : at + count, :]
            return lax.dot_general(q2, keys, nt, preferred_element_type=F32)

        parts_of = [(window, scores(window, n_all_ctx))]
        edges = []
        if b == 0:
            edges.append((0, lambda s: jnp.where(delta >= low_edge, s, MASKED)))
        if b == blocks - 1:
            edges.append((reach + tok, lambda s: jnp.where(delta <= high_edge, s, MASKED)))
        for at, _ in edges:
            parts_of.append((at, scores(at, reach)))
        fades, powers = {}, [[] for _ in parts_of]
        for i, h in enumerate(some):
            groups = [[s + bias[h] for s in tiles(parts_of[0][1], i)]]
            for (_, mask), (_, s) in zip(edges, parts_of[1:]):
                groups.append([mask(s) for s in tiles(s, i)])
            top = jnp.maximum(top_of(sum(groups, [])), tops[h])
            fade = jnp.exp(tops[h] - top)
            mass = masses[h] * fade
            for kept, parts in zip(powers, groups):
                e, more = soften(parts, top)
                kept.append(e)
                mass = mass + more
            share = 1.0 / mass
            fades[h] = (fade * share, share)
        more = weigh(powers[0], window)
        for kept, (at, _) in zip(powers[1:], parts_of[1:]):
            more = more + weigh(kept, at)
        low = low_half((reach, LANES))
        for p in range(some[0] // 2, some[-1] // 2 + 1):
            halves = []
            for h in (2 * p, 2 * p + 1):
                rows = slice(h * reach, (h + 1) * reach)
                mine = slice(h * reach - first, (h + 1) * reach - first)
                halves.append(weighed[rows, :] * fades[h][0] + more[mine, :] * fades[h][1])
            att[0, b, :, p * LANES : (p + 1) * LANES] = jnp.where(low, *halves).astype(BF16)

    middle = reach // 2

    def send(b, o, relay, first=0, count=q_width):
        if relayed:
            at = (o - 1) * middle if relay else (2 - o) * middle
            span = (b, pl.ds(at, middle), pl.ds(first, count))
        else:
            span = (b, slice(None), pl.ds(first, count))
        remote(
            att.at[(0, *span)], att.at[(o, *span)], g_s.at[0], g_r.at[b, 0 if relay else 1],
            tp=partner(o),
        ).start()

    def forward(b):
        bytes_of(att.at[1, b], g_r.at[b, 0])
        for o in direct:
            part = pl.ds((o - 1) * middle, middle)
            remote(
                att.at[o, b, part], att.at[3, b, part], g_s.at[0], g_r.at[b, 2], tp=partner(3 - o)
            ).start()

    order = list(range(1, blocks - 1)) + ([0, blocks - 1] if blocks > 1 else [0])
    states = {}
    early = order[: max(len(order) - 1, 1)]
    for b in early:
        states[b] = within(b)
    w_copies = [
        remote(
            gateb.at[lax.rem(dp + e, n_dp)], gatev.at[pair], w_s.at[0], w_r.at[0],
            dp=lax.rem(dp + e, n_dp),
        )
        for e in range(1, n_dp)
    ]

    @pl.when(core == 1)
    def _():
        bytes_of(gates, v_r.at[0])
        for c in range(2):
            summed = gatef[...] if c else gates[0]
            for o in range(1, n_sp):
                summed = summed + gates[2 * o - 1 + c]
            for d in range(n_dp):
                gateb[d, c] = jnp.broadcast_to(summed[d : d + 1, :], (8, cols))
        for copy in w_copies:
            copy.start()
        gatev[pair] = gateb[dp]


    @pl.when(core == 0)
    def _():
        bytes_of(cxb.at[pl.ds(0, n_sp)], c_r.at[0])

    @pl.when(core == 1)
    def _():
        bytes_of(cxb.at[pl.ds(1, n_sp - 1)], c_r.at[0])

    for r in range(n_sp):
        expand(cxb[r].astype(F32), window + r * n_ctx)
    held = []
    for b in order:
        if b not in states:
            states[b] = within(b)
        if b == 0:
            @pl.when(sp > 0)
            def _():
                up.wait_recv()

            @pl.when(sp == 0)
            def _():
                kvb[0:reach, :] = jnp.zeros((reach, LANES), BF16)

            expand(kvb[0:reach, :].astype(F32), 0)
        if b == blocks - 1:
            @pl.when(sp < n_sp - 1)
            def _():
                down.wait_recv()

            @pl.when(sp == n_sp - 1)
            def _():
                kvb[reach + tok : window, :] = jnp.zeros((reach, LANES), BF16)

            expand(kvb[reach + tok : window, :].astype(F32), reach + tok)
        if b == order[0]:
            for p in range(pairs):
                beyond(b, states[b], (2 * p, 2 * p + 1))
                for o in direct:
                    send(b, o, True, p * LANES, LANES)
        else:
            beyond(b, states[b], tuple(range(heads)))
            for o in direct:
                send(b, o, True)
        if relayed:
            held.append(b)
            if b == order[0] or b == order[-1]:
                for c in held:
                    for o in direct:
                        send(c, o, False)
                held.clear()

    loads[12].wait()
    out_cols = ow.shape[1]
    mine = pl.ds(pl.multiple_of(tp * out_cols, out_cols), out_cols)

    @pl.when(core == 0)
    def _():
        bytes_of(gatev, w_r.at[0])

    if n_pairs > 1:
        @pl.when(core == 1)
        def _():
            bytes_of(gatev.at[pl.ds(1, n_pairs - 1)], w_r.at[0])

    for d in range(n_dp):
        modv[0, :, d * cols : (d + 1) * cols] = gatev[d // 2, d % 2]
    gate = modv[0, 0:1, :]

    def project(b, o):
        w = ow[pl.ds(pl.multiple_of(owner(o) * q_width, q_width), q_width), :]
        return jnp.dot(att[o, b], w, preferred_element_type=F32)

    for b in order:
        if relayed:
            forward(b)
        else:
            bytes_of(att.at[pl.ds(1, n_tp - 1), b], g_r.at[b, 0])
        outv[b * reach : (b + 1) * reach, :] = project(b, 0)
    for b in order:
        if relayed:
            bytes_of(att.at[1, b], g_r.at[b, 1])
        rows = slice(b * reach, (b + 1) * reach)
        mixed = outv[rows, :]
        for o in direct:
            mixed = mixed + project(b, o)
        outv[rows, :] = mixed
    for b in order:
        rows = slice(b * reach, (b + 1) * reach)
        mixed = outv[rows, :]
        if relayed:
            bytes_of(att.at[3, b], g_r.at[b, 2])
            mixed = mixed + project(b, 3)
        outv[rows, :] = lat[rows, mine].astype(F32) + gate * mixed

    bytes_of(att.at[pl.ds(1, n_tp - 1)], g_s.at[0])

    @pl.when(core == 0)
    def _():
        bytes_of(packs.at[pl.ds(0, n_sp)], a_s.at[0])
        bytes_of(gates.at[pl.ds(0, n_sp)], v_s.at[0])
        spare.wait_send()

    @pl.when(core == 1)
    def _():
        bytes_of(packs.at[pl.ds(0, n_sp - 1)], a_s.at[0])
        bytes_of(gates.at[pl.ds(0, n_sp - 1)], v_s.at[0])
        bytes_of(sendb.at[pl.ds(0, n_td - 1)], b_s.at[0])
        bytes_of(gateb.at[pl.ds(0, n_dp - 1)], w_s.at[0])
        bytes_of(cxb, c_s.at[0])

    edge = jnp.logical_or(sp == 0, sp == n_sp - 1)

    @pl.when(edge)
    def _():
        bytes_of(kvb.at[pl.ds(0, reach)], h_s.at[0])

    @pl.when(jnp.logical_not(edge))
    def _():
        bytes_of(kvb.at[pl.ds(0, 2 * reach)], h_s.at[0])


def per_device(
    latent, conditioning, context_cond, modulation, context, query_weight, key_projection,
    value_projection, out_weight, sink_head_logit, prefix_logit_bias,
):
    n_sp, n_tp, n_dp = lax.axis_size("sp"), lax.axis_size("tp"), lax.axis_size("dp")
    samples = conditioning.shape[0]
    _, tok, width = latent.shape
    n_ctx = context.shape[1]
    depth, cols = modulation.shape[1:]
    q_width = query_weight.shape[1]
    heads = q_width // HEAD_SIZE
    out_cols = out_weight.shape[1]
    blocks = tok // WINDOW_REACH
    window = tok + 2 * WINDOW_REACH
    keys = window + n_sp * n_ctx
    n_td = n_tp * n_dp
    act_rows = -(-(samples + 1) // 8) * 8
    pack_rows = -(-(2 * samples + 2) // 8) * 8
    row_table, col_table = rotary_tables(n_sp * tok // GRID_W)
    table = np.concatenate([col_table, row_table], axis=1)
    vm = pltpu.VMEM
    dma = pltpu.SemaphoreType.DMA
    group = n_dp * cols
    scratch = [
        vm((tok, width), BF16), vm((samples, depth), BF16), vm((depth,), BF16),
        vm((3, depth, cols), BF16), vm((2, n_ctx, width), BF16), vm((width, q_width + LANES), BF16),
        vm(out_weight.shape, BF16), pltpu.SMEM((heads,), F32), pltpu.SMEM((heads,), F32),
        vm(table.shape, F32),
        vm((act_rows, depth), F32), vm((pack_rows, cols), F32), vm((pack_rows, cols), BF16),
        vm((2 * n_sp - 1, pack_rows, cols), BF16), vm((2, pack_rows, cols), F32),
        vm((n_td, 2, 8, cols), BF16), vm((n_tp, n_dp // 2, 2, 8, cols), BF16),
        vm((n_tp, 8, group), F32), vm((act_rows, cols), F32),
        vm((2 * n_sp - 1, act_rows, cols), F32), vm((n_dp, 2, 8, cols), F32),
        vm((n_dp // 2, 2, 8, cols), F32),
        vm((n_tp, tok, group), F32), vm((n_tp, 2 * n_ctx, group), F32), vm((n_tp, tok, group), BF16),
        vm((n_tp, 2 * n_ctx, group), BF16), vm((LANES, width), BF16), vm((tok, LANES), F32),
        vm((tok, LANES), F32), vm((tok, q_width + LANES), F32), vm((2 * n_ctx, LANES), F32),
        vm((window, LANES), BF16), vm((2, n_ctx, LANES), BF16), vm((2 * n_sp - 1, n_ctx, LANES), BF16),
        vm((keys, LANES), BF16), vm((keys, LANES), BF16),
        vm((blocks, heads * WINDOW_REACH, LANES), BF16),
        vm((n_tp, blocks, WINDOW_REACH, q_width), BF16),
        dma((11,)), dma((1,)), dma((1,)), dma((1,)), dma((1,)), dma((1,)), dma((n_tp,)),
        dma((1,)), dma((2,)), dma((1,)), dma((1,)), dma((1,)), dma((blocks, 3)), dma((1,)),
        dma((1,)), dma((1,)), dma((1,)),
    ]
    stays = pl.BlockSpec(memory_space=pltpu.HBM)
    out = pl.pallas_call(
        functools.partial(block_kernel, (n_sp, n_tp, n_dp, samples)),
        out_shape=pltpu.VMEM((tok, out_cols), F32),
        in_specs=[stays] * 12,
        out_specs=pl.BlockSpec(memory_space=pltpu.VMEM),
        scratch_shapes=scratch,
        compiler_params=pltpu.CompilerParams(
            collective_id=0, has_side_effects=True, vmem_limit_bytes=66000000
        ),
        name="fused_block",
    )(
        latent[0], conditioning, context_cond, modulation, context[0], query_weight,
        key_projection.T, value_projection.T, out_weight, sink_head_logit, prefix_logit_bias,
        jnp.asarray(table),
    )
    return out[None]


def solution(mesh):
    placed = (
        P("dp", "sp", None),
        P(None, "sp"),
        P("sp"),
        P(None, "sp", ("tp", "dp")),
        P("dp", "sp", None),
        P(None, "tp"),
        P(None, "tp"),
        P(None, "tp"),
        P(None, "tp"),
        P("tp"),
        P("tp"),
    )
    return jax.shard_map(
        per_device, mesh=mesh, in_specs=placed, out_specs=P("dp", "sp", "tp"), check_vma=False
    )
```

```python
import functools

import jax
import jax.numpy as jnp
import numpy as np
from jax import lax
from jax.experimental import pallas as pl
from jax.experimental.pallas import tpu as pltpu
from jax.sharding import PartitionSpec as P

HEAD_SIZE = 64
GRID_W = 64
WINDOW_REACH = 128
NORM_EPSILON = 1e-06
ROTARY_BASE = 10000.0
MASKED = -1e30
LANES = 128
MESH = pl.DeviceIdType.MESH
F32 = jnp.float32
BF16 = jnp.bfloat16


def rotary_tables(grid_rows):
    half = HEAD_SIZE // 2
    quarter = half // 2
    lane = np.arange(LANES) % HEAD_SIZE
    frequency = ROTARY_BASE ** (-2.0 * (lane % quarter) / half)
    frequency = frequency.astype(np.float32).astype(np.float64)
    sign = np.where(lane % half < quarter, -1.0, 1.0)
    by_row = lane < half

    def tables(count, keep):
        angles = np.arange(count)[:, None] * frequency[None, :]
        cosine = np.where(keep[None, :], np.cos(angles), 0.0)
        sine = np.where(keep[None, :], np.sin(angles) * sign[None, :], 0.0)
        return np.stack([cosine, sine]).astype(np.float32)

    return tables(grid_rows, by_row), tables(GRID_W, ~by_row)


def block_kernel(
    dims,
    lat_hbm, cond_hbm, cctx_hbm, mod_hbm, ctx_hbm, qw_hbm, kw_hbm, vw_hbm, ow_hbm,
    sink_hbm, bias_hbm, turn_hbm,
    outv,
    lat, cond, cctx, mod, ctx, wall, ow, sink, bias, angles,
    act, packf, pack, packs, sendb, slots, modv, gatef, gates, gateb, gatev,
    xn, xnc, nrm, nrmc, kvw, cosv, sinv, acc, accc, kvb, cxs, cxb, kd, vd, q4, att,
    a_r, x_r, b_r, h_r, c_r, g_r, v_r, w_r, in_sem, a_s, x_s, b_s, h_s, c_s, g_s, v_s, w_s,
):
    n_sp, n_tp, n_dp, samples = dims
    sp, tp, dp = lax.axis_index("sp"), lax.axis_index("tp"), lax.axis_index("dp")
    n_td = n_tp * n_dp
    me = tp * n_dp + dp
    tok, width = lat.shape
    cols = mod.shape[2]
    group = n_dp * cols
    n_ctx = ctx.shape[1]
    core, lead, pair = lax.rem(dp, 2), dp - lax.rem(dp, 2) + 1, dp // 2
    n_pairs = n_dp // 2
    reach = WINDOW_REACH
    blocks = tok // reach
    q_width = wall.shape[1] - LANES
    pairs = q_width // LANES
    heads = 2 * pairs

    barrier = pltpu.get_barrier_semaphore()
    @pl.when(core == 1)
    def _():
        for o in range(1, n_sp):
            for d in (2 * pair, 2 * pair + 1):
                pl.semaphore_signal(
                    barrier, inc=1, device_id={"sp": lax.rem(sp + o, n_sp), "dp": d},
                    device_id_type=MESH,
                )

    for o in range(1, n_td):
        lin = lax.rem(me + o, n_td)
        pl.semaphore_signal(
            barrier, inc=1, device_id={"tp": lin // n_dp, "dp": lax.rem(lin, n_dp)},
            device_id_type=MESH,
        )

    relayed = n_tp == 4
    direct = (1, 2) if relayed else range(1, n_tp)

    def partner(o):
        if not relayed:
            return lax.rem(tp + o, n_tp)
        x, y = lax.rem(tp, 2), tp // 2
        x = 1 - x if o % 2 else x
        y = 1 - y if o // 2 else y
        return 2 * y + x

    def owner(o):
        return partner(o) if relayed else lax.rem(tp + n_tp - o, n_tp)

    pairs_in = [
        (cond_hbm, cond, 0), (cctx_hbm, cctx, 1),
        (mod_hbm.at[pl.ds(0, 2)], mod.at[pl.ds(0, 2)], 2), (ctx_hbm, ctx.at[0], 3),
        (mod_hbm.at[2], mod.at[2], 4), (lat_hbm, lat, 5),
        (kw_hbm, kvw.at[pl.ds(0, HEAD_SIZE)], 6),
        (vw_hbm, kvw.at[pl.ds(HEAD_SIZE, HEAD_SIZE)], 6),
        (qw_hbm, wall.at[:, pl.ds(0, q_width)], 6), (turn_hbm, angles, 7), (sink_hbm, sink, 8),
        (bias_hbm, bias, 9), (ow_hbm, ow, 10),
    ]
    loads = [pltpu.make_async_copy(src, dst, in_sem.at[i]) for src, dst, i in pairs_in]
    for load in loads[:4]:
        load.start()

    def remote(src, dst, left, arrived, **device):
        return pltpu.make_async_remote_copy(
            src_ref=src, dst_ref=dst, send_sem=left, recv_sem=arrived, device_id=device,
            device_id_type=MESH,
        )

    def bytes_of(ref, semaphore):
        pltpu.make_async_copy(ref, ref, semaphore).wait()

    act[...] = jnp.zeros_like(act)
    loads[0].wait()
    loads[1].wait()
    act[0:samples, :] = cond[...].astype(F32)
    act[samples : samples + 1, :] = cctx[...].astype(F32).reshape(1, cctx.shape[0])
    v = act[...]
    activated = (v / (1.0 + jnp.exp(-v))).astype(BF16)
    for load in loads[4:]:
        load.start()
    loads[2].wait()
    shift = jnp.dot(activated, mod[0], preferred_element_type=F32)
    scale = jnp.dot(activated, mod[1], preferred_element_type=F32)
    rows = [
        part[r : r + 1, :] for d in range(samples) for r in (d, samples) for part in (shift, scale)
    ]
    rows += [jnp.zeros_like(rows[0])] * (packf.shape[0] - len(rows))
    packf[...] = jnp.concatenate(rows, axis=0)
    pack[...] = packf[...].astype(BF16)

    pl.semaphore_wait(barrier, n_sp - 1 + n_td - 1)
    a_copies = [
        remote(
            pack, packs.at[2 * o - 1 + core if o else 0], a_s.at[0], a_r.at[0],
            sp=lax.rem(sp + o, n_sp), dp=lead,
        )
        for o in range(n_sp)
    ]
    for copy in a_copies[:0:-1]:
        copy.start()
    spare = remote(ctx.at[0], ctx.at[1], x_s.at[0], x_r.at[0], dp=lead)

    @pl.when(core == 0)
    def _():
        a_copies[0].start()

    loads[4].wait()
    gatef[...] = jnp.dot(activated, mod[2], preferred_element_type=F32)
    v_copies = [
        remote(
            gatef, gates.at[2 * o - 1 + core if o else 0], v_s.at[0], v_r.at[0],
            sp=lax.rem(sp + o, n_sp), dp=lead,
        )
        for o in range(n_sp)
    ]
    for copy in v_copies[1:]:
        copy.start()
    loads[3].wait()

    @pl.when(core == 0)
    def _():
        v_copies[0].start()
        spare.start()

    chunk = 64

    def normalise(src, dst, first, last):
        def body(i, carry):
            rows = pl.ds(pl.multiple_of(i * chunk, chunk), chunk)
            x = src[rows, :].astype(F32)
            x = x - jnp.mean(x, axis=-1, keepdims=True)
            spread = jnp.mean(x * x, axis=-1, keepdims=True)
            x = x * lax.rsqrt(spread + NORM_EPSILON)
            for t in range(n_tp):
                dst[t, rows, :] = x[:, t * group : (t + 1) * group]
            return carry

        lax.fori_loop(first, last, body, 0)

    def normalise_context(which):
        for i in range(0, n_ctx, chunk):
            x = ctx[which, i : i + chunk, :].astype(F32)
            x = x - jnp.mean(x, axis=-1, keepdims=True)
            spread = jnp.mean(x * x, axis=-1, keepdims=True)
            x = x * lax.rsqrt(spread + NORM_EPSILON)
            at = which * n_ctx + i
            for t in range(n_tp):
                xnc[t, at : at + chunk, :] = x[:, t * group : (t + 1) * group]

    loads[5].wait()
    normalise(lat, xn, 0, tok // chunk)

    @pl.when(core == 1)
    def _():
        normalise_context(0)
        spare.wait_recv()
        normalise_context(1)


    b_copies = [
        remote(
            sendb.at[lax.rem(dp + e, n_dp)], slots.at[o, pair], b_s.at[0], b_r.at[o],
            tp=partner(o), dp=lax.rem(dp + e, n_dp),
        )
        for o in reversed(range(n_tp))
        for e in range(n_dp)
        if o or e
    ]

    @pl.when(core == 1)
    def _():
        bytes_of(packs, a_r.at[0])
        for c in range(2):
            summed = packf[...] if c else packs[0].astype(F32)
            for o in range(1, n_sp):
                summed = summed + packs[2 * o - 1 + c].astype(F32)
            for d in range(n_dp):
                sendb[d, c] = summed[4 * d : 4 * d + 4, :].astype(BF16)
        for copy in b_copies:
            copy.start()
        slots[0, pair] = sendb[dp]

    bytes_of(wall, in_sem.at[6])
    for load in loads[9:12]:
        load.wait()
    groups = tok // GRID_W
    for g in range(groups):
        row = pl.ds(GRID_W + sp * groups + g, 1)
        span = slice(g * GRID_W, (g + 1) * GRID_W)
        cosv[span, :] = angles[0, row, :] + angles[0, 0:GRID_W, :]
        sinv[span, :] = angles[1, row, :] + angles[1, 0:GRID_W, :]
    for j in range(width // LANES):
        span = slice(j * LANES, (j + 1) * LANES)
        wall[span, q_width:] = kvw[:, span].astype(F32).T.astype(BF16)

    def condition(src, dst, count, o, g, shift_row, scale_row):
        scale = 1.0 + modv[o, scale_row : scale_row + 1, :]
        shift = modv[o, shift_row : shift_row + 1, :]
        for i in range(0, count, chunk):
            rows = slice(i, i + chunk)
            dst[o, rows, :] = (src[g, rows, :] * scale + shift).astype(BF16)

    c_copies = [remote(cxs.at[0], cxb.at[0], c_s.at[0], c_r.at[0], dp=dp - core)]
    for r in range(1, n_sp):
        for c in range(2):
            c_copies.append(
                remote(
                    cxs.at[c], cxb.at[r], c_s.at[0], c_r.at[0],
                    sp=lax.rem(sp + r, n_sp), dp=2 * pair + c,
                )
            )
    def land(o):
        if o:
            bytes_of(slots.at[o], b_r.at[o])
        else:
            @pl.when(core == 0)
            def _():
                bytes_of(slots.at[0], b_r.at[0])

            if n_pairs > 1:
                @pl.when(core == 1)
                def _():
                    bytes_of(slots.at[0, pl.ds(1, n_pairs - 1)], b_r.at[0])
        for d in range(n_dp):
            modv[o, 0:4, d * cols : (d + 1) * cols] = slots[o, d // 2, d % 2].astype(F32)

    def weight_rows(o):
        return pl.ds(pl.multiple_of(owner(o) * group, group), group)

    def context_part(o):
        condition(xnc, nrmc, 2 * n_ctx, o, owner(o), 2, 3)
        weights = wall[weight_rows(o), q_width:]
        return jnp.dot(nrmc[o], weights, preferred_element_type=F32)

    def latent_part(o):
        condition(xn, nrm, tok, o, owner(o), 0, 1)
        u = jnp.dot(nrm[o], wall[weight_rows(o), :], preferred_element_type=F32)
        acc[...] = acc[...] + u if o else u

    land(0)

    @pl.when(core == 1)
    def _():
        accc[...] = context_part(0)

    latent_part(0)

    @pl.when(core == 1)
    def _():
        u = accc[...]
        for o in range(1, n_tp):
            land(o)
            u = u + context_part(o)
        cxs[0] = u[n_ctx:, :].astype(BF16)
        cxs[1] = u[0:n_ctx, :].astype(BF16)
        for copy in c_copies[1:] + c_copies[:1]:
            copy.start()
        cxb[0] = u[0:n_ctx, :].astype(BF16)
        for o in range(1, n_tp):
            latent_part(o)

    @pl.when(core == 0)
    def _():
        for o in range(1, n_tp):
            land(o)
            latent_part(o)

    half = HEAD_SIZE // 2
    quarter = half // 2

    def turn(u, cosine, sine):
        w = u.shape[1]
        lane = lax.broadcasted_iota(jnp.int32, u.shape, 1)
        first = lax.rem(lane, half) < quarter
        swapped = jnp.where(first, pltpu.roll(u, w - quarter, 1), pltpu.roll(u, quarter, 1))
        return u * cosine + swapped * sine

    def low_half(shape):
        return lax.broadcasted_iota(jnp.int32, shape, 1) < HEAD_SIZE

    def expand(x, at):
        low = low_half(x.shape)
        other = pltpu.roll(x, HEAD_SIZE, 1)
        span = slice(at, at + x.shape[0])
        kd[span, :] = jnp.where(low, x, other).astype(BF16)
        vd[span, :] = jnp.where(low, other, x).astype(BF16)

    u = acc[:, q_width:]
    kv_rows = jnp.where(low_half(u.shape), turn(u, cosv[...], sinv[...]), u)
    kvb[reach : reach + tok, :] = kv_rows.astype(BF16)

    up = remote(
        kvb.at[pl.ds(tok, reach)], kvb.at[pl.ds(0, reach)], h_s.at[0], h_r.at[0],
         sp=lax.rem(sp + 1, n_sp)
    )
    down = remote(
        kvb.at[pl.ds(reach, reach)], kvb.at[pl.ds(reach + tok, reach)], h_s.at[0], h_r.at[1],
        sp=lax.rem(sp + n_sp - 1, n_sp),
    )

    @pl.when(sp < n_sp - 1)
    def _():
        up.start()

    @pl.when(sp > 0)
    def _():
        down.start()

    expand(kv_rows, reach)

    factor = HEAD_SIZE ** (-0.5)
    for p in range(pairs):
        t = turn(acc[:, p * LANES : (p + 1) * LANES], cosv[...], sinv[...]) * factor
        low = low_half(t.shape)
        for parity, kept in ((0, jnp.where(low, t, 0.0)), (1, jnp.where(low, 0.0, t))):
            kept = kept.astype(BF16)
            at = (2 * p + parity) * reach
            for b in range(blocks):
                q4[b, at : at + reach, :] = kept[b * reach : (b + 1) * reach, :]

    window = tok + 2 * reach
    nt = (((1,), (1,)), ((), ()))
    n_all_ctx = n_sp * n_ctx
    delta = lax.broadcasted_iota(jnp.int32, (reach, reach), 1) - lax.broadcasted_iota(
        jnp.int32, (reach, reach), 0
    )
    far = 4 * reach
    low_edge = jnp.where(sp == 0, far, 0)
    high_edge = jnp.where(sp == n_sp - 1, -far, 0)

    def scores(b, first, count):
        keys = kd[first : first + count, :]
        return lax.dot_general(q4[b], keys, nt, preferred_element_type=F32)

    def tiles(s, h):
        rows = slice(h * reach, (h + 1) * reach)
        return [s[rows, c * LANES : (c + 1) * LANES] for c in range(s.shape[1] // LANES)]

    def soften(parts, highest):
        powers = [jnp.exp(s - highest) for s in parts]
        mass = powers[0]
        for e in powers[1:]:
            mass = mass + e
        powers = jnp.concatenate([e.astype(BF16) for e in powers], axis=1)
        return powers, jnp.sum(mass, axis=-1, keepdims=True)

    def top_of(parts):
        top = parts[0]
        for s in parts[1:]:
            top = jnp.maximum(top, s)
        return jnp.max(top, axis=-1, keepdims=True)

    def weigh(powers, first):
        e = jnp.concatenate(powers, axis=0)
        return jnp.dot(e, vd[first : first + e.shape[1], :], preferred_element_type=F32)

    def within(b):
        first, last = max(b - 1, 0), min(b + 1, blocks - 1)
        at = reach + first * reach
        s = scores(b, at, (last - first + 1) * reach)
        tops, masses, powers = [], [], []
        for h in range(heads):
            parts = tiles(s, h)
            if b > 0:
                parts[0] = jnp.where(delta >= 0, parts[0], MASKED)
            if b < blocks - 1:
                parts[-1] = jnp.where(delta <= 0, parts[-1], MASKED)
            highest = jnp.maximum(top_of(parts), sink[h])
            e, mass = soften(parts, highest)
            tops.append(highest)
            masses.append(mass + jnp.exp(sink[h] - highest))
            powers.append(e)
        return tops, masses, weigh(powers, at)


    def beyond(b, state, some):
        tops, masses, weighed = state
        first, last = some[0] * reach, (some[-1] + 1) * reach
        q2 = q4[b, first:last, :]

        def scores(at, count):
            keys = kd[at : at + count, :]
            return lax.dot_general(q2, keys, nt, preferred_element_type=F32)

        parts_of = [(window, scores(window, n_all_ctx))]
        edges = []
        if b == 0:
            edges.append((0, lambda s: jnp.where(delta >= low_edge, s, MASKED)))
        if b == blocks - 1:
            edges.append((reach + tok, lambda s: jnp.where(delta <= high_edge, s, MASKED)))
        for at, _ in edges:
            parts_of.append((at, scores(at, reach)))
        fades, powers = {}, [[] for _ in parts_of]
        for i, h in enumerate(some):
            groups = [[s + bias[h] for s in tiles(parts_of[0][1], i)]]
            for (_, mask), (_, s) in zip(edges, parts_of[1:]):
                groups.append([mask(s) for s in tiles(s, i)])
            top = jnp.maximum(top_of(sum(groups, [])), tops[h])
            fade = jnp.exp(tops[h] - top)
            mass = masses[h] * fade
            for kept, parts in zip(powers, groups):
                e, more = soften(parts, top)
                kept.append(e)
                mass = mass + more
            share = 1.0 / mass
            fades[h] = (fade * share, share)
        more = weigh(powers[0], window)
        for kept, (at, _) in zip(powers[1:], parts_of[1:]):
            more = more + weigh(kept, at)
        low = low_half((reach, LANES))
        for p in range(some[0] // 2, some[-1] // 2 + 1):
            halves = []
            for h in (2 * p, 2 * p + 1):
                rows = slice(h * reach, (h + 1) * reach)
                mine = slice(h * reach - first, (h + 1) * reach - first)
                halves.append(weighed[rows, :] * fades[h][0] + more[mine, :] * fades[h][1])
            att[0, b, :, p * LANES : (p + 1) * LANES] = jnp.where(low, *halves).astype(BF16)

    middle = reach // 2

    def send(b, o, relay, first=0, count=q_width):
        if relayed:
            at = (o - 1) * middle if relay else (2 - o) * middle
            span = (b, pl.ds(at, middle), pl.ds(first, count))
        else:
            span = (b, slice(None), pl.ds(first, count))
        remote(
            att.at[(0, *span)], att.at[(o, *span)], g_s.at[0], g_r.at[b, 0 if relay else 1],
            tp=partner(o),
        ).start()

    def forward(b):
        bytes_of(att.at[1, b], g_r.at[b, 0])
        for o in direct:
            part = pl.ds((o - 1) * middle, middle)
            remote(
                att.at[o, b, part], att.at[3, b, part], g_s.at[0], g_r.at[b, 2], tp=partner(3 - o)
            ).start()

    order = list(range(1, blocks - 1)) + ([0, blocks - 1] if blocks > 1 else [0])
    states = {}
    early = order
    for b in early:
        states[b] = within(b)
    w_copies = [
        remote(
            gateb.at[lax.rem(dp + e, n_dp)], gatev.at[pair], w_s.at[0], w_r.at[0],
            dp=lax.rem(dp + e, n_dp),
        )
        for e in range(1, n_dp)
    ]

    @pl.when(core == 1)
    def _():
        bytes_of(gates, v_r.at[0])
        for c in range(2):
            summed = gatef[...] if c else gates[0]
            for o in range(1, n_sp):
                summed = summed + gates[2 * o - 1 + c]
            for d in range(n_dp):
                gateb[d, c] = jnp.broadcast_to(summed[d : d + 1, :], (8, cols))
        for copy in w_copies:
            copy.start()
        gatev[pair] = gateb[dp]


    @pl.when(core == 0)
    def _():
        bytes_of(cxb.at[pl.ds(0, n_sp)], c_r.at[0])

    @pl.when(core == 1)
    def _():
        bytes_of(cxb.at[pl.ds(1, n_sp - 1)], c_r.at[0])

    for r in range(n_sp):
        expand(cxb[r].astype(F32), window + r * n_ctx)
    held = []
    for b in order:
        if b not in states:
            states[b] = within(b)
        if b == 0:
            @pl.when(sp > 0)
            def _():
                up.wait_recv()

            @pl.when(sp == 0)
            def _():
                kvb[0:reach, :] = jnp.zeros((reach, LANES), BF16)

            expand(kvb[0:reach, :].astype(F32), 0)
        if b == blocks - 1:
            @pl.when(sp < n_sp - 1)
            def _():
                down.wait_recv()

            @pl.when(sp == n_sp - 1)
            def _():
                kvb[reach + tok : window, :] = jnp.zeros((reach, LANES), BF16)

            expand(kvb[reach + tok : window, :].astype(F32), reach + tok)
        if b == order[0]:
            for p in range(pairs):
                beyond(b, states[b], (2 * p, 2 * p + 1))
                for o in direct:
                    send(b, o, True, p * LANES, LANES)
        else:
            beyond(b, states[b], tuple(range(heads)))
            for o in direct:
                send(b, o, True)
        if relayed:
            held.append(b)
            if b == order[0] or b == order[-1]:
                for c in held:
                    for o in direct:
                        send(c, o, False)
                held.clear()

    loads[12].wait()
    out_cols = ow.shape[1]
    mine = pl.ds(pl.multiple_of(tp * out_cols, out_cols), out_cols)

    @pl.when(core == 0)
    def _():
        bytes_of(gatev, w_r.at[0])

    if n_pairs > 1:
        @pl.when(core == 1)
        def _():
            bytes_of(gatev.at[pl.ds(1, n_pairs - 1)], w_r.at[0])

    for d in range(n_dp):
        modv[0, :, d * cols : (d + 1) * cols] = gatev[d // 2, d % 2]
    gate = modv[0, 0:1, :]

    def project(b, o):
        w = ow[pl.ds(pl.multiple_of(owner(o) * q_width, q_width), q_width), :]
        return jnp.dot(att[o, b], w, preferred_element_type=F32)

    for b in order:
        if relayed:
            forward(b)
        else:
            bytes_of(att.at[pl.ds(1, n_tp - 1), b], g_r.at[b, 0])
        outv[b * reach : (b + 1) * reach, :] = project(b, 0)
    for b in order:
        if relayed:
            bytes_of(att.at[1, b], g_r.at[b, 1])
        rows = slice(b * reach, (b + 1) * reach)
        mixed = outv[rows, :]
        for o in direct:
            mixed = mixed + project(b, o)
        outv[rows, :] = mixed
    for b in order:
        rows = slice(b * reach, (b + 1) * reach)
        mixed = outv[rows, :]
        if relayed:
            bytes_of(att.at[3, b], g_r.at[b, 2])
            mixed = mixed + project(b, 3)
        outv[rows, :] = lat[rows, mine].astype(F32) + gate * mixed

    bytes_of(att.at[pl.ds(1, n_tp - 1)], g_s.at[0])

    @pl.when(core == 0)
    def _():
        bytes_of(packs.at[pl.ds(0, n_sp)], a_s.at[0])
        bytes_of(gates.at[pl.ds(0, n_sp)], v_s.at[0])
        spare.wait_send()

    @pl.when(core == 1)
    def _():
        bytes_of(packs.at[pl.ds(0, n_sp - 1)], a_s.at[0])
        bytes_of(gates.at[pl.ds(0, n_sp - 1)], v_s.at[0])
        bytes_of(sendb.at[pl.ds(0, n_td - 1)], b_s.at[0])
        bytes_of(gateb.at[pl.ds(0, n_dp - 1)], w_s.at[0])
        bytes_of(cxb, c_s.at[0])

    edge = jnp.logical_or(sp == 0, sp == n_sp - 1)

    @pl.when(edge)
    def _():
        bytes_of(kvb.at[pl.ds(0, reach)], h_s.at[0])

    @pl.when(jnp.logical_not(edge))
    def _():
        bytes_of(kvb.at[pl.ds(0, 2 * reach)], h_s.at[0])


def scoped_kernel(dims, *refs):
    dma = pltpu.SemaphoreType.DMA
    pl.run_scoped(
        lambda *local: block_kernel(dims, *refs, *local), dma((11,)), *[dma((1,))] * 8
    )


def per_device(
    latent, conditioning, context_cond, modulation, context, query_weight, key_projection,
    value_projection, out_weight, sink_head_logit, prefix_logit_bias,
):
    n_sp, n_tp, n_dp = lax.axis_size("sp"), lax.axis_size("tp"), lax.axis_size("dp")
    samples = conditioning.shape[0]
    _, tok, width = latent.shape
    n_ctx = context.shape[1]
    depth, cols = modulation.shape[1:]
    q_width = query_weight.shape[1]
    heads = q_width // HEAD_SIZE
    out_cols = out_weight.shape[1]
    blocks = tok // WINDOW_REACH
    window = tok + 2 * WINDOW_REACH
    keys = window + n_sp * n_ctx
    n_td = n_tp * n_dp
    act_rows = -(-(samples + 1) // 8) * 8
    pack_rows = -(-(4 * samples) // 8) * 8
    row_table, col_table = rotary_tables(n_sp * tok // GRID_W)
    table = np.concatenate([col_table, row_table], axis=1)
    vm = pltpu.VMEM
    dma = pltpu.SemaphoreType.DMA
    group = n_dp * cols
    scratch = [
        vm((tok, width), BF16), vm((samples, depth), BF16), vm((depth,), BF16),
        vm((3, depth, cols), BF16), vm((2, n_ctx, width), BF16), vm((width, q_width + LANES), BF16),
        vm(out_weight.shape, BF16), pltpu.SMEM((heads,), F32), pltpu.SMEM((heads,), F32),
        vm(table.shape, F32),
        vm((act_rows, depth), F32), vm((pack_rows, cols), F32), vm((pack_rows, cols), BF16),
        vm((2 * n_sp - 1, pack_rows, cols), BF16),
        vm((n_td, 2, 4, cols), BF16), vm((n_tp, n_dp // 2, 2, 4, cols), BF16),
        vm((n_tp, 8, group), F32), vm((act_rows, cols), F32),
        vm((2 * n_sp - 1, act_rows, cols), F32), vm((n_dp, 2, 8, cols), F32),
        vm((n_dp // 2, 2, 8, cols), F32),
        vm((n_tp, tok, group), F32), vm((n_tp, 2 * n_ctx, group), F32), vm((n_tp, tok, group), BF16),
        vm((n_tp, 2 * n_ctx, group), BF16), vm((LANES, width), BF16), vm((tok, LANES), F32),
        vm((tok, LANES), F32), vm((tok, q_width + LANES), F32), vm((2 * n_ctx, LANES), F32),
        vm((window, LANES), BF16), vm((2, n_ctx, LANES), BF16), vm((2 * n_sp - 1, n_ctx, LANES), BF16),
        vm((keys, LANES), BF16), vm((keys, LANES), BF16),
        vm((blocks, heads * WINDOW_REACH, LANES), BF16),
        vm((n_tp, blocks, WINDOW_REACH, q_width), BF16),
        dma((1,)), dma((1,)), dma((n_tp,)), dma((2,)), dma((1,)), dma((blocks, 3)), dma((1,)),
        dma((1,)),
    ]
    stays = pl.BlockSpec(memory_space=pltpu.HBM)
    out = pl.pallas_call(
        functools.partial(scoped_kernel, (n_sp, n_tp, n_dp, samples)),
        out_shape=pltpu.VMEM((tok, out_cols), F32),
        in_specs=[stays] * 12,
        out_specs=pl.BlockSpec(memory_space=pltpu.VMEM),
        scratch_shapes=scratch,
        compiler_params=pltpu.CompilerParams(
            collective_id=0, has_side_effects=True, vmem_limit_bytes=66000000
        ),
        name="fused_block",
    )(
        latent[0], conditioning, context_cond, modulation, context[0], query_weight,
        key_projection.T, value_projection.T, out_weight, sink_head_logit, prefix_logit_bias,
        jnp.asarray(table),
    )
    return out[None]


def solution(mesh):
    placed = (
        P("dp", "sp", None),
        P(None, "sp"),
        P("sp"),
        P(None, "sp", ("tp", "dp")),
        P("dp", "sp", None),
        P(None, "tp"),
        P(None, "tp"),
        P(None, "tp"),
        P(None, "tp"),
        P("tp"),
        P("tp"),
    )
    return jax.shard_map(
        per_device, mesh=mesh, in_specs=placed, out_specs=P("dp", "sp", "tp"), check_vma=False
    )
```

```python
import functools

import jax
import jax.numpy as jnp
import numpy as np
from jax import lax
from jax.experimental import pallas as pl
from jax.experimental.pallas import tpu as pltpu
from jax.sharding import PartitionSpec as P

HEAD_SIZE = 64
GRID_W = 64
WINDOW_REACH = 128
NORM_EPSILON = 1e-06
ROTARY_BASE = 10000.0
MASKED = -1e30
LANES = 128
MESH = pl.DeviceIdType.MESH
F32 = jnp.float32
BF16 = jnp.bfloat16


def rotary_tables(grid_rows):
    half = HEAD_SIZE // 2
    quarter = half // 2
    lane = np.arange(LANES) % HEAD_SIZE
    frequency = ROTARY_BASE ** (-2.0 * (lane % quarter) / half)
    frequency = frequency.astype(np.float32).astype(np.float64)
    sign = np.where(lane % half < quarter, -1.0, 1.0)
    by_row = lane < half

    def tables(count, keep):
        angles = np.arange(count)[:, None] * frequency[None, :]
        cosine = np.where(keep[None, :], np.cos(angles), 0.0)
        sine = np.where(keep[None, :], np.sin(angles) * sign[None, :], 0.0)
        return np.stack([cosine, sine]).astype(np.float32)

    return tables(grid_rows, by_row), tables(GRID_W, ~by_row)


def block_kernel(
    dims,
    lat_hbm, cond_hbm, cctx_hbm, mod_hbm, ctx_hbm, qw_hbm, kw_hbm, vw_hbm, ow_hbm,
    sink_hbm, bias_hbm, turn_hbm,
    outv,
    lat, cond, cctx, mod, ctx, wall, ow, sink, bias, angles,
    act, packf, pack, packs, sendb, slots, modv, gatef, gates, gateb, gatev,
    xn, xnc, nrm, nrmc, kvw, cosv, sinv, acc, accc, kvb, cxs, cxb, kd, vd, q4, att,
    a_r, x_r, b_r, h_r, c_r, g_r, v_r, w_r, in_sem, a_s, x_s, b_s, h_s, c_s, g_s, v_s, w_s,
):
    n_sp, n_tp, n_dp, samples = dims
    sp, tp, dp = lax.axis_index("sp"), lax.axis_index("tp"), lax.axis_index("dp")
    n_td = n_tp * n_dp
    me = tp * n_dp + dp
    tok, width = lat.shape
    cols = mod.shape[2]
    group = n_dp * cols
    n_ctx = ctx.shape[1]
    core, lead, pair = lax.rem(dp, 2), dp - lax.rem(dp, 2) + 1, dp // 2
    n_pairs = n_dp // 2
    reach = WINDOW_REACH
    blocks = tok // reach
    q_width = wall.shape[1] - LANES
    pairs = q_width // LANES
    heads = 2 * pairs

    barrier = pltpu.get_barrier_semaphore()
    @pl.when(core == 1)
    def _():
        for o in range(1, n_sp):
            for d in (2 * pair, 2 * pair + 1):
                pl.semaphore_signal(
                    barrier, inc=1, device_id={"sp": lax.rem(sp + o, n_sp), "dp": d},
                    device_id_type=MESH,
                )

    for o in range(1, n_td):
        lin = lax.rem(me + o, n_td)
        pl.semaphore_signal(
            barrier, inc=1, device_id={"tp": lin // n_dp, "dp": lax.rem(lin, n_dp)},
            device_id_type=MESH,
        )

    relayed = n_tp == 4
    direct = (1, 2) if relayed else range(1, n_tp)

    def partner(o):
        if not relayed:
            return lax.rem(tp + o, n_tp)
        x, y = lax.rem(tp, 2), tp // 2
        x = 1 - x if o % 2 else x
        y = 1 - y if o // 2 else y
        return 2 * y + x

    def owner(o):
        return partner(o) if relayed else lax.rem(tp + n_tp - o, n_tp)

    pairs_in = [
        (cond_hbm, cond, 0), (cctx_hbm, cctx, 1),
        (mod_hbm.at[pl.ds(0, 2)], mod.at[pl.ds(0, 2)], 2), (ctx_hbm, ctx.at[0], 3),
        (mod_hbm.at[2], mod.at[2], 4), (lat_hbm, lat, 5),
        (kw_hbm, kvw.at[pl.ds(0, HEAD_SIZE)], 6),
        (vw_hbm, kvw.at[pl.ds(HEAD_SIZE, HEAD_SIZE)], 6),
        (qw_hbm, wall.at[:, pl.ds(0, q_width)], 6), (turn_hbm, angles, 7), (sink_hbm, sink, 8),
        (bias_hbm, bias, 9), (ow_hbm, ow, 10),
    ]
    loads = [pltpu.make_async_copy(src, dst, in_sem.at[i]) for src, dst, i in pairs_in]
    for load in loads[:4]:
        load.start()

    def remote(src, dst, left, arrived, **device):
        return pltpu.make_async_remote_copy(
            src_ref=src, dst_ref=dst, send_sem=left, recv_sem=arrived, device_id=device,
            device_id_type=MESH,
        )

    def bytes_of(ref, semaphore):
        pltpu.make_async_copy(ref, ref, semaphore).wait()

    act[...] = jnp.zeros_like(act)
    loads[0].wait()
    loads[1].wait()
    act[0:samples, :] = cond[...].astype(F32)
    act[samples : samples + 1, :] = cctx[...].astype(F32).reshape(1, cctx.shape[0])
    v = act[...]
    activated = (v / (1.0 + jnp.exp(-v))).astype(BF16)
    for load in loads[4:]:
        load.start()
    loads[2].wait()
    shift = jnp.dot(activated, mod[0], preferred_element_type=F32)
    scale = jnp.dot(activated, mod[1], preferred_element_type=F32)
    rows = [
        part[r : r + 1, :] for d in range(samples) for r in (d, samples) for part in (shift, scale)
    ]
    rows += [jnp.zeros_like(rows[0])] * (packf.shape[0] - len(rows))
    packf[...] = jnp.concatenate(rows, axis=0)
    pack[...] = packf[...].astype(BF16)

    pl.semaphore_wait(barrier, n_sp - 1 + n_td - 1)
    a_copies = [
        remote(
            pack, packs.at[2 * o - 1 + core if o else 0], a_s.at[0], a_r.at[0],
            sp=lax.rem(sp + o, n_sp), dp=lead,
        )
        for o in range(n_sp)
    ]
    for copy in a_copies[:0:-1]:
        copy.start()
    spare = remote(ctx.at[0], ctx.at[1], x_s.at[0], x_r.at[0], dp=lead)

    @pl.when(core == 0)
    def _():
        a_copies[0].start()

    loads[4].wait()
    gatef[...] = jnp.dot(activated, mod[2], preferred_element_type=F32)
    v_copies = [
        remote(
            gatef, gates.at[2 * o - 1 + core if o else 0], v_s.at[0], v_r.at[0],
            sp=lax.rem(sp + o, n_sp), dp=lead,
        )
        for o in range(n_sp)
    ]
    for copy in v_copies[1:]:
        copy.start()
    loads[3].wait()

    @pl.when(core == 0)
    def _():
        v_copies[0].start()
        spare.start()

    chunk = 64

    def normalise(src, dst, first, last):
        def body(i, carry):
            rows = pl.ds(pl.multiple_of(i * chunk, chunk), chunk)
            x = src[rows, :].astype(F32)
            x = x - jnp.mean(x, axis=-1, keepdims=True)
            spread = jnp.mean(x * x, axis=-1, keepdims=True)
            x = x * lax.rsqrt(spread + NORM_EPSILON)
            for t in range(n_tp):
                dst[t, rows, :] = x[:, t * group : (t + 1) * group]
            return carry

        lax.fori_loop(first, last, body, 0)

    def normalise_context(which):
        for i in range(0, n_ctx, chunk):
            x = ctx[which, i : i + chunk, :].astype(F32)
            x = x - jnp.mean(x, axis=-1, keepdims=True)
            spread = jnp.mean(x * x, axis=-1, keepdims=True)
            x = x * lax.rsqrt(spread + NORM_EPSILON)
            at = which * n_ctx + i
            for t in range(n_tp):
                xnc[t, at : at + chunk, :] = x[:, t * group : (t + 1) * group]

    loads[5].wait()
    normalise(lat, xn, 0, tok // chunk)

    @pl.when(core == 1)
    def _():
        normalise_context(0)
        spare.wait_recv()
        normalise_context(1)


    b_copies = [
        remote(
            sendb.at[lax.rem(dp + e, n_dp)], slots.at[o, pair], b_s.at[0], b_r.at[o],
            tp=partner(o), dp=lax.rem(dp + e, n_dp),
        )
        for o in reversed(range(n_tp))
        for e in range(n_dp)
        if o or e
    ]

    @pl.when(core == 1)
    def _():
        bytes_of(packs, a_r.at[0])
        for c in range(2):
            summed = packf[...] if c else packs[0].astype(F32)
            for o in range(1, n_sp):
                summed = summed + packs[2 * o - 1 + c].astype(F32)
            for d in range(n_dp):
                sendb[d, c] = summed[4 * d : 4 * d + 4, :].astype(BF16)
        for copy in b_copies:
            copy.start()
        slots[0, pair] = sendb[dp]

    bytes_of(wall, in_sem.at[6])
    for load in loads[9:12]:
        load.wait()
    groups = tok // GRID_W
    for g in range(groups):
        row = pl.ds(GRID_W + sp * groups + g, 1)
        span = slice(g * GRID_W, (g + 1) * GRID_W)
        cosv[span, :] = angles[0, row, :] + angles[0, 0:GRID_W, :]
        sinv[span, :] = angles[1, row, :] + angles[1, 0:GRID_W, :]
    for j in range(width // LANES):
        span = slice(j * LANES, (j + 1) * LANES)
        wall[span, q_width:] = kvw[:, span].astype(F32).T.astype(BF16)

    def condition(src, dst, count, o, g, shift_row, scale_row):
        scale = 1.0 + modv[o, scale_row : scale_row + 1, :]
        shift = modv[o, shift_row : shift_row + 1, :]
        for i in range(0, count, chunk):
            rows = slice(i, i + chunk)
            dst[o, rows, :] = (src[g, rows, :] * scale + shift).astype(BF16)

    c_copies = [remote(cxs.at[0], cxb.at[0], c_s.at[0], c_r.at[0], dp=dp - core)]
    for r in range(1, n_sp):
        for c in range(2):
            c_copies.append(
                remote(
                    cxs.at[c], cxb.at[r], c_s.at[0], c_r.at[0],
                    sp=lax.rem(sp + r, n_sp), dp=2 * pair + c,
                )
            )
    def land(o):
        if o:
            bytes_of(slots.at[o], b_r.at[o])
        else:
            @pl.when(core == 0)
            def _():
                bytes_of(slots.at[0], b_r.at[0])

            if n_pairs > 1:
                @pl.when(core == 1)
                def _():
                    bytes_of(slots.at[0, pl.ds(1, n_pairs - 1)], b_r.at[0])
        for d in range(n_dp):
            modv[o, 0:4, d * cols : (d + 1) * cols] = slots[o, d // 2, d % 2].astype(F32)

    def weight_rows(o):
        return pl.ds(pl.multiple_of(owner(o) * group, group), group)

    def context_part(o):
        condition(xnc, nrmc, 2 * n_ctx, o, owner(o), 2, 3)
        weights = wall[weight_rows(o), q_width:]
        return jnp.dot(nrmc[o], weights, preferred_element_type=F32)

    def latent_part(o):
        condition(xn, nrm, tok, o, owner(o), 0, 1)
        u = jnp.dot(nrm[o], wall[weight_rows(o), :], preferred_element_type=F32)
        acc[...] = acc[...] + u if o else u

    land(0)

    @pl.when(core == 1)
    def _():
        accc[...] = context_part(0)

    latent_part(0)

    @pl.when(core == 1)
    def _():
        u = accc[...]
        for o in range(1, n_tp):
            land(o)
            u = u + context_part(o)
        cxs[0] = u[n_ctx:, :].astype(BF16)
        cxs[1] = u[0:n_ctx, :].astype(BF16)
        for copy in c_copies[1:] + c_copies[:1]:
            copy.start()
        cxb[0] = u[0:n_ctx, :].astype(BF16)
        for o in range(1, n_tp):
            latent_part(o)

    @pl.when(core == 0)
    def _():
        for o in range(1, n_tp):
            land(o)
            latent_part(o)

    half = HEAD_SIZE // 2
    quarter = half // 2

    def turn(u, cosine, sine):
        w = u.shape[1]
        lane = lax.broadcasted_iota(jnp.int32, u.shape, 1)
        first = lax.rem(lane, half) < quarter
        swapped = jnp.where(first, pltpu.roll(u, w - quarter, 1), pltpu.roll(u, quarter, 1))
        return u * cosine + swapped * sine

    def low_half(shape):
        return lax.broadcasted_iota(jnp.int32, shape, 1) < HEAD_SIZE

    def expand(x, at):
        low = low_half(x.shape)
        other = pltpu.roll(x, HEAD_SIZE, 1)
        span = slice(at, at + x.shape[0])
        kd[span, :] = jnp.where(low, x, other).astype(BF16)
        vd[span, :] = jnp.where(low, other, x).astype(BF16)

    u = acc[:, q_width:]
    kv_rows = jnp.where(low_half(u.shape), turn(u, cosv[...], sinv[...]), u)
    kvb[reach : reach + tok, :] = kv_rows.astype(BF16)

    up = remote(
        kvb.at[pl.ds(tok, reach)], kvb.at[pl.ds(0, reach)], h_s.at[0], h_r.at[0],
         sp=lax.rem(sp + 1, n_sp)
    )
    down = remote(
        kvb.at[pl.ds(reach, reach)], kvb.at[pl.ds(reach + tok, reach)], h_s.at[0], h_r.at[1],
        sp=lax.rem(sp + n_sp - 1, n_sp),
    )

    @pl.when(sp < n_sp - 1)
    def _():
        up.start()

    @pl.when(sp > 0)
    def _():
        down.start()

    expand(kv_rows, reach)

    factor = HEAD_SIZE ** (-0.5)
    for p in range(pairs):
        t = turn(acc[:, p * LANES : (p + 1) * LANES], cosv[...], sinv[...]) * factor
        low = low_half(t.shape)
        for parity, kept in ((0, jnp.where(low, t, 0.0)), (1, jnp.where(low, 0.0, t))):
            kept = kept.astype(BF16)
            at = (2 * p + parity) * reach
            for b in range(blocks):
                q4[b, at : at + reach, :] = kept[b * reach : (b + 1) * reach, :]

    window = tok + 2 * reach
    nt = (((1,), (1,)), ((), ()))
    n_all_ctx = n_sp * n_ctx
    delta = lax.broadcasted_iota(jnp.int32, (reach, reach), 1) - lax.broadcasted_iota(
        jnp.int32, (reach, reach), 0
    )
    far = 4 * reach
    low_edge = jnp.where(sp == 0, far, 0)
    high_edge = jnp.where(sp == n_sp - 1, -far, 0)

    def scores(b, first, count):
        keys = kd[first : first + count, :]
        return lax.dot_general(q4[b], keys, nt, preferred_element_type=F32)

    def tiles(s, h):
        rows = slice(h * reach, (h + 1) * reach)
        return [s[rows, c * LANES : (c + 1) * LANES] for c in range(s.shape[1] // LANES)]

    def soften(parts, highest):
        powers = [jnp.exp(s - highest) for s in parts]
        mass = powers[0]
        for e in powers[1:]:
            mass = mass + e
        powers = jnp.concatenate([e.astype(BF16) for e in powers], axis=1)
        return powers, jnp.sum(mass, axis=-1, keepdims=True)

    def top_of(parts):
        top = parts[0]
        for s in parts[1:]:
            top = jnp.maximum(top, s)
        return jnp.max(top, axis=-1, keepdims=True)

    def weigh(powers, first):
        e = jnp.concatenate(powers, axis=0)
        return jnp.dot(e, vd[first : first + e.shape[1], :], preferred_element_type=F32)

    def within(b):
        first, last = max(b - 1, 0), min(b + 1, blocks - 1)
        at = reach + first * reach
        s = scores(b, at, (last - first + 1) * reach)
        tops, masses, powers = [], [], []
        for h in range(heads):
            parts = tiles(s, h)
            if b > 0:
                parts[0] = jnp.where(delta >= 0, parts[0], MASKED)
            if b < blocks - 1:
                parts[-1] = jnp.where(delta <= 0, parts[-1], MASKED)
            highest = jnp.maximum(top_of(parts), sink[h])
            e, mass = soften(parts, highest)
            tops.append(highest)
            masses.append(mass + jnp.exp(sink[h] - highest))
            powers.append(e)
        return tops, masses, weigh(powers, at)


    def beyond(b, state, some):
        tops, masses, weighed = state
        first, last = some[0] * reach, (some[-1] + 1) * reach
        q2 = q4[b, first:last, :]

        def scores(at, count):
            keys = kd[at : at + count, :]
            return lax.dot_general(q2, keys, nt, preferred_element_type=F32)

        parts_of = [(window, scores(window, n_all_ctx))]
        edges = []
        if b == 0:
            edges.append((0, lambda s: jnp.where(delta >= low_edge, s, MASKED)))
        if b == blocks - 1:
            edges.append((reach + tok, lambda s: jnp.where(delta <= high_edge, s, MASKED)))
        for at, _ in edges:
            parts_of.append((at, scores(at, reach)))
        fades, powers = {}, [[] for _ in parts_of]
        for i, h in enumerate(some):
            groups = [[s + bias[h] for s in tiles(parts_of[0][1], i)]]
            for (_, mask), (_, s) in zip(edges, parts_of[1:]):
                groups.append([mask(s) for s in tiles(s, i)])
            top = jnp.maximum(top_of(sum(groups, [])), tops[h])
            fade = jnp.exp(tops[h] - top)
            mass = masses[h] * fade
            for kept, parts in zip(powers, groups):
                e, more = soften(parts, top)
                kept.append(e)
                mass = mass + more
            share = 1.0 / mass
            fades[h] = (fade * share, share)
        more = weigh(powers[0], window)
        for kept, (at, _) in zip(powers[1:], parts_of[1:]):
            more = more + weigh(kept, at)
        low = low_half((reach, LANES))
        for p in range(some[0] // 2, some[-1] // 2 + 1):
            halves = []
            for h in (2 * p, 2 * p + 1):
                rows = slice(h * reach, (h + 1) * reach)
                mine = slice(h * reach - first, (h + 1) * reach - first)
                halves.append(weighed[rows, :] * fades[h][0] + more[mine, :] * fades[h][1])
            att[0, b, :, p * LANES : (p + 1) * LANES] = jnp.where(low, *halves).astype(BF16)

    middle = reach // 2

    def send(b, o, relay, first=0, count=q_width):
        if relayed:
            at = (o - 1) * middle if relay else (2 - o) * middle
            span = (b, pl.ds(at, middle), pl.ds(first, count))
        else:
            span = (b, slice(None), pl.ds(first, count))
        remote(
            att.at[(0, *span)], att.at[(o, *span)], g_s.at[0], g_r.at[b, 0 if relay else 1],
            tp=partner(o),
        ).start()

    def forward(b):
        bytes_of(att.at[1, b], g_r.at[b, 0])
        for o in direct:
            part = pl.ds((o - 1) * middle, middle)
            remote(
                att.at[o, b, part], att.at[3, b, part], g_s.at[0], g_r.at[b, 2], tp=partner(3 - o)
            ).start()

    order = list(range(1, blocks - 1)) + ([0, blocks - 1] if blocks > 1 else [0])
    states = {}
    early = order
    for b in early:
        states[b] = within(b)
    w_copies = [
        remote(
            gateb.at[lax.rem(dp + e, n_dp)], gatev.at[pair], w_s.at[0], w_r.at[0],
            dp=lax.rem(dp + e, n_dp),
        )
        for e in range(1, n_dp)
    ]

    @pl.when(core == 1)
    def _():
        bytes_of(gates, v_r.at[0])
        for c in range(2):
            summed = gatef[...] if c else gates[0]
            for o in range(1, n_sp):
                summed = summed + gates[2 * o - 1 + c]
            for d in range(n_dp):
                gateb[d, c] = jnp.broadcast_to(summed[d : d + 1, :], (8, cols))
        for copy in w_copies:
            copy.start()
        gatev[pair] = gateb[dp]


    @pl.when(core == 0)
    def _():
        bytes_of(cxb.at[pl.ds(0, n_sp)], c_r.at[0])

    @pl.when(core == 1)
    def _():
        bytes_of(cxb.at[pl.ds(1, n_sp - 1)], c_r.at[0])

    for r in range(n_sp):
        expand(cxb[r].astype(F32), window + r * n_ctx)
    held = []
    for b in order:
        if b not in states:
            states[b] = within(b)
        if b == 0:
            @pl.when(sp > 0)
            def _():
                up.wait_recv()

            @pl.when(sp == 0)
            def _():
                kvb[0:reach, :] = jnp.zeros((reach, LANES), BF16)

            expand(kvb[0:reach, :].astype(F32), 0)
        if b == blocks - 1:
            @pl.when(sp < n_sp - 1)
            def _():
                down.wait_recv()

            @pl.when(sp == n_sp - 1)
            def _():
                kvb[reach + tok : window, :] = jnp.zeros((reach, LANES), BF16)

            expand(kvb[reach + tok : window, :].astype(F32), reach + tok)
        beyond(b, states[b], tuple(range(heads)))
        for o in direct:
            send(b, o, True)
        if relayed:
            held.append(b)
            if b == order[0] or b == order[-1]:
                for c in held:
                    for o in direct:
                        send(c, o, False)
                held.clear()

    loads[12].wait()
    out_cols = ow.shape[1]
    mine = pl.ds(pl.multiple_of(tp * out_cols, out_cols), out_cols)

    @pl.when(core == 0)
    def _():
        bytes_of(gatev, w_r.at[0])

    if n_pairs > 1:
        @pl.when(core == 1)
        def _():
            bytes_of(gatev.at[pl.ds(1, n_pairs - 1)], w_r.at[0])

    for d in range(n_dp):
        modv[0, :, d * cols : (d + 1) * cols] = gatev[d // 2, d % 2]
    gate = modv[0, 0:1, :]

    def project(b, o):
        w = ow[pl.ds(pl.multiple_of(owner(o) * q_width, q_width), q_width), :]
        return jnp.dot(att[o, b], w, preferred_element_type=F32)

    for b in order:
        if relayed:
            forward(b)
        else:
            bytes_of(att.at[pl.ds(1, n_tp - 1), b], g_r.at[b, 0])
        outv[b * reach : (b + 1) * reach, :] = project(b, 0)
    for b in order:
        if relayed:
            bytes_of(att.at[1, b], g_r.at[b, 1])
        rows = slice(b * reach, (b + 1) * reach)
        mixed = outv[rows, :]
        for o in direct:
            mixed = mixed + project(b, o)
        outv[rows, :] = mixed
    for b in order:
        rows = slice(b * reach, (b + 1) * reach)
        mixed = outv[rows, :]
        if relayed:
            bytes_of(att.at[3, b], g_r.at[b, 2])
            mixed = mixed + project(b, 3)
        outv[rows, :] = lat[rows, mine].astype(F32) + gate * mixed

    bytes_of(att.at[pl.ds(1, n_tp - 1)], g_s.at[0])

    @pl.when(core == 0)
    def _():
        bytes_of(packs.at[pl.ds(0, n_sp)], a_s.at[0])
        bytes_of(gates.at[pl.ds(0, n_sp)], v_s.at[0])
        spare.wait_send()

    @pl.when(core == 1)
    def _():
        bytes_of(packs.at[pl.ds(0, n_sp - 1)], a_s.at[0])
        bytes_of(gates.at[pl.ds(0, n_sp - 1)], v_s.at[0])
        bytes_of(sendb.at[pl.ds(0, n_td - 1)], b_s.at[0])
        bytes_of(gateb.at[pl.ds(0, n_dp - 1)], w_s.at[0])
        bytes_of(cxb, c_s.at[0])

    edge = jnp.logical_or(sp == 0, sp == n_sp - 1)

    @pl.when(edge)
    def _():
        bytes_of(kvb.at[pl.ds(0, reach)], h_s.at[0])

    @pl.when(jnp.logical_not(edge))
    def _():
        bytes_of(kvb.at[pl.ds(0, 2 * reach)], h_s.at[0])


def scoped_kernel(dims, *refs):
    dma = pltpu.SemaphoreType.DMA
    pl.run_scoped(
        lambda *local: block_kernel(dims, *refs, *local), dma((11,)), *[dma((1,))] * 8
    )


def per_device(
    latent, conditioning, context_cond, modulation, context, query_weight, key_projection,
    value_projection, out_weight, sink_head_logit, prefix_logit_bias,
):
    n_sp, n_tp, n_dp = lax.axis_size("sp"), lax.axis_size("tp"), lax.axis_size("dp")
    samples = conditioning.shape[0]
    _, tok, width = latent.shape
    n_ctx = context.shape[1]
    depth, cols = modulation.shape[1:]
    q_width = query_weight.shape[1]
    heads = q_width // HEAD_SIZE
    out_cols = out_weight.shape[1]
    blocks = tok // WINDOW_REACH
    window = tok + 2 * WINDOW_REACH
    keys = window + n_sp * n_ctx
    n_td = n_tp * n_dp
    act_rows = -(-(samples + 1) // 8) * 8
    pack_rows = -(-(4 * samples) // 8) * 8
    row_table, col_table = rotary_tables(n_sp * tok // GRID_W)
    table = np.concatenate([col_table, row_table], axis=1)
    vm = pltpu.VMEM
    dma = pltpu.SemaphoreType.DMA
    group = n_dp * cols
    scratch = [
        vm((tok, width), BF16), vm((samples, depth), BF16), vm((depth,), BF16),
        vm((3, depth, cols), BF16), vm((2, n_ctx, width), BF16), vm((width, q_width + LANES), BF16),
        vm(out_weight.shape, BF16), pltpu.SMEM((heads,), F32), pltpu.SMEM((heads,), F32),
        vm(table.shape, F32),
        vm((act_rows, depth), F32), vm((pack_rows, cols), F32), vm((pack_rows, cols), BF16),
        vm((2 * n_sp - 1, pack_rows, cols), BF16),
        vm((n_td, 2, 4, cols), BF16), vm((n_tp, n_dp // 2, 2, 4, cols), BF16),
        vm((n_tp, 8, group), F32), vm((act_rows, cols), F32),
        vm((2 * n_sp - 1, act_rows, cols), F32), vm((n_dp, 2, 8, cols), F32),
        vm((n_dp // 2, 2, 8, cols), F32),
        vm((n_tp, tok, group), F32), vm((n_tp, 2 * n_ctx, group), F32), vm((n_tp, tok, group), BF16),
        vm((n_tp, 2 * n_ctx, group), BF16), vm((LANES, width), BF16), vm((tok, LANES), F32),
        vm((tok, LANES), F32), vm((tok, q_width + LANES), F32), vm((2 * n_ctx, LANES), F32),
        vm((window, LANES), BF16), vm((2, n_ctx, LANES), BF16), vm((2 * n_sp - 1, n_ctx, LANES), BF16),
        vm((keys, LANES), BF16), vm((keys, LANES), BF16),
        vm((blocks, heads * WINDOW_REACH, LANES), BF16),
        vm((n_tp, blocks, WINDOW_REACH, q_width), BF16),
        dma((1,)), dma((1,)), dma((n_tp,)), dma((2,)), dma((1,)), dma((blocks, 3)), dma((1,)),
        dma((1,)),
    ]
    stays = pl.BlockSpec(memory_space=pltpu.HBM)
    out = pl.pallas_call(
        functools.partial(scoped_kernel, (n_sp, n_tp, n_dp, samples)),
        out_shape=pltpu.VMEM((tok, out_cols), F32),
        in_specs=[stays] * 12,
        out_specs=pl.BlockSpec(memory_space=pltpu.VMEM),
        scratch_shapes=scratch,
        compiler_params=pltpu.CompilerParams(
            collective_id=0, has_side_effects=True, vmem_limit_bytes=66000000
        ),
        name="fused_block",
    )(
        latent[0], conditioning, context_cond, modulation, context[0], query_weight,
        key_projection.T, value_projection.T, out_weight, sink_head_logit, prefix_logit_bias,
        jnp.asarray(table),
    )
    return out[None]


def solution(mesh):
    placed = (
        P("dp", "sp", None),
        P(None, "sp"),
        P("sp"),
        P(None, "sp", ("tp", "dp")),
        P("dp", "sp", None),
        P(None, "tp"),
        P(None, "tp"),
        P(None, "tp"),
        P(None, "tp"),
        P("tp"),
        P("tp"),
    )
    return jax.shard_map(
        per_device, mesh=mesh, in_specs=placed, out_specs=P("dp", "sp", "tp"), check_vma=False
    )
```
